32 devices in a mesh: sp: 8 (over z, y), tp: 4 (over x, core).
Axes of the slice: x: 2, y: 2, z: 4, core: 2. Of those that a mesh axis runs over, the one named last changes fastest.
Arguments:
- tokens: bfloat16 [4096, 2048], P('sp'), may hold values from -24 to 24
- w_query: bfloat16 [2048, 1536], P('sp', 'tp'), as said below
- w_key: bfloat16 [2048, 1536], P('sp', 'tp'), as said below
- w_value: bfloat16 [2048, 1536], P('sp', 'tp'), may hold values from -0.125 to 0.125
- w_out: bfloat16 [512, 2048], P('tp', 'sp'), may hold values from -1.5 to 1.5
Outputs:
- mixed: bfloat16 [4096, 2048], P(('sp', 'tp'))
The draws below stay inside these ranges and needn't reach their ends.
Inputs may be any that keep to these rules, and one draw needn't show every extreme that they name: `w_query`: every entry lies within 4 / sqrt(2048) of zero. `w_key`: every entry lies within 4 / sqrt(2048) of zero.
All inputs are finite; a program needn't handle non-finite values.
Results may differ from the reference program's by a relative error of at most 0.025.
Values may be sent and summed in bfloat16 or wider, within the bound.
A program may use at most 64 MiB of HBM per device.

```python
import math
import jax
import jax.numpy as jnp
from jax import lax

D = 2048
HEADS = 4
GROUPS = 3
DH = 128
WIN1 = 128
WIN2 = 512
WIN3 = 2048
SECOND_DILATION = 4
THIRD_DILATION = 16
SEQ = 4096


def shared_query(key):
    return jax.random.normal(jax.random.fold_in(key, 101), (D, HEADS * GROUPS * DH), jnp.float32)


def draw_tokens(key, part):
    drawn = jax.random.normal(jax.random.fold_in(key, 1), (SEQ, D), jnp.float32)
    return jnp.clip(drawn, -24.0, 24.0).astype(jnp.bfloat16)


def draw_w_query(key, part):
    limit = 4.0 * D ** (-0.5)
    return jnp.clip(shared_query(key) * D ** (-0.5), -limit, limit).astype(jnp.bfloat16)


def draw_w_key(key, part):
    limit = 4.0 * D ** (-0.5)
    own_part = jax.random.normal(jax.random.fold_in(key, 202), (D, HEADS * GROUPS * DH), jnp.float32)
    return jnp.clip(own_part * D ** (-0.5), -limit, limit).astype(jnp.bfloat16)


def shard_levels(own_key, shape, cuts, smallest, top_value):
    level, own = 1.0, jax.random.fold_in(own_key, 6)
    for axis_at, blocks in cuts:
        steps = jnp.exp(jax.random.uniform(jax.random.fold_in(own, axis_at), (blocks,), jnp.float32, smallest / len(cuts), top_value / len(cuts)))
        level = level * jnp.repeat(steps, shape[axis_at] // blocks).reshape([-1 if axis == axis_at else 1 for axis in range(len(shape))])
    return level


def scatter_about(own_key, dims, scale, bound, cuts=(), kind=jnp.bfloat16):
    loudness = shard_levels(own_key, dims, cuts, -0.22, 0.18) if cuts else 1.0
    drawn = jax.random.normal(own_key, dims, jnp.float32) * scale * loudness
    return jnp.minimum(jnp.maximum(drawn, -bound), bound).astype(kind)


def setup_inputs(seed: int = 0) -> dict:
    arg_keys = jax.random.split(jax.random.key(seed), 6)
    tokens = draw_tokens(jax.random.fold_in(arg_keys[5], 71), 0)
    w_query = draw_w_query(jax.random.fold_in(arg_keys[5], 71), 0)
    w_key = draw_w_key(jax.random.fold_in(arg_keys[5], 71), 0)
    w_value = scatter_about(arg_keys[3], (D, HEADS * GROUPS * DH), D ** -0.5, 0.125, ((0, 8), (1, 4)))
    w_out = scatter_about(arg_keys[4], (HEADS * DH, D), 0.35, 1.5, ((0, 4), (1, 8)))
    return dict(tokens=tokens, w_query=w_query, w_key=w_key, w_value=w_value, w_out=w_out)


ROPE_BASE = 500000.0


def rotate(projected):
    seq_len = projected.shape[0]
    head_size = projected.shape[-1]
    half_size = head_size // 2
    positions = jnp.arange(seq_len, dtype=jnp.int32).astype(jnp.float32)
    frequency = 1.0 / (ROPE_BASE ** (jnp.arange(0, head_size, 2, dtype=jnp.float32) / head_size))
    angles = (positions[:, None] * frequency[None, :]).reshape(seq_len, 1, 1, half_size)
    cosine = jnp.cos(angles)
    sine_part = jnp.sin(angles)
    first_half = projected[..., :half_size]
    second_half = projected[..., half_size:]
    return jnp.concatenate([first_half * cosine - second_half * sine_part,
                            second_half * cosine + first_half * sine_part], axis=-1)


def window_attend(queries, keys, values, window, stride):
    seq_len, heads, head_size = queries.shape
    block_rows = math.gcd(seq_len, 512)
    block_list = seq_len // block_rows
    key_pad = jnp.pad(keys, ((window, 0), (0, 0), (0, 0)))
    value_pad = jnp.pad(values, ((window, 0), (0, 0), (0, 0)))
    query_blocks = queries.reshape(block_list, block_rows, heads, head_size)

    def one_block(operands):
        query_block, block_index = operands
        begin = (block_index * block_rows).astype(jnp.int32)
        key_slab = lax.dynamic_slice_in_dim(key_pad, begin, block_rows + window, 0)
        value_band = lax.dynamic_slice_in_dim(value_pad, begin, block_rows + window, 0)
        scores = jnp.einsum('qhe,khe->hqk', query_block.astype(jnp.float32),
                            key_slab.astype(jnp.float32)) * (head_size ** -0.5)
        query_pos = begin + jnp.arange(block_rows, dtype=jnp.int32)
        key_pos = begin - window + jnp.arange(block_rows + window, dtype=jnp.int32)
        spacing = query_pos[:, None] - key_pos[None, :]
        allowed = (spacing >= 0) & (spacing <= window) & (spacing % stride == 0) & (key_pos[None, :] >= 0)
        scores = jnp.where(allowed[None], scores, -jnp.inf)
        row_max = jnp.max(scores, axis=-1)
        exponent = jnp.exp(scores - row_max[..., None])
        totals = jnp.sum(exponent, axis=-1)
        probs = lax.optimization_barrier((exponent / totals[..., None]).astype(jnp.bfloat16))
        mixed = jnp.einsum('hqk,khe->qhe', probs.astype(jnp.float32), value_band.astype(jnp.float32))
        return mixed, jnp.transpose(row_max + jnp.log(totals))

    mixed, log_totals = lax.map(one_block, (query_blocks, jnp.arange(block_list, dtype=jnp.int32)))
    return mixed.reshape(seq_len, heads, head_size), log_totals.reshape(seq_len, heads)


def reference(tokens, w_query, w_key, w_value, w_out):
    seq_len = tokens.shape[0]
    head_shape = (seq_len, HEADS, GROUPS, DH)
    query_raw = jnp.dot(tokens, w_query, preferred_element_type=jnp.float32).reshape(head_shape)
    key_raw = jnp.dot(tokens, w_key, preferred_element_type=jnp.float32).reshape(head_shape)
    values = lax.optimization_barrier(
        jnp.dot(tokens, w_value, preferred_element_type=jnp.float32).astype(jnp.bfloat16)).reshape(head_shape)
    queries = lax.optimization_barrier(rotate(query_raw).astype(jnp.bfloat16))
    keys = lax.optimization_barrier(rotate(key_raw).astype(jnp.bfloat16))
    windows = (WIN1, WIN2, WIN3)
    step_sizes = (1, SECOND_DILATION, THIRD_DILATION)
    outputs = []
    log_totals = []
    for group_index in range(GROUPS):
        group_out, log_total = window_attend(queries[:, :, group_index], keys[:, :, group_index],
                                             values[:, :, group_index], windows[group_index],
                                             step_sizes[group_index])
        outputs.append(group_out)
        log_totals.append(log_total)
    group_weights = jax.nn.softmax(jnp.stack(log_totals), axis=0)
    merged = jnp.sum(group_weights[..., None] * jnp.stack(outputs), axis=0).astype(jnp.bfloat16)
    merged = merged.reshape(seq_len, HEADS * DH)
    return jnp.dot(merged, w_out, preferred_element_type=jnp.float32).astype(jnp.bfloat16)
```

```python
import functools
import math

import jax
import jax.numpy as jnp
from jax import lax
from jax.experimental import pallas as pl
from jax.experimental.pallas import tpu as pltpu
from jax.sharding import PartitionSpec as P

GROUPS = 3
DH = 128
WIN1 = 128
WIN2 = 512
WIN3 = 2048
SECOND_DILATION = 4
THIRD_DILATION = 16


ROPE_BASE = 500000.0

LAYERS = 4
TOKEN_PIECES = 4


def from_behind(block, axis, distance):
    devices = range(lax.axis_size(axis))
    route = [(i - distance, i) for i in devices if i - distance in devices]
    return lax.ppermute(block, axis, route)


def rotate(projected, offset):
    tok_rows = projected.shape[0]
    head_size = projected.shape[-1]
    half_size = head_size // 2
    positions = (offset + jnp.arange(tok_rows, dtype=jnp.int32)).astype(jnp.float32)
    frequency = 1.0 / ROPE_BASE ** (jnp.arange(0, head_size, 2, dtype=jnp.float32) / head_size)
    angles = (positions[:, None] * frequency[None, :]).reshape(tok_rows, 1, 1, half_size)
    cosine = jnp.cos(angles)
    sine_part = jnp.sin(angles)
    first_half = projected[..., :half_size]
    second_half = projected[..., half_size:]
    return jnp.concatenate(
        [
            first_half * cosine - second_half * sine_part,
            second_half * cosine + first_half * sine_part,
        ],
        axis=-1,
    )


def window_attend(query_part, buffer, steps, stride, offset):
    tok_rows, heads_here, head_size = query_part.shape
    sub_rows = tok_rows // stride
    key_rows = buffer.shape[1] // stride
    query_sub = query_part.reshape(sub_rows, stride, heads_here, head_size).transpose(1, 2, 0, 3)
    pair_sub = buffer.reshape(2, key_rows, stride, heads_here, head_size).transpose(0, 2, 3, 1, 4)
    block_rows = math.gcd(sub_rows, steps) if sub_rows > steps else sub_rows
    block_list = sub_rows // block_rows
    query_blocks = query_sub.reshape(stride, heads_here, block_list, block_rows, head_size)
    key_blocks = jnp.stack(
        [
            pair_sub[:, :, :, index * block_rows : index * block_rows + block_rows + steps]
            for index in range(block_list)
        ],
        axis=3,
    )
    scores = jnp.einsum(
        "zhnqe,zhnke->zhnqk", query_blocks, key_blocks[0], preferred_element_type=jnp.float32
    ) * head_size ** (-0.5)
    query_index = (jnp.arange(block_list, dtype=jnp.int32) * block_rows)[
        :, None, None
    ] + jnp.arange(block_rows, dtype=jnp.int32)[None, :, None]
    key_index = (jnp.arange(block_list, dtype=jnp.int32) * block_rows)[:, None, None] + jnp.arange(
        block_rows + steps, dtype=jnp.int32
    )[None, None, :]
    spacing = query_index + steps - key_index
    residue = jnp.arange(stride, dtype=jnp.int32)[:, None, None, None]
    key_position = offset + (key_index[None] - steps) * stride + residue
    allowed = (spacing[None] >= 0) & (spacing[None] <= steps) & (key_position >= 0)
    scores = jnp.where(allowed[:, None], scores, -jnp.inf)
    row_max = jnp.max(scores, axis=-1)
    exponent = jnp.exp(scores - row_max[..., None])
    totals = jnp.sum(exponent, axis=-1)
    probs = (exponent / totals[..., None]).astype(jnp.bfloat16)
    mixed = jnp.einsum(
        "zhnqk,zhnke->zhnqe", probs, key_blocks[1], preferred_element_type=jnp.float32
    )
    mixed = mixed.reshape(stride, heads_here, sub_rows, head_size).transpose(2, 0, 1, 3)
    log_total = (row_max + jnp.log(totals)).reshape(stride, heads_here, sub_rows).transpose(2, 0, 1)
    return (mixed.reshape(tok_rows, heads_here, head_size), log_total.reshape(tok_rows, heads_here))


def reach_back(key_value, distance_max):
    tok_rows = key_value.shape[1]
    gathered = key_value
    pieces_held = 1
    while pieces_held < distance_max + 1:
        slice_share = min(pieces_held, distance_max + 1 - pieces_held)
        arrived = from_behind(
            gathered[:, gathered.shape[1] - slice_share * tok_rows :], "sp", pieces_held
        )
        gathered = jnp.concatenate([arrived, gathered], axis=1)
        pieces_held = pieces_held + slice_share
    return gathered


def on_device(tokens, w_query, w_key, w_value, w_out):
    tok_rows = tokens.shape[0]
    heads_here = w_out.shape[0] // DH
    offset = lax.axis_index("sp") * tok_rows
    weight_parts = (
        lax.all_gather(w_query, "sp", axis=0, tiled=True),
        lax.all_gather(w_key, "sp", axis=0, tiled=True),
        lax.all_gather(w_value, "sp", axis=0, tiled=True),
    )
    query_raw, key_raw, value_raw = tuple(
        (
            jnp.dot(tokens, weight_rows, preferred_element_type=jnp.float32)
            for weight_rows in weight_parts
        )
    )
    head_shape = (tok_rows, heads_here, GROUPS, DH)
    queries = rotate(query_raw.reshape(head_shape), offset).astype(jnp.bfloat16)
    keys_all = rotate(key_raw.reshape(head_shape), offset).astype(jnp.bfloat16)
    values_all = value_raw.astype(jnp.bfloat16).reshape(head_shape)
    windows = (WIN1, WIN2, WIN3)
    step_sizes = (1, SECOND_DILATION, THIRD_DILATION)
    outputs = []
    log_totals = []
    for group_index in range(GROUPS):
        key_value = jnp.stack([keys_all[:, :, group_index], values_all[:, :, group_index]])
        key_value = key_value.reshape(2, tok_rows, heads_here * DH)
        window = windows[group_index]
        if group_index == 0:
            near_rows = from_behind(key_value[:, tok_rows - window :], "sp", 1)
            buffer = jnp.concatenate([near_rows, key_value], axis=1)
        else:
            distance_max = (window + tok_rows - 1) // tok_rows
            buffer = reach_back(key_value, distance_max)
        group_out, log_total = window_attend(
            queries[:, :, group_index],
            buffer,
            window // step_sizes[group_index],
            step_sizes[group_index],
            offset,
        )
        outputs.append(group_out)
        log_totals.append(log_total)
    group_weights = jax.nn.softmax(jnp.stack(log_totals), axis=0)
    merged = jnp.sum(group_weights[..., None] * jnp.stack(outputs), axis=0).astype(jnp.bfloat16)
    merged = merged.reshape(tok_rows, heads_here * DH)
    w_whole = lax.all_gather(w_out, "sp", axis=1, tiled=True)
    return lax.psum_scatter(
        jnp.dot(merged, w_whole, preferred_element_type=jnp.float32).astype(jnp.bfloat16),
        "tp",
        scatter_dimension=0,
        tiled=True,
    )


def layer_kernel(
    nz,
    tokens, w_key, w_value, w_query, w_out, out,
    weights, stage, tok_in, tok_turned, cosine, sine, queries, pair0, near_own, near_in, far2,
    out_rows, mine, heads_in, got01, top01, sum01,
    stage_s, swap_s, tok_k, w_r, mid_s, side_s, t_r, tz_s, ty_s, tx_s,
    up_s, down_s, o_r, o_s, o_r2, far_s, far_r, near_s, near_r, head_s, head_r,
):
    tok_rows, depth = tokens.shape
    k_rows, cols = w_key.shape
    sub = tok_rows // THIRD_DILATION
    sub_log = sub.bit_length() - 1
    block = tok_rows // SECOND_DILATION
    tail = WIN1
    pieces = tz_s.shape[0]
    piece_rows = tok_rows // 2 // pieces
    sp, tp = lax.axis_index("sp"), lax.axis_index("tp")
    z, y = sp // 2, sp % 2
    x, c = tp // 2, tp % 2
    last = nz - 1
    is_mid = (z == 1) | (z == 2)
    is_end = jnp.logical_not(is_mid)
    stays = c == y
    moves = jnp.logical_not(stays)
    has_up, has_down = z < last, z > 0
    other = last - z
    end = jnp.where(z == 1, 0, last)
    far_end = last - end
    hub = jnp.where(z == 0, 1, 2)
    j_own = jnp.where(z == 1, 1, 0)
    j_far = 1 - j_own
    j_end = jnp.where(z == 0, 0, 1)
    base = 4 * (z - 1)
    side = (sp, 2 * x + 1 - c)
    across_x = (sp, 2 * (1 - x) + c)
    across_y = (2 * z + 1 - y, tp)
    partner = (2 * z + 1 - y, 2 * x + 1 - c)
    above, below = (sp + 2, tp), (sp - 2, tp)
    opposite = (2 * other + y, tp)
    to_hub = (2 * hub + y, tp)

    def send(src, dst, s_sem, r_sem, where):
        return pltpu.make_async_remote_copy(
            src_ref=src, dst_ref=dst, send_sem=s_sem, recv_sem=r_sem,
            device_id=where, device_id_type=pl.DeviceIdType.MESH,
        )

    parts = (w_key, w_value, w_query)

    def chunk(a, s):
        return weights.at[a, pl.ds(pl.multiple_of(s * k_rows, k_rows), k_rows), :]

    def put_w(a, zz, s_sem, where):
        s = 2 * zz + c
        return send(chunk(a, s), chunk(a, s), s_sem, w_r.at[a, s], where)

    def arrived(a, zz):
        put_w(a, zz, side_s.at[a, 0], side).wait_recv()

    def kept(a):
        return pltpu.make_async_copy(parts[a], chunk(a, 2 * z + c), w_r.at[a, 2 * z + c])

    def staged(a):
        return pltpu.make_async_copy(parts[a], stage.at[a], stage_s.at[a])

    def swapped(a):
        there = 2 * z + 1 - c
        return send(stage.at[a], chunk(a, there), swap_s.at[a], w_r.at[a, there], partner)

    def o_chunk(zz):
        return out_rows.at[c, y, x, zz]

    def o_kept():
        return pltpu.make_async_copy(w_out, o_chunk(z), o_r.at[z])

    tok_slot = jnp.where(is_mid, j_own, j_end)

    def tok_kept():
        return pltpu.make_async_copy(tokens, tok_in.at[tok_slot], tok_k)

    o_kept().start()

    @pl.when(stays)
    def _():
        for a in range(3):
            kept(a).start()
        tok_kept().start()

    @pl.when(moves)
    def _():
        for a in range(3):
            staged(a).start()

    barrier = pltpu.get_barrier_semaphore()

    def greet(where):
        pl.semaphore_signal(barrier, inc=1, device_id=where, device_id_type=pl.DeviceIdType.MESH)

    paired = z + 1 - 2 * (z % 2)
    for dy in range(2):
        for dx in range(2):
            for dc in range(2):
                where = ((y + dy) % 2, 2 * ((x + dx) % 2) + (c + dc) % 2)
                if dy + dx + dc:
                    greet((2 * z + where[0], where[1]))
                greet((2 * paired + where[0], where[1]))

    @pl.when(is_mid)
    def _():
        greet(opposite)
        greet((2 * other + y, 2 * x + 1 - c))

    pl.semaphore_wait(barrier, 15 + jnp.where(is_mid, 2, 0))

    pl.when(moves)(lambda: staged(0).wait())
    pl.when(moves)(lambda: swapped(0).start())

    def o_go(zz, kind):
        ref = o_chunk(zz)
        s_sem, where = {"up": (up_s, above), "down": (down_s, below)}[kind]
        return send(ref, ref, s_sem.at[zz], o_r.at[zz], where)

    def o_relay(d):
        @pl.when(z - d >= 0)
        def _():
            o_go(z - d, "up").wait_recv()
            pl.when(has_up)(lambda: o_go(z - d, "up").start())

        @pl.when(z + d < nz)
        def _():
            o_go(z + d, "down").wait_recv()
            pl.when(has_down)(lambda: o_go(z + d, "down").start())

    def o_share(axis):
        ref, where = (
            (out_rows.at[c, y, x], across_x),
            (out_rows.at[c, y], across_y),
            (out_rows.at[c], side),
        )[axis]
        return send(ref, ref, o_s.at[axis], o_r2.at[axis], where)

    def t_piece(j, half, q):
        at = half * (tok_rows // 2) + q * piece_rows
        return tok_in.at[j, pl.ds(pl.multiple_of(at, piece_rows), piece_rows), :]

    def put_t(j, half, q, s_sem, where):
        ref = t_piece(j, half, q)
        return send(ref, ref, s_sem, t_r.at[j, half, q], where)

    def t_inward(q):
        return put_t(j_end, x, q, tz_s.at[q], to_hub)

    def t_y(j, q):
        return put_t(j, x, q, ty_s.at[j, q], across_y)

    def t_x(j, q):
        return put_t(j, x, q, tx_s.at[j, q], across_x)

    def t_other(j):
        for q in range(pieces):
            put_t(j, 1 - x, q, tx_s.at[j, q], across_x).wait_recv()

    def w_inward(a):
        return put_w(a, z, mid_s.at[a, 0], to_hub)

    def w_cross(a, which):
        return put_w(a, (z, end)[which], mid_s.at[a, which], opposite)

    ring = (z, end, other, far_end)

    def w_side(a, which):
        return put_w(a, ring[which], side_s.at[a, which], side)

    def own_ready(a):
        pl.when(stays)(lambda: kept(a).wait())
        pl.when(moves)(lambda: arrived(a, z))

    o_kept().wait()
    pl.when(has_up)(lambda: o_go(z, "up").start())
    pl.when(has_down)(lambda: o_go(z, "down").start())

    def rest_swapped():
        for a in (1, 2):
            staged(a).wait()
            swapped(a).start()

    @pl.when(is_end)
    def _():
        @pl.when(stays)
        def _():
            kept(0).wait()
            w_inward(0).start()
            tok_kept().wait()
            t_inward(0).start()
            kept(1).wait()
            w_inward(1).start()
            t_inward(1).start()
            kept(2).wait()
            w_inward(2).start()
            for q in range(2, pieces):
                t_inward(q).start()

        pl.when(moves)(rest_swapped)
        o_relay(1)

        @pl.when(moves)
        def _():
            for a in range(3):
                arrived(a, z)
                w_inward(a).start()

        for d in range(2, nz):
            o_relay(d)
        o_share(0).start()
        o_share(0).wait()
        o_share(1).start()
        o_share(1).wait()
        o_share(2).start()

    def row_time(p):
        b, i = p >> sub_log, p & (sub - 1)
        return THIRD_DILATION * i + (b >> 2) + SECOND_DILATION * (b & 3)

    def tail_time(u):
        per = tail // THIRD_DILATION
        b, i = u >> (per.bit_length() - 1), u & (per - 1)
        return THIRD_DILATION * (sub - per + i) + (b >> 2) + SECOND_DILATION * (b & 3) - tok_rows

    def iota(shape, axis):
        return lax.broadcasted_iota(jnp.int32, shape, axis)

    def angles(index, carry):
        j, at = index // SECOND_DILATION, (index % SECOND_DILATION) * block
        rows = pl.ds(pl.multiple_of(at, block), block)
        pair_at = iota((1, DH), 1) & (DH // 2 - 1)
        freq = jnp.exp(pair_at.astype(jnp.float32) * (-2.0 * math.log(ROPE_BASE) / DH))
        first = (base + 2 * j + c) * tok_rows
        angle = (row_time(iota((block, DH), 0) + at) + first).astype(jnp.float32) * freq
        cosine[j, rows, :] = jnp.cos(angle)
        turned = jnp.sin(angle)
        sine[j, rows, :] = jnp.where(iota((block, DH), 1) < DH // 2, -turned, turned)
        return carry

    def order(j):
        p = row_time(iota((tok_rows, tok_rows), 0))
        t = iota((tok_rows, tok_rows), 1)
        pick = jnp.where(p == t, 1.0, 0.0).astype(jnp.bfloat16)

        def piece(index, carry):
            at = pl.ds(pl.multiple_of(index * 256, 256), 256)
            tok_turned[j, :, at] = jnp.dot(
                pick, tok_in[j, :, at], preferred_element_type=jnp.float32
            ).astype(jnp.bfloat16)
            return carry

        lax.fori_loop(0, depth // 256, piece, 0)

    def project(j, a, store):
        def piece(index, carry):
            rows = pl.ds(pl.multiple_of(index * block, block), block)
            raw = jnp.dot(tok_turned[j, rows, :], weights[a], preferred_element_type=jnp.float32)
            for g in range(GROUPS):
                part = raw[:, g * DH : (g + 1) * DH]
                if a != 1:
                    part = part * cosine[j, rows, :] + pltpu.roll(part, DH // 2, 1) * sine[j, rows, :]
                store(index, rows, g, part)
            return carry

        lax.fori_loop(0, SECOND_DILATION, piece, 0)

    def keep_pair(j, which):
        def store(index, rows, g, part):
            if g == 2:
                far2[4 + 2 * j + c, which, rows, :] = part.astype(jnp.bfloat16)
            elif g == 1:
                near_own[j, which, rows, :] = part.astype(jnp.bfloat16)
            else:
                pair0[j, which, rows, :] = part.astype(jnp.bfloat16)
                per = tail // THIRD_DILATION
                ends = jnp.concatenate(
                    [part[b * sub + sub - per : (b + 1) * sub] for b in range(4)], axis=0
                )
                at = pl.ds(pl.multiple_of(tok_rows + index * 4 * per, 4 * per), 4 * per)
                near_own[j, which, at, :] = ends.astype(jnp.bfloat16)

        return store

    def keep_query(j):
        def store(index, rows, g, part):
            queries[j, g, rows, :] = part.astype(jnp.bfloat16)

        return store

    def others(a):
        for zz in range(nz):
            s = 2 * zz + 1 - c
            send(chunk(a, s), chunk(a, s), side_s.at[a, 0], w_r.at[a, s], side).wait_recv()

    def far(kind, src, dst, where):
        return send(far2.at[src], far2.at[dst], far_s.at[kind], far_r.at[dst], where)

    def far_side(j):
        return far(j, 4 + 2 * j + c, 4 + 2 * j + c, side)

    def far_up(j):
        return far(2 + j, 4 + 2 * j + c, 2 * j + c, above)

    def far_pass(j):
        return far(4 + j, 2 * j + c, 2 * j + c, side)

    def near(j, dst, where):
        return send(near_own.at[j], near_in.at[dst], near_s.at[j], near_r.at[dst], where)

    up_other = (sp + 2, 2 * x)

    def halos(j):
        @pl.when((c == 1) & (j == 1) & (z == 1))
        def _():
            near(1, 0, up_other).start()

        pl.when(z == 1)(lambda: far_up(j).start())
        pl.when(c == 0)(lambda: near(j, j, side).start())
        pl.when((c == 1) & (j == 0))(lambda: near(0, 1, side).start())
        pl.when((c == 0) | (j == 0))(lambda: far_side(j).start())

    scale = DH ** (-0.5)
    far_off = 1 << 24

    def dots(q, k):
        return lax.dot_general(q, k, (((1,), (1,)), ((), ())), preferred_element_type=jnp.float32)

    def soft(scores, time_q, time_k, reach, first):
        gap = time_q - jnp.where(time_k >= first, time_k, far_off)
        scores = jnp.where((gap >= 0) & (gap <= reach), scores * scale, -jnp.inf)
        top = jnp.max(scores, axis=-1, keepdims=True)
        weight = jnp.exp(scores - top)
        return top, jnp.sum(weight, axis=-1, keepdims=True), weight.astype(jnp.bfloat16)

    def near_groups(j):
        rank = base + 2 * j + c

        def piece(index, carry):
            begin = index * block
            rows = pl.ds(pl.multiple_of(begin, block), block)
            q = queries[j, 0, rows, :]
            tails = pl.ds(tok_rows, tail)
            scores = jnp.concatenate([dots(q, near_in[j, 0, tails, :]), dots(q, pair0[j, 0])], axis=1)
            lane = iota((1, tail + tok_rows), 1)
            time_k = jnp.where(lane < tail, tail_time(lane & (tail - 1)), row_time(lane - tail))
            time_q = row_time(iota((block, 1), 0) + begin)
            top0, sum0, weight = soft(scores, time_q, time_k, WIN1, -rank * tok_rows)
            got0 = jnp.dot(weight[:, :tail], near_in[j, 1, tails, :], preferred_element_type=jnp.float32)
            got0 += jnp.dot(weight[:, tail:], pair0[j, 1], preferred_element_type=jnp.float32)
            q = queries[j, 1, rows, :]
            scores = jnp.concatenate(
                [dots(q, near_in[j, 0, rows, :]), dots(q, near_own[j, 0, rows, :])], axis=1
            )

            def step_of(place):
                return 4 * (place & (sub - 1)) + (place >> sub_log)

            lane = iota((1, 2 * block), 1)
            step_k = step_of(lane & (block - 1)) + jnp.where(lane < block, -block, 0)
            top1, sum1, weight = soft(
                scores, step_of(iota((block, 1), 0)), step_k, WIN2 // SECOND_DILATION, -rank * block
            )
            got1 = jnp.dot(weight[:, :block], near_in[j, 1, rows, :], preferred_element_type=jnp.float32)
            got1 += jnp.dot(weight[:, block:], near_own[j, 1, rows, :], preferred_element_type=jnp.float32)
            top = jnp.maximum(top0, top1)
            f0, f1 = jnp.exp(top0 - top), jnp.exp(top1 - top)
            got01[j, rows, :] = f0 * got0 + f1 * got1
            top01[j, rows, :] = top
            sum01[j, rows, :] = f0 * sum0 + f1 * sum1
            return carry

        lax.fori_loop(0, SECOND_DILATION, piece, 0)

    def far_group(j):
        rank = base + 2 * j + c
        slots = [4 + 2 * j + c - d for d in (4, 3, 2, 1, 0)]

        def piece(index, carry):
            begin = index * block
            rows = pl.ds(pl.multiple_of(begin, block), block)
            all_scores = []
            for b in range(4):
                here = pl.ds(pl.multiple_of(begin + b * sub, sub), sub)
                keys = jnp.concatenate([far2[s, 0, here, :] for s in slots], axis=0)
                all_scores.append(dots(queries[j, 2, here, :], keys))
            scores = jnp.concatenate(all_scores, axis=0)
            step_q = iota((block, 1), 0) & (sub - 1)
            step_k = iota((1, 5 * sub), 1) - 4 * sub
            top2, sum2, weight = soft(scores, step_q, step_k, WIN3 // THIRD_DILATION, -rank * sub)
            got = []
            for b in range(4):
                here = pl.ds(pl.multiple_of(begin + b * sub, sub), sub)
                vals = jnp.concatenate([far2[s, 1, here, :] for s in slots], axis=0)
                got.append(
                    jnp.dot(weight[b * sub : (b + 1) * sub], vals, preferred_element_type=jnp.float32)
                )
            got2 = jnp.concatenate(got, axis=0)
            top1 = top01[j, rows, :]
            top = jnp.maximum(top1, top2)
            f1, f2 = jnp.exp(top1 - top), jnp.exp(top2 - top)
            total = f1 * sum01[j, rows, :] + f2 * sum2
            mine[2, rows, :] = ((f1 * got01[j, rows, :] + f2 * got2) / total).astype(jnp.bfloat16)
            return carry

        lax.fori_loop(0, SECOND_DILATION, piece, 0)
        t = iota((tok_rows, tok_rows), 0)
        p = row_time(iota((tok_rows, tok_rows), 1))
        mine[j] = jnp.dot(
            jnp.where(p == t, 1.0, 0.0).astype(jnp.bfloat16), mine[2], preferred_element_type=jnp.float32
        ).astype(jnp.bfloat16)

    head = 2 * x + y
    quarter = tok_rows // 4

    def deal(j, k):
        return send(
            mine.at[j, pl.ds(k * quarter, quarter), :], heads_in.at[head], head_s.at[j, k], head_r.at[head],
            (base + 2 * j + c, k),
        )

    def deal_self(j, k):
        return pltpu.make_async_copy(mine.at[j, pl.ds(k * quarter, quarter), :], heads_in.at[head], head_r.at[head])

    def self_here(j, k):
        return (j == j_own) & stays & (tp == k)

    def deal_all(j):
        for k in range(4):
            pl.when(self_here(j, k))(lambda k=k: deal_self(j, k).start())
            pl.when(jnp.logical_not(self_here(j, k)))(lambda k=k: deal(j, k).start())

    @pl.when(is_mid)
    def _():
        @pl.when(stays)
        def _():
            kept(0).wait()
            w_cross(0, 0).start()
            w_side(0, 0).start()
            tok_kept().wait()
            for q in range(pieces):
                t_y(j_own, q).start()

        pl.when(moves)(rest_swapped)
        o_relay(1)
        lax.fori_loop(0, 2 * SECOND_DILATION, angles, 0)

        @pl.when(moves)
        def _():
            arrived(0, z)
            w_cross(0, 0).start()
            w_side(0, 0).start()

        def relay_end(a):
            arrived(a, end)
            w_cross(a, 1).start()
            w_side(a, 1).start()

        def relay_side(a, which):
            arrived(a, ring[which])
            w_side(a, which).start()

        def own_on(a):
            own_ready(a)
            w_cross(a, 0).start()
            w_side(a, 0).start()

        def far_on_stays(q):
            put_t(j_far, x, q, tz_s.at[q], to_hub).wait_recv()
            t_x(j_far, q).start()
            t_y(j_far, q).start()

        def on_moves(j, q):
            t_y(j, q).wait_recv()
            t_x(j, q).start()

        def advance(stay_list, move_list):
            @pl.when(stays)
            def _():
                for q in stay_list:
                    far_on_stays(q)

            @pl.when(moves)
            def _():
                for j, q in move_list:
                    on_moves(j, q)

        relay_end(0)
        own_on(1)
        o_relay(2)
        o_relay(3)
        o_share(0).start()
        advance([0], [(j_own, 0)])
        own_on(2)
        relay_side(0, 2)
        relay_side(0, 3)
        advance([], [(j_own, 1)])
        relay_end(1)
        o_share(0).wait()
        o_share(1).start()
        advance([1], [(j_own, 2), (j_own, 3)])
        relay_end(2)
        relay_side(1, 2)
        pl.when(moves)(lambda: t_other(j_own))
        order(j_own)
        others(0)
        project(j_own, 0, keep_pair(j_own, 0))
        advance([2], [(j_far, 0), (j_far, 1)])
        relay_side(2, 2)
        relay_side(1, 3)
        others(1)
        project(j_own, 1, keep_pair(j_own, 1))
        halos(j_own)
        advance([3], [(j_far, 2), (j_far, 3)])
        relay_side(2, 3)
        o_share(1).wait()
        o_share(2).start()

        @pl.when(z == 1)
        def _():
            for s in range(4):
                far2[s] = jnp.zeros(far2.shape[1:], far2.dtype)

        @pl.when((z == 1) & (c == 0))
        def _():
            near_in[0] = jnp.zeros(near_in.shape[1:], near_in.dtype)

        t_other(j_far)
        order(j_far)
        project(j_far, 0, keep_pair(j_far, 0))
        project(j_far, 1, keep_pair(j_far, 1))
        halos(j_far)
        others(2)
        project(j_own, 2, keep_query(j_own))

        @pl.when(z == 2)
        def _():
            far_up(1).wait_recv()
            far_pass(1).start()

        project(j_far, 2, keep_query(j_far))
        pl.when((z == 2) | (c == 1))(lambda: near(0, 0, side).wait_recv())
        near(1, 1, side).wait_recv()
        near_groups(0)
        near_groups(1)
        for j in range(2):
            pl.when((c == 1) | (j == 0))(lambda j=j: far(j, 4, 5 - c + 2 * j, side).wait_recv())

        @pl.when(z == 2)
        def _():
            far(4, 0, 3 - c, side).wait_recv()

        far_group(1)
        deal_all(1)

        @pl.when(z == 2)
        def _():
            far_up(0).wait_recv()
            pl.when(c == 1)(lambda: far_pass(0).start())
            pl.when(c == 0)(lambda: far(4, 0, 1, side).wait_recv())

        far_group(0)
        deal_all(0)

    o_share(2).wait()
    for h in range(4):
        pltpu.make_async_copy(heads_in.at[h], heads_in.at[h], head_r.at[h]).wait()
    for zz in range(nz):
        for yy in range(2):
            acc = None
            for h in range(4):
                one = jnp.dot(heads_in[h], out_rows[h % 2, yy, h // 2, zz], preferred_element_type=jnp.float32)
                acc = one if acc is None else acc + one
            width = w_out.shape[1]
            s = 2 * zz + yy
            out[:, s * width : (s + 1) * width] = acc.astype(jnp.bfloat16)

    @pl.when(moves)
    def _():
        for a in range(3):
            swapped(a).wait_send()

    for zz in range(nz):
        pl.when(has_up & (zz <= z))(lambda zz=zz: o_go(zz, "up").wait_send())
        pl.when(has_down & (zz >= z))(lambda zz=zz: o_go(zz, "down").wait_send())

    @pl.when(is_end)
    def _():
        for a in range(3):
            w_inward(a).wait_send()

        @pl.when(stays)
        def _():
            for q in range(pieces):
                t_inward(q).wait_send()

    @pl.when(is_mid)
    def _():
        for a in range(3):
            for which in range(2):
                w_cross(a, which).wait_send()
            for which in range(4):
                w_side(a, which).wait_send()
        for q in range(pieces):
            t_x(j_far, q).wait_send()

            @pl.when(stays)
            def _(q=q):
                t_y(j_own, q).wait_send()
                t_y(j_far, q).wait_send()

            pl.when(moves)(lambda q=q: t_x(j_own, q).wait_send())
        for j in range(2):
            pl.when(z == 1)(lambda j=j: far_up(j).wait_send())
            pl.when((c == 0) | (j == 0))(lambda j=j: far_side(j).wait_send())
            pl.when((c == 0) | (j == 0) | (z == 1))(lambda j=j: near(j, j, side).wait_send())
            pl.when((z == 2) & ((c == 1) | (j == 1)))(lambda j=j: far_pass(j).wait_send())
            for k in range(4):
                pl.when(jnp.logical_not(self_here(j, k)))(lambda j=j, k=k: deal(j, k).wait_send())


def fits_kernel(n_sp, n_tp, tokens, w_query, w_out):
    tok_rows, depth = tokens.shape
    return (
        n_sp == 2 * LAYERS
        and n_tp == 4
        and w_query.shape[1] == GROUPS * DH
        and w_out.shape[0] == DH
        and w_out.shape[1] % 128 == 0
        and w_query.shape[0] % 16 == 0
        and tok_rows == WIN2
        and 4 * tok_rows == WIN3
        and 4 * WIN1 == tok_rows
    )


def one_kernel(n_sp, tokens, w_query, w_key, w_value, w_out):
    nz = n_sp // 2
    tok_rows, depth = tokens.shape
    cols = w_query.shape[1]
    bf, dma = jnp.bfloat16, pltpu.SemaphoreType.DMA
    return pl.pallas_call(
        functools.partial(layer_kernel, nz),
        out_shape=jax.ShapeDtypeStruct((tok_rows // 4, w_out.shape[1] * n_sp), bf),
        in_specs=[pl.BlockSpec(memory_space=pltpu.HBM)] * 5,
        out_specs=pl.BlockSpec(memory_space=pltpu.VMEM),
        scratch_shapes=[
            pltpu.VMEM((3, depth, cols), bf),
            pltpu.VMEM((3, *w_query.shape), bf),
            pltpu.VMEM((2, tok_rows, depth), bf),
            pltpu.VMEM((2, tok_rows, depth), bf),
            pltpu.VMEM((2, tok_rows, DH), jnp.float32),
            pltpu.VMEM((2, tok_rows, DH), jnp.float32),
            pltpu.VMEM((2, GROUPS, tok_rows, DH), bf),
            pltpu.VMEM((2, 2, tok_rows, DH), bf),
            pltpu.VMEM((2, 2, tok_rows + WIN1, DH), bf),
            pltpu.VMEM((2, 2, tok_rows + WIN1, DH), bf),
            pltpu.VMEM((8, 2, tok_rows, DH), bf),
            pltpu.VMEM((2, 2, 2, nz, *w_out.shape), bf),
            pltpu.VMEM((3, tok_rows, DH), bf),
            pltpu.VMEM((4, tok_rows // 4, DH), bf),
            pltpu.VMEM((2, tok_rows, DH), jnp.float32),
            pltpu.VMEM((2, tok_rows, 1), jnp.float32),
            pltpu.VMEM((2, tok_rows, 1), jnp.float32),
            dma((3,)), dma((3,)), dma, dma((3, n_sp)), dma((3, 2)), dma((3, 4)),
            dma((2, 2, TOKEN_PIECES)), dma((TOKEN_PIECES,)), dma((2, TOKEN_PIECES)), dma((2, TOKEN_PIECES)),
            dma((nz,)), dma((nz,)), dma((nz,)), dma((3,)), dma((3,)),
            dma((6,)), dma((8,)), dma((2,)), dma((2,)), dma((2, 4)), dma((4,)),
        ],
        compiler_params=pltpu.CompilerParams(
            collective_id=0, has_side_effects=True, vmem_limit_bytes=60 * 1024 * 1024
        ),
    )(tokens, w_key, w_value, w_query, w_out)


def on_mesh(n_sp, n_tp, *operands):
    tokens, w_query, _, _, w_out = operands
    if fits_kernel(n_sp, n_tp, tokens, w_query, w_out):
        return one_kernel(n_sp, *operands)
    return on_device(*operands)


def solution(mesh):
    placed = (P("sp", None), P("sp", "tp"), P("sp", "tp"), P("sp", "tp"), P("tp", "sp"))
    body = functools.partial(on_mesh, mesh.shape["sp"], mesh.shape["tp"])
    return jax.shard_map(
        body, mesh=mesh, in_specs=placed, out_specs=P(("sp", "tp"), None), check_vma=False
    )
```

```python
import functools
import math

import jax
import jax.numpy as jnp
from jax import lax
from jax.experimental import pallas as pl
from jax.experimental.pallas import tpu as pltpu
from jax.sharding import PartitionSpec as P

GROUPS = 3
DH = 128
WIN1 = 128
WIN2 = 512
WIN3 = 2048
SECOND_DILATION = 4
THIRD_DILATION = 16


ROPE_BASE = 500000.0

LAYERS = 4


def from_behind(block, axis, distance):
    devices = range(lax.axis_size(axis))
    route = [(i - distance, i) for i in devices if i - distance in devices]
    return lax.ppermute(block, axis, route)


def rotate(projected, offset):
    tok_rows = projected.shape[0]
    head_size = projected.shape[-1]
    half_size = head_size // 2
    positions = (offset + jnp.arange(tok_rows, dtype=jnp.int32)).astype(jnp.float32)
    frequency = 1.0 / ROPE_BASE ** (jnp.arange(0, head_size, 2, dtype=jnp.float32) / head_size)
    angles = (positions[:, None] * frequency[None, :]).reshape(tok_rows, 1, 1, half_size)
    cosine = jnp.cos(angles)
    sine_part = jnp.sin(angles)
    first_half = projected[..., :half_size]
    second_half = projected[..., half_size:]
    return jnp.concatenate(
        [
            first_half * cosine - second_half * sine_part,
            second_half * cosine + first_half * sine_part,
        ],
        axis=-1,
    )


def window_attend(query_part, buffer, steps, stride, offset):
    tok_rows, heads_here, head_size = query_part.shape
    sub_rows = tok_rows // stride
    key_rows = buffer.shape[1] // stride
    query_sub = query_part.reshape(sub_rows, stride, heads_here, head_size).transpose(1, 2, 0, 3)
    pair_sub = buffer.reshape(2, key_rows, stride, heads_here, head_size).transpose(0, 2, 3, 1, 4)
    block_rows = math.gcd(sub_rows, steps) if sub_rows > steps else sub_rows
    block_list = sub_rows // block_rows
    query_blocks = query_sub.reshape(stride, heads_here, block_list, block_rows, head_size)
    key_blocks = jnp.stack(
        [
            pair_sub[:, :, :, index * block_rows : index * block_rows + block_rows + steps]
            for index in range(block_list)
        ],
        axis=3,
    )
    scores = jnp.einsum(
        "zhnqe,zhnke->zhnqk", query_blocks, key_blocks[0], preferred_element_type=jnp.float32
    ) * head_size ** (-0.5)
    query_index = (jnp.arange(block_list, dtype=jnp.int32) * block_rows)[
        :, None, None
    ] + jnp.arange(block_rows, dtype=jnp.int32)[None, :, None]
    key_index = (jnp.arange(block_list, dtype=jnp.int32) * block_rows)[:, None, None] + jnp.arange(
        block_rows + steps, dtype=jnp.int32
    )[None, None, :]
    spacing = query_index + steps - key_index
    residue = jnp.arange(stride, dtype=jnp.int32)[:, None, None, None]
    key_position = offset + (key_index[None] - steps) * stride + residue
    allowed = (spacing[None] >= 0) & (spacing[None] <= steps) & (key_position >= 0)
    scores = jnp.where(allowed[:, None], scores, -jnp.inf)
    row_max = jnp.max(scores, axis=-1)
    exponent = jnp.exp(scores - row_max[..., None])
    totals = jnp.sum(exponent, axis=-1)
    probs = (exponent / totals[..., None]).astype(jnp.bfloat16)
    mixed = jnp.einsum(
        "zhnqk,zhnke->zhnqe", probs, key_blocks[1], preferred_element_type=jnp.float32
    )
    mixed = mixed.reshape(stride, heads_here, sub_rows, head_size).transpose(2, 0, 1, 3)
    log_total = (row_max + jnp.log(totals)).reshape(stride, heads_here, sub_rows).transpose(2, 0, 1)
    return (mixed.reshape(tok_rows, heads_here, head_size), log_total.reshape(tok_rows, heads_here))


def reach_back(key_value, distance_max):
    tok_rows = key_value.shape[1]
    gathered = key_value
    pieces_held = 1
    while pieces_held < distance_max + 1:
        slice_share = min(pieces_held, distance_max + 1 - pieces_held)
        arrived = from_behind(
            gathered[:, gathered.shape[1] - slice_share * tok_rows :], "sp", pieces_held
        )
        gathered = jnp.concatenate([arrived, gathered], axis=1)
        pieces_held = pieces_held + slice_share
    return gathered


def on_device(tokens, w_query, w_key, w_value, w_out):
    tok_rows = tokens.shape[0]
    heads_here = w_out.shape[0] // DH
    offset = lax.axis_index("sp") * tok_rows
    weight_parts = (
        lax.all_gather(w_query, "sp", axis=0, tiled=True),
        lax.all_gather(w_key, "sp", axis=0, tiled=True),
        lax.all_gather(w_value, "sp", axis=0, tiled=True),
    )
    query_raw, key_raw, value_raw = tuple(
        (
            jnp.dot(tokens, weight_rows, preferred_element_type=jnp.float32)
            for weight_rows in weight_parts
        )
    )
    head_shape = (tok_rows, heads_here, GROUPS, DH)
    queries = rotate(query_raw.reshape(head_shape), offset).astype(jnp.bfloat16)
    keys_all = rotate(key_raw.reshape(head_shape), offset).astype(jnp.bfloat16)
    values_all = value_raw.astype(jnp.bfloat16).reshape(head_shape)
    windows = (WIN1, WIN2, WIN3)
    step_sizes = (1, SECOND_DILATION, THIRD_DILATION)
    outputs = []
    log_totals = []
    for group_index in range(GROUPS):
        key_value = jnp.stack([keys_all[:, :, group_index], values_all[:, :, group_index]])
        key_value = key_value.reshape(2, tok_rows, heads_here * DH)
        window = windows[group_index]
        if group_index == 0:
            near_rows = from_behind(key_value[:, tok_rows - window :], "sp", 1)
            buffer = jnp.concatenate([near_rows, key_value], axis=1)
        else:
            distance_max = (window + tok_rows - 1) // tok_rows
            buffer = reach_back(key_value, distance_max)
        group_out, log_total = window_attend(
            queries[:, :, group_index],
            buffer,
            window // step_sizes[group_index],
            step_sizes[group_index],
            offset,
        )
        outputs.append(group_out)
        log_totals.append(log_total)
    group_weights = jax.nn.softmax(jnp.stack(log_totals), axis=0)
    merged = jnp.sum(group_weights[..., None] * jnp.stack(outputs), axis=0).astype(jnp.bfloat16)
    merged = merged.reshape(tok_rows, heads_here * DH)
    w_whole = lax.all_gather(w_out, "sp", axis=1, tiled=True)
    return lax.psum_scatter(
        jnp.dot(merged, w_whole, preferred_element_type=jnp.float32).astype(jnp.bfloat16),
        "tp",
        scatter_dimension=0,
        tiled=True,
    )


def layer_kernel(
    nz,
    tokens, w_key, w_value, w_query, w_out, out,
    weights, stage, tok_in, tok_turned, cosine, sine, queries, pair0, near_own, near_in, far2,
    out_rows, mine, heads_in, got01, top01, sum01,
    stage_s, swap_s, tok_r, w_r, up_s, down_s, side_s, o_r, o_s, o_r2, far_s, far_r, near_s, near_r, head_s, head_r,
):
    tok_rows, depth = tokens.shape
    k_rows, cols = w_key.shape
    sub = tok_rows // THIRD_DILATION
    sub_log = sub.bit_length() - 1
    block = tok_rows // SECOND_DILATION
    tail = WIN1
    last = nz - 1
    sp, tp = lax.axis_index("sp"), lax.axis_index("tp")
    z, y = sp // 2, sp % 2
    x, c = tp // 2, tp % 2
    rank = 2 * z + c
    stays = c == y
    moves = jnp.logical_not(stays)
    has_up, has_down = z < last, z > 0
    side = (sp, 2 * x + 1 - c)
    across_x = (sp, 2 * (1 - x) + c)
    across_y = (2 * z + 1 - y, tp)
    partner = (2 * z + 1 - y, 2 * x + 1 - c)
    above, below = (sp + 2, tp), (sp - 2, tp)
    up_other = (sp + 2, 2 * x)

    def send(src, dst, s_sem, r_sem, where):
        return pltpu.make_async_remote_copy(
            src_ref=src, dst_ref=dst, send_sem=s_sem, recv_sem=r_sem,
            device_id=where, device_id_type=pl.DeviceIdType.MESH,
        )

    parts = (w_key, w_value, w_query)
    upward, downward = (2, 0, 1), (0, 1, 2)

    def chunk(a, s):
        return weights.at[a, pl.ds(pl.multiple_of(s * k_rows, k_rows), k_rows), :]

    def o_chunk(zz):
        return out_rows.at[c, y, x, zz]

    def kept(a):
        return pltpu.make_async_copy(parts[a], chunk(a, rank), w_r.at[a, rank])

    def staged(a):
        return pltpu.make_async_copy(parts[a], stage.at[a], stage_s.at[a])

    def swapped(a):
        there = 2 * z + 1 - c
        return send(stage.at[a], chunk(a, there), swap_s.at[a], w_r.at[a, there], partner)

    def tok_kept():
        return pltpu.make_async_copy(tokens, tok_in, tok_r)

    def tok_swapped():
        return send(tokens, tok_in, swap_s.at[3], tok_r, partner)

    def o_kept():
        return pltpu.make_async_copy(w_out, o_chunk(z), o_r.at[z])

    o_kept().start()

    @pl.when(stays)
    def _():
        for a in (2, 0, 1):
            kept(a).start()
        tok_kept().start()

    @pl.when(moves)
    def _():
        for a in (2, 0, 1):
            staged(a).start()

    barrier = pltpu.get_barrier_semaphore()

    def greet(where):
        pl.semaphore_signal(barrier, inc=1, device_id=where, device_id_type=pl.DeviceIdType.MESH)

    for dy in range(2):
        for dx in range(2):
            for dc in range(2):
                if dy + dx + dc:
                    greet((2 * z + (y + dy) % 2, 2 * ((x + dx) % 2) + (c + dc) % 2))
    pl.when(has_up)(lambda: greet(above))
    pl.when(has_down)(lambda: greet(below))
    pl.when(has_up & (c == 1))(lambda: greet(up_other))
    pl.when(has_down & (c == 0))(lambda: greet((sp - 2, 2 * x + 1)))
    pl.semaphore_wait(barrier, 7 + jnp.where(has_up, 1 + c, 0) + jnp.where(has_down, 2 - c, 0))

    def go(a, zz, kind):
        s = 2 * zz + c
        ref = chunk(a, s) if a < 3 else o_chunk(zz)
        r_sem = w_r.at[a, s] if a < 3 else o_r.at[zz]
        s_sem = {"up": up_s, "down": down_s, "side": side_s}[kind].at[a, zz]
        return send(ref, ref, s_sem, r_sem, {"up": above, "down": below, "side": side}[kind])

    def swap_order(layer):
        return {0: (2, 0, 1), last: (0, 1, 2)}.get(layer, (0, 2, 1))

    @pl.when(moves)
    def _():
        for layer in range(nz):
            @pl.when(z == layer)
            def _(layer=layer):
                for a in swap_order(layer):
                    staged(a).wait()
                    swapped(a).start()
        tok_swapped().start()

    def o_relay(layer, d):
        if layer - d >= 0:
            go(3, layer - d, "up").wait_recv()
            if layer < last:
                go(3, layer - d, "up").start()
        if layer + d < nz:
            go(3, layer + d, "down").wait_recv()
            if layer > 0:
                go(3, layer + d, "down").start()

    def o_share(axis):
        ref, where = (
            (out_rows.at[c, y, x], across_x),
            (out_rows.at[c, y], across_y),
            (out_rows.at[c], side),
        )[axis]
        return send(ref, ref, o_s.at[axis], o_r2.at[axis], where)

    def events(layer):
        listed = []
        for i in range(3):
            for d in range(1, layer + 1):
                listed.append((i * layer + d, "up", upward[i], layer - d, d))
            for d in range(1, last - layer + 1):
                listed.append((i * (last - layer) + d, "down", downward[i], layer + d, d))
        return sorted(listed)

    def handle(layer, event):
        _, kind, a, zz, d = event
        go(a, zz, kind).wait_recv()
        if kind == "up":
            if layer < last:
                go(a, zz, "up").start()
            if d == layer and a == upward[0] and layer < last:
                go(upward[2], layer, "up").start()
        else:
            if layer > 0:
                go(a, zz, "down").start()
            if d == last - layer and a == downward[0] and layer > 0:
                go(downward[2], layer, "down").start()
        go(a, zz, "side").start()

    def begin(layer):
        o_kept().wait()
        if layer < last:
            go(3, layer, "up").start()
        if layer > 0:
            go(3, layer, "down").start()
        for a in swap_order(layer):
            pl.when(stays)(lambda a=a: kept(a).wait())
            pl.when(moves)(lambda a=a: go(a, layer, "side").wait_recv())
            if layer < last and (layer == 0 or a != upward[2]):
                go(a, layer, "up").start()
            if layer > 0 and (layer == last or a != downward[2]):
                go(a, layer, "down").start()
            go(a, layer, "side").start()

    def row_time(p):
        b, i = p >> sub_log, p & (sub - 1)
        return THIRD_DILATION * i + (b >> 2) + SECOND_DILATION * (b & 3)

    def tail_time(u):
        per = tail // THIRD_DILATION
        b, i = u >> (per.bit_length() - 1), u & (per - 1)
        return THIRD_DILATION * (sub - per + i) + (b >> 2) + SECOND_DILATION * (b & 3) - tok_rows

    def iota(shape, axis):
        return lax.broadcasted_iota(jnp.int32, shape, axis)

    def angles(index, carry):
        at = index * block
        rows = pl.ds(pl.multiple_of(at, block), block)
        pair_at = iota((1, DH), 1) & (DH // 2 - 1)
        freq = jnp.exp(pair_at.astype(jnp.float32) * (-2.0 * math.log(ROPE_BASE) / DH))
        angle = (row_time(iota((block, DH), 0) + at) + rank * tok_rows).astype(jnp.float32) * freq
        cosine[rows, :] = jnp.cos(angle)
        turned = jnp.sin(angle)
        sine[rows, :] = jnp.where(iota((block, DH), 1) < DH // 2, -turned, turned)
        return carry

    def order():
        p = row_time(iota((tok_rows, tok_rows), 0))
        t = iota((tok_rows, tok_rows), 1)
        pick = jnp.where(p == t, 1.0, 0.0).astype(jnp.bfloat16)

        def piece(index, carry):
            at = pl.ds(pl.multiple_of(index * 256, 256), 256)
            tok_turned[:, at] = jnp.dot(
                pick, tok_in[:, at], preferred_element_type=jnp.float32
            ).astype(jnp.bfloat16)
            return carry

        lax.fori_loop(0, depth // 256, piece, 0)

    def project(a, store):
        def piece(index, carry):
            rows = pl.ds(pl.multiple_of(index * block, block), block)
            raw = jnp.dot(tok_turned[rows, :], weights[a], preferred_element_type=jnp.float32)
            for g in range(GROUPS):
                part = raw[:, g * DH : (g + 1) * DH]
                if a != 1:
                    part = part * cosine[rows, :] + pltpu.roll(part, DH // 2, 1) * sine[rows, :]
                store(index, rows, g, part)
            return carry

        lax.fori_loop(0, SECOND_DILATION, piece, 0)

    def keep_pair(which):
        def store(index, rows, g, part):
            if g == 2:
                far2[4 + c, which, rows, :] = part.astype(jnp.bfloat16)
            elif g == 1:
                near_own[which, rows, :] = part.astype(jnp.bfloat16)
            else:
                pair0[which, rows, :] = part.astype(jnp.bfloat16)
                per = tail // THIRD_DILATION
                ends = jnp.concatenate(
                    [part[b * sub + sub - per : (b + 1) * sub] for b in range(4)], axis=0
                )
                at = pl.ds(pl.multiple_of(tok_rows + index * 4 * per, 4 * per), 4 * per)
                near_own[which, at, :] = ends.astype(jnp.bfloat16)

        return store

    def keep_query(index, rows, g, part):
        queries[g, rows, :] = part.astype(jnp.bfloat16)

    def others(a):
        for zz in range(nz):
            s = 2 * zz + 1 - c
            send(chunk(a, s), chunk(a, s), side_s.at[a, zz], w_r.at[a, s], side).wait_recv()

    def far(kind, src, dst, where):
        return send(far2.at[src], far2.at[dst], far_s.at[kind], far_r.at[dst], where)

    def own_side():
        return far(0, 4 + c, 4 + c, side)

    def own_up():
        return far(1, 4 + c, 2 + c, above)

    def pass_side(kind, slot):
        return far(kind, slot, slot, side)

    def pass_up():
        return far(3, 2 + c, c, above)

    def near(where):
        return send(near_own, near_in, near_s, near_r, where)

    def halos():
        pl.when(has_up & (c == 1))(lambda: near(up_other).start())
        pl.when(has_up)(lambda: own_up().start())
        pl.when(c == 0)(lambda: near(side).start())
        pl.when(c == 0)(lambda: own_side().start())

    scale = DH ** (-0.5)
    far_off = 1 << 24

    def dots(q, k):
        return lax.dot_general(q, k, (((1,), (1,)), ((), ())), preferred_element_type=jnp.float32)

    def soft(scores, time_q, time_k, reach, first):
        gap = time_q - jnp.where(time_k >= first, time_k, far_off)
        scores = jnp.where((gap >= 0) & (gap <= reach), scores * scale, -jnp.inf)
        top = jnp.max(scores, axis=-1, keepdims=True)
        weight = jnp.exp(scores - top)
        return top, jnp.sum(weight, axis=-1, keepdims=True), weight.astype(jnp.bfloat16)

    def near_groups():
        def piece(index, carry):
            begin = index * block
            rows = pl.ds(pl.multiple_of(begin, block), block)
            q = queries[0, rows, :]
            tails = pl.ds(tok_rows, tail)
            scores = jnp.concatenate([dots(q, near_in[0, tails, :]), dots(q, pair0[0])], axis=1)
            lane = iota((1, tail + tok_rows), 1)
            time_k = jnp.where(lane < tail, tail_time(lane & (tail - 1)), row_time(lane - tail))
            time_q = row_time(iota((block, 1), 0) + begin)
            top0, sum0, weight = soft(scores, time_q, time_k, WIN1, -rank * tok_rows)
            got0 = jnp.dot(weight[:, :tail], near_in[1, tails, :], preferred_element_type=jnp.float32)
            got0 += jnp.dot(weight[:, tail:], pair0[1], preferred_element_type=jnp.float32)
            q = queries[1, rows, :]
            scores = jnp.concatenate(
                [dots(q, near_in[0, rows, :]), dots(q, near_own[0, rows, :])], axis=1
            )

            def step_of(place):
                return 4 * (place & (sub - 1)) + (place >> sub_log)

            lane = iota((1, 2 * block), 1)
            step_k = step_of(lane & (block - 1)) + jnp.where(lane < block, -block, 0)
            top1, sum1, weight = soft(
                scores, step_of(iota((block, 1), 0)), step_k, WIN2 // SECOND_DILATION, -rank * block
            )
            got1 = jnp.dot(weight[:, :block], near_in[1, rows, :], preferred_element_type=jnp.float32)
            got1 += jnp.dot(weight[:, block:], near_own[1, rows, :], preferred_element_type=jnp.float32)
            top = jnp.maximum(top0, top1)
            f0, f1 = jnp.exp(top0 - top), jnp.exp(top1 - top)
            got01[rows, :] = f0 * got0 + f1 * got1
            top01[rows, :] = top
            sum01[rows, :] = f0 * sum0 + f1 * sum1
            return carry

        lax.fori_loop(0, SECOND_DILATION, piece, 0)

    def far_group():
        slots = [4 + c - d for d in (4, 3, 2, 1, 0)]

        def piece(index, carry):
            begin = index * block
            rows = pl.ds(pl.multiple_of(begin, block), block)
            all_scores = []
            for b in range(4):
                here = pl.ds(pl.multiple_of(begin + b * sub, sub), sub)
                keys = jnp.concatenate([far2[s, 0, here, :] for s in slots], axis=0)
                all_scores.append(dots(queries[2, here, :], keys))
            scores = jnp.concatenate(all_scores, axis=0)
            step_q = iota((block, 1), 0) & (sub - 1)
            step_k = iota((1, 5 * sub), 1) - 4 * sub
            top2, sum2, weight = soft(scores, step_q, step_k, WIN3 // THIRD_DILATION, -rank * sub)
            got = []
            for b in range(4):
                here = pl.ds(pl.multiple_of(begin + b * sub, sub), sub)
                vals = jnp.concatenate([far2[s, 1, here, :] for s in slots], axis=0)
                got.append(
                    jnp.dot(weight[b * sub : (b + 1) * sub], vals, preferred_element_type=jnp.float32)
                )
            got2 = jnp.concatenate(got, axis=0)
            top1 = top01[rows, :]
            top = jnp.maximum(top1, top2)
            f1, f2 = jnp.exp(top1 - top), jnp.exp(top2 - top)
            total = f1 * sum01[rows, :] + f2 * sum2
            mine[0, rows, :] = ((f1 * got01[rows, :] + f2 * got2) / total).astype(jnp.bfloat16)
            return carry

        lax.fori_loop(0, SECOND_DILATION, piece, 0)
        t = iota((tok_rows, tok_rows), 0)
        p = row_time(iota((tok_rows, tok_rows), 1))
        mine[1] = jnp.dot(
            jnp.where(p == t, 1.0, 0.0).astype(jnp.bfloat16), mine[0], preferred_element_type=jnp.float32
        ).astype(jnp.bfloat16)

    head = 2 * x + y
    quarter = tok_rows // 4

    def deal(k):
        return send(
            mine.at[1, pl.ds(k * quarter, quarter), :], heads_in.at[head], head_s.at[k], head_r.at[head], (rank, k)
        )

    def deal_self(k):
        return pltpu.make_async_copy(mine.at[1, pl.ds(k * quarter, quarter), :], heads_in.at[head], head_r.at[head])

    def turn_tokens():
        pl.when(stays)(lambda: tok_kept().wait())
        pl.when(moves)(lambda: tok_swapped().wait_recv())
        order()

    def key_value(which):
        others(which)
        project(which, keep_pair(which))

    def query():
        others(2)
        project(2, keep_query)

    def run(layer):
        begin(layer)
        o_relay(layer, 1)
        lax.fori_loop(0, SECOND_DILATION, angles, 0)
        pl.when(stays)(turn_tokens)
        todo = events(layer)
        for event in todo[:3]:
            handle(layer, event)
        o_relay(layer, 2)
        o_relay(layer, 3)
        o_share(0).start()
        split = 9 if layer == 2 else 6 if layer != 1 else 7
        for event in todo[3:split]:
            handle(layer, event)
        late = todo[split:]
        if layer == 1:
            @pl.when(moves)
            def _():
                for event in late:
                    handle(layer, event)

        o_share(0).wait()
        o_share(1).start()
        pl.when(moves)(turn_tokens)
        if layer == last:
            query()
            key_value(0)
        else:
            key_value(0)
            key_value(1)
            halos()
        if layer == 1:
            @pl.when(stays)
            def _():
                for event in late:
                    handle(layer, event)
        else:
            for event in late:
                handle(layer, event)
        if layer == last:
            key_value(1)
            halos()
        else:
            query()

    for layer in range(nz):
        pl.when(z == layer)(functools.partial(run, layer))

    for slot in range(4):
        @pl.when(2 * z + slot < 4)
        def _(slot=slot):
            far2[slot] = jnp.zeros(far2.shape[1:], far2.dtype)

    @pl.when(rank == 0)
    def _():
        near_in[...] = jnp.zeros(near_in.shape, near_in.dtype)

    pl.when(rank >= 1)(lambda: near(side).wait_recv())
    near_groups()
    o_share(1).wait()
    o_share(2).start()

    @pl.when(z >= 1)
    def _():
        own_up().wait_recv()
        pl.when(has_up)(lambda: pass_up().start())
        pass_side(2, 2 + c).start()

    @pl.when(z >= 2)
    def _():
        pass_up().wait_recv()
        pl.when(c == 1)(lambda: pass_side(4, 1).start())
        pl.when(c == 0)(lambda: pass_side(4, 1).wait_recv())

    pl.when(c == 1)(lambda: pass_side(0, 4).wait_recv())
    pl.when(z >= 1)(lambda: pass_side(2, 3 - c).wait_recv())
    far_group()
    for k in range(4):
        self_here = stays & (tp == k)
        pl.when(self_here)(lambda k=k: deal_self(k).start())
        pl.when(jnp.logical_not(self_here))(lambda k=k: deal(k).start())

    o_share(2).wait()
    for h in range(4):
        pltpu.make_async_copy(heads_in.at[h], heads_in.at[h], head_r.at[h]).wait()
    for zz in range(nz):
        for yy in range(2):
            acc = None
            for h in range(4):
                one = jnp.dot(heads_in[h], out_rows[h % 2, yy, h // 2, zz], preferred_element_type=jnp.float32)
                acc = one if acc is None else acc + one
            width = w_out.shape[1]
            s = 2 * zz + yy
            out[:, s * width : (s + 1) * width] = acc.astype(jnp.bfloat16)

    for k in range(4):
        pl.when(jnp.logical_not(stays & (tp == k)))(lambda k=k: deal(k).wait_send())

    @pl.when(moves)
    def _():
        for a in range(3):
            swapped(a).wait_send()
        tok_swapped().wait_send()

    for a in range(4):
        for zz in range(nz):
            pl.when(has_up & (zz <= z))(lambda a=a, zz=zz: go(a, zz, "up").wait_send())
            pl.when(has_down & (zz >= z))(lambda a=a, zz=zz: go(a, zz, "down").wait_send())
            if a < 3:
                go(a, zz, "side").wait_send()
    pl.when((c == 0) | has_up)(lambda: near(side).wait_send())
    pl.when(c == 0)(lambda: own_side().wait_send())
    pl.when(has_up)(lambda: own_up().wait_send())
    pl.when(z >= 1)(lambda: pass_side(2, 2 + c).wait_send())
    pl.when((z >= 1) & has_up)(lambda: pass_up().wait_send())
    pl.when((z >= 2) & (c == 1))(lambda: pass_side(4, 1).wait_send())


def fits_kernel(n_sp, n_tp, tokens, w_query, w_out):
    tok_rows, depth = tokens.shape
    return (
        n_sp == 2 * LAYERS
        and n_tp == 4
        and w_query.shape[1] == GROUPS * DH
        and w_out.shape[0] == DH
        and w_out.shape[1] % 128 == 0
        and w_query.shape[0] % 16 == 0
        and tok_rows == WIN2
        and 4 * tok_rows == WIN3
        and 4 * WIN1 == tok_rows
    )


def one_kernel(n_sp, tokens, w_query, w_key, w_value, w_out):
    nz = n_sp // 2
    tok_rows, depth = tokens.shape
    cols = w_query.shape[1]
    bf, dma = jnp.bfloat16, pltpu.SemaphoreType.DMA
    return pl.pallas_call(
        functools.partial(layer_kernel, nz),
        out_shape=jax.ShapeDtypeStruct((tok_rows // 4, w_out.shape[1] * n_sp), bf),
        in_specs=[pl.BlockSpec(memory_space=pltpu.HBM)] * 5,
        out_specs=pl.BlockSpec(memory_space=pltpu.VMEM),
        scratch_shapes=[
            pltpu.VMEM((3, depth, cols), bf),
            pltpu.VMEM((3, *w_query.shape), bf),
            pltpu.VMEM((tok_rows, depth), bf),
            pltpu.VMEM((tok_rows, depth), bf),
            pltpu.VMEM((tok_rows, DH), jnp.float32),
            pltpu.VMEM((tok_rows, DH), jnp.float32),
            pltpu.VMEM((GROUPS, tok_rows, DH), bf),
            pltpu.VMEM((2, tok_rows, DH), bf),
            pltpu.VMEM((2, tok_rows + WIN1, DH), bf),
            pltpu.VMEM((2, tok_rows + WIN1, DH), bf),
            pltpu.VMEM((6, 2, tok_rows, DH), bf),
            pltpu.VMEM((2, 2, 2, nz, *w_out.shape), bf),
            pltpu.VMEM((2, tok_rows, DH), bf),
            pltpu.VMEM((4, tok_rows // 4, DH), bf),
            pltpu.VMEM((tok_rows, DH), jnp.float32),
            pltpu.VMEM((tok_rows, 1), jnp.float32),
            pltpu.VMEM((tok_rows, 1), jnp.float32),
            dma((3,)), dma((4,)), dma, dma((3, n_sp)), dma((4, nz)), dma((4, nz)), dma((3, nz)),
            dma((nz,)), dma((3,)), dma((3,)),
            dma((5,)), dma((6,)), dma, dma, dma((4,)), dma((4,)),
        ],
        compiler_params=pltpu.CompilerParams(
            collective_id=0, has_side_effects=True, vmem_limit_bytes=60 * 1024 * 1024
        ),
    )(tokens, w_key, w_value, w_query, w_out)


def on_mesh(n_sp, n_tp, *operands):
    tokens, w_query, _, _, w_out = operands
    if fits_kernel(n_sp, n_tp, tokens, w_query, w_out):
        return one_kernel(n_sp, *operands)
    return on_device(*operands)


def solution(mesh):
    placed = (P("sp", None), P("sp", "tp"), P("sp", "tp"), P("sp", "tp"), P("tp", "sp"))
    body = functools.partial(on_mesh, mesh.shape["sp"], mesh.shape["tp"])
    return jax.shard_map(
        body, mesh=mesh, in_specs=placed, out_specs=P(("sp", "tp"), None), check_vma=False
    )
```

```python
import functools
import math

import jax
import jax.numpy as jnp
from jax import lax
from jax.experimental import pallas as pl
from jax.experimental.pallas import tpu as pltpu
from jax.sharding import PartitionSpec as P

GROUPS = 3
DH = 128
WIN1 = 128
WIN2 = 512
WIN3 = 2048
SECOND_DILATION = 4
THIRD_DILATION = 16


ROPE_BASE = 500000.0

LAYERS = 4


def from_behind(block, axis, distance):
    devices = range(lax.axis_size(axis))
    route = [(i - distance, i) for i in devices if i - distance in devices]
    return lax.ppermute(block, axis, route)


def rotate(projected, offset):
    tok_rows = projected.shape[0]
    head_size = projected.shape[-1]
    half_size = head_size // 2
    positions = (offset + jnp.arange(tok_rows, dtype=jnp.int32)).astype(jnp.float32)
    frequency = 1.0 / ROPE_BASE ** (jnp.arange(0, head_size, 2, dtype=jnp.float32) / head_size)
    angles = (positions[:, None] * frequency[None, :]).reshape(tok_rows, 1, 1, half_size)
    cosine = jnp.cos(angles)
    sine_part = jnp.sin(angles)
    first_half = projected[..., :half_size]
    second_half = projected[..., half_size:]
    return jnp.concatenate(
        [
            first_half * cosine - second_half * sine_part,
            second_half * cosine + first_half * sine_part,
        ],
        axis=-1,
    )


def window_attend(query_part, buffer, steps, stride, offset):
    tok_rows, heads_here, head_size = query_part.shape
    sub_rows = tok_rows // stride
    key_rows = buffer.shape[1] // stride
    query_sub = query_part.reshape(sub_rows, stride, heads_here, head_size).transpose(1, 2, 0, 3)
    pair_sub = buffer.reshape(2, key_rows, stride, heads_here, head_size).transpose(0, 2, 3, 1, 4)
    block_rows = math.gcd(sub_rows, steps) if sub_rows > steps else sub_rows
    block_list = sub_rows // block_rows
    query_blocks = query_sub.reshape(stride, heads_here, block_list, block_rows, head_size)
    key_blocks = jnp.stack(
        [
            pair_sub[:, :, :, index * block_rows : index * block_rows + block_rows + steps]
            for index in range(block_list)
        ],
        axis=3,
    )
    scores = jnp.einsum(
        "zhnqe,zhnke->zhnqk", query_blocks, key_blocks[0], preferred_element_type=jnp.float32
    ) * head_size ** (-0.5)
    query_index = (jnp.arange(block_list, dtype=jnp.int32) * block_rows)[
        :, None, None
    ] + jnp.arange(block_rows, dtype=jnp.int32)[None, :, None]
    key_index = (jnp.arange(block_list, dtype=jnp.int32) * block_rows)[:, None, None] + jnp.arange(
        block_rows + steps, dtype=jnp.int32
    )[None, None, :]
    spacing = query_index + steps - key_index
    residue = jnp.arange(stride, dtype=jnp.int32)[:, None, None, None]
    key_position = offset + (key_index[None] - steps) * stride + residue
    allowed = (spacing[None] >= 0) & (spacing[None] <= steps) & (key_position >= 0)
    scores = jnp.where(allowed[:, None], scores, -jnp.inf)
    row_max = jnp.max(scores, axis=-1)
    exponent = jnp.exp(scores - row_max[..., None])
    totals = jnp.sum(exponent, axis=-1)
    probs = (exponent / totals[..., None]).astype(jnp.bfloat16)
    mixed = jnp.einsum(
        "zhnqk,zhnke->zhnqe", probs, key_blocks[1], preferred_element_type=jnp.float32
    )
    mixed = mixed.reshape(stride, heads_here, sub_rows, head_size).transpose(2, 0, 1, 3)
    log_total = (row_max + jnp.log(totals)).reshape(stride, heads_here, sub_rows).transpose(2, 0, 1)
    return (mixed.reshape(tok_rows, heads_here, head_size), log_total.reshape(tok_rows, heads_here))


def reach_back(key_value, distance_max):
    tok_rows = key_value.shape[1]
    gathered = key_value
    pieces_held = 1
    while pieces_held < distance_max + 1:
        slice_share = min(pieces_held, distance_max + 1 - pieces_held)
        arrived = from_behind(
            gathered[:, gathered.shape[1] - slice_share * tok_rows :], "sp", pieces_held
        )
        gathered = jnp.concatenate([arrived, gathered], axis=1)
        pieces_held = pieces_held + slice_share
    return gathered


def on_device(tokens, w_query, w_key, w_value, w_out):
    tok_rows = tokens.shape[0]
    heads_here = w_out.shape[0] // DH
    offset = lax.axis_index("sp") * tok_rows
    weight_parts = (
        lax.all_gather(w_query, "sp", axis=0, tiled=True),
        lax.all_gather(w_key, "sp", axis=0, tiled=True),
        lax.all_gather(w_value, "sp", axis=0, tiled=True),
    )
    query_raw, key_raw, value_raw = tuple(
        (
            jnp.dot(tokens, weight_rows, preferred_element_type=jnp.float32)
            for weight_rows in weight_parts
        )
    )
    head_shape = (tok_rows, heads_here, GROUPS, DH)
    queries = rotate(query_raw.reshape(head_shape), offset).astype(jnp.bfloat16)
    keys_all = rotate(key_raw.reshape(head_shape), offset).astype(jnp.bfloat16)
    values_all = value_raw.astype(jnp.bfloat16).reshape(head_shape)
    windows = (WIN1, WIN2, WIN3)
    step_sizes = (1, SECOND_DILATION, THIRD_DILATION)
    outputs = []
    log_totals = []
    for group_index in range(GROUPS):
        key_value = jnp.stack([keys_all[:, :, group_index], values_all[:, :, group_index]])
        key_value = key_value.reshape(2, tok_rows, heads_here * DH)
        window = windows[group_index]
        if group_index == 0:
            near_rows = from_behind(key_value[:, tok_rows - window :], "sp", 1)
            buffer = jnp.concatenate([near_rows, key_value], axis=1)
        else:
            distance_max = (window + tok_rows - 1) // tok_rows
            buffer = reach_back(key_value, distance_max)
        group_out, log_total = window_attend(
            queries[:, :, group_index],
            buffer,
            window // step_sizes[group_index],
            step_sizes[group_index],
            offset,
        )
        outputs.append(group_out)
        log_totals.append(log_total)
    group_weights = jax.nn.softmax(jnp.stack(log_totals), axis=0)
    merged = jnp.sum(group_weights[..., None] * jnp.stack(outputs), axis=0).astype(jnp.bfloat16)
    merged = merged.reshape(tok_rows, heads_here * DH)
    w_whole = lax.all_gather(w_out, "sp", axis=1, tiled=True)
    return lax.psum_scatter(
        jnp.dot(merged, w_whole, preferred_element_type=jnp.float32).astype(jnp.bfloat16),
        "tp",
        scatter_dimension=0,
        tiled=True,
    )


def layer_kernel(
    nz,
    tokens, w_key, w_value, w_query, w_out, out,
    weights, stage, tok_in, tok_turned, cosine, sine, queries, pair0, near_own, near_in, far2,
    out_rows, mine, heads_in, got01, top01, sum01, asked, part, part_log, got_part, got_log,
    stage_s, swap_s, tok_k, t_r, ty_s, tx_s, w_r, up_s, down_s, side_s, o_r, o_s, o_r2, far_s, far_r, near_s, near_r, head_s, head_r, part_s, part_r,
):
    tok_rows, depth = tokens.shape
    k_rows, cols = w_key.shape
    sub = tok_rows // THIRD_DILATION
    sub_log = sub.bit_length() - 1
    block = tok_rows // SECOND_DILATION
    tail = WIN1
    last = nz - 1
    sp, tp = lax.axis_index("sp"), lax.axis_index("tp")
    z, y = sp // 2, sp % 2
    x, c = tp // 2, tp % 2
    rank = 2 * z + c
    stays = c == y
    moves = jnp.logical_not(stays)
    has_up, has_down = z < last, z > 0
    side = (sp, 2 * x + 1 - c)
    across_x = (sp, 2 * (1 - x) + c)
    across_y = (2 * z + 1 - y, tp)
    partner = (2 * z + 1 - y, 2 * x + 1 - c)
    above, below = (sp + 2, tp), (sp - 2, tp)
    up_other = (sp + 2, 2 * x)

    def send(src, dst, s_sem, r_sem, where):
        return pltpu.make_async_remote_copy(
            src_ref=src, dst_ref=dst, send_sem=s_sem, recv_sem=r_sem,
            device_id=where, device_id_type=pl.DeviceIdType.MESH,
        )

    parts = (w_key, w_value, w_query)
    upward, downward = (2, 0, 1), (0, 1, 2)

    def chunk(a, s):
        return weights.at[a, pl.ds(pl.multiple_of(s * k_rows, k_rows), k_rows), :]

    def o_chunk(zz):
        return out_rows.at[c, y, x, zz]

    def kept(a):
        return pltpu.make_async_copy(parts[a], chunk(a, rank), w_r.at[a, rank])

    def staged(a):
        return pltpu.make_async_copy(parts[a], stage.at[a], stage_s.at[a])

    def swapped(a):
        there = 2 * z + 1 - c
        return send(stage.at[a], chunk(a, there), swap_s.at[a], w_r.at[a, there], partner)

    def tok_kept():
        return pltpu.make_async_copy(tokens, tok_in, tok_k)

    pieces = ty_s.shape[0]
    piece_rows = tok_rows // 2 // pieces

    def piece_at(half, q):
        return pl.ds(pl.multiple_of(half * (tok_rows // 2) + q * piece_rows, piece_rows), piece_rows)

    def t_y(q):
        at = piece_at(x, q)
        return send(tokens.at[at, :], tok_in.at[at, :], ty_s.at[q], t_r.at[x, q], partner)

    def t_x(half, q):
        at = piece_at(half, q)
        return send(tok_in.at[at, :], tok_in.at[at, :], tx_s.at[q], t_r.at[half, q], across_x)

    def pass_token(q):
        t_y(q).wait_recv()
        t_x(x, q).start()

    def o_kept():
        return pltpu.make_async_copy(w_out, o_chunk(z), o_r.at[z])

    o_kept().start()

    @pl.when(stays)
    def _():
        for a in (2, 0, 1):
            kept(a).start()
        tok_kept().start()

    @pl.when(moves)
    def _():
        for a in (2, 0, 1):
            staged(a).start()

    barrier = pltpu.get_barrier_semaphore()

    def greet(where):
        pl.semaphore_signal(barrier, inc=1, device_id=where, device_id_type=pl.DeviceIdType.MESH)

    for dy in range(2):
        for dx in range(2):
            for dc in range(2):
                if dy + dx + dc:
                    greet((2 * z + (y + dy) % 2, 2 * ((x + dx) % 2) + (c + dc) % 2))
    pl.when(has_up)(lambda: greet(above))
    pl.when(has_down)(lambda: greet(below))
    pl.when(has_up & (c == 1))(lambda: greet(up_other))
    pl.when(has_down & (c == 0))(lambda: greet((sp - 2, 2 * x + 1)))
    pl.semaphore_wait(barrier, 7 + jnp.where(has_up, 1 + c, 0) + jnp.where(has_down, 2 - c, 0))

    def go(a, zz, kind):
        s = 2 * zz + c
        ref = chunk(a, s) if a < 3 else o_chunk(zz)
        r_sem = w_r.at[a, s] if a < 3 else o_r.at[zz]
        s_sem = {"up": up_s, "down": down_s, "side": side_s}[kind].at[a, zz]
        return send(ref, ref, s_sem, r_sem, {"up": above, "down": below, "side": side}[kind])

    def swap_order(layer):
        return {0: (2, 0, 1), last: (0, 1, 2)}.get(layer, (0, 2, 1))

    @pl.when(moves)
    def _():
        for layer in range(nz):
            @pl.when(z == layer)
            def _(layer=layer):
                for a in swap_order(layer):
                    staged(a).wait()
                    swapped(a).start()
        for q in range(pieces):
            t_y(q).start()

    def o_relay(layer, d):
        if layer - d >= 0:
            go(3, layer - d, "up").wait_recv()
            if layer < last:
                go(3, layer - d, "up").start()
        if layer + d < nz:
            go(3, layer + d, "down").wait_recv()
            if layer > 0:
                go(3, layer + d, "down").start()

    def o_share(axis):
        ref, where = (
            (out_rows.at[c, y, x], across_x),
            (out_rows.at[c, y], across_y),
            (out_rows.at[c], side),
        )[axis]
        return send(ref, ref, o_s.at[axis], o_r2.at[axis], where)

    def events(layer):
        listed = []
        for i in range(3):
            for d in range(1, layer + 1):
                listed.append((i * layer + d, "up", upward[i], layer - d, d))
            for d in range(1, last - layer + 1):
                listed.append((i * (last - layer) + d, "down", downward[i], layer + d, d))
        return sorted(listed)

    def handle(layer, event):
        _, kind, a, zz, d = event
        go(a, zz, kind).wait_recv()
        if kind == "up":
            if layer < last:
                go(a, zz, "up").start()
            if d == layer and a == upward[1] and layer < last:
                go(upward[2], layer, "up").start()
        else:
            if layer > 0:
                go(a, zz, "down").start()
        go(a, zz, "side").start()

    def begin(layer):
        o_kept().wait()
        if layer < last:
            go(3, layer, "up").start()
        if layer > 0:
            go(3, layer, "down").start()
        for a in swap_order(layer):
            pl.when(stays)(lambda a=a: kept(a).wait())
            pl.when(moves)(lambda a=a: go(a, layer, "side").wait_recv())
            if layer < last and (layer == 0 or a != upward[2]):
                go(a, layer, "up").start()
            if layer > 0 and (layer == last or a != downward[2]):
                go(a, layer, "down").start()
            go(a, layer, "side").start()

    def row_time(p):
        b, i = p >> sub_log, p & (sub - 1)
        return THIRD_DILATION * i + (b >> 2) + SECOND_DILATION * (b & 3)

    def tail_time(u):
        per = tail // THIRD_DILATION
        b, i = u >> (per.bit_length() - 1), u & (per - 1)
        return THIRD_DILATION * (sub - per + i) + (b >> 2) + SECOND_DILATION * (b & 3) - tok_rows

    def iota(shape, axis):
        return lax.broadcasted_iota(jnp.int32, shape, axis)

    def angles(index, carry):
        at = index * block
        rows = pl.ds(pl.multiple_of(at, block), block)
        pair_at = iota((1, DH), 1) & (DH // 2 - 1)
        freq = jnp.exp(pair_at.astype(jnp.float32) * (-2.0 * math.log(ROPE_BASE) / DH))
        angle = (row_time(iota((block, DH), 0) + at) + rank * tok_rows).astype(jnp.float32) * freq
        cosine[rows, :] = jnp.cos(angle)
        turned = jnp.sin(angle)
        sine[rows, :] = jnp.where(iota((block, DH), 1) < DH // 2, -turned, turned)
        return carry

    def order():
        p = row_time(iota((tok_rows, tok_rows), 0))
        t = iota((tok_rows, tok_rows), 1)
        pick = jnp.where(p == t, 1.0, 0.0).astype(jnp.bfloat16)

        def piece(index, carry):
            at = pl.ds(pl.multiple_of(index * 256, 256), 256)
            tok_turned[:, at] = jnp.dot(
                pick, tok_in[:, at], preferred_element_type=jnp.float32
            ).astype(jnp.bfloat16)
            return carry

        lax.fori_loop(0, depth // 256, piece, 0)

    def project(a, store):
        def piece(index, carry):
            rows = pl.ds(pl.multiple_of(index * block, block), block)
            raw = jnp.dot(tok_turned[rows, :], weights[a], preferred_element_type=jnp.float32)
            for g in range(GROUPS):
                part = raw[:, g * DH : (g + 1) * DH]
                if a != 1:
                    part = part * cosine[rows, :] + pltpu.roll(part, DH // 2, 1) * sine[rows, :]
                store(index, rows, g, part)
            return carry

        lax.fori_loop(0, SECOND_DILATION, piece, 0)

    def keep_pair(which):
        def store(index, rows, g, part):
            if g == 2:
                far2[4 + c, which, rows, :] = part.astype(jnp.bfloat16)
            elif g == 1:
                near_own[which, rows, :] = part.astype(jnp.bfloat16)
            else:
                pair0[which, rows, :] = part.astype(jnp.bfloat16)
                per = tail // THIRD_DILATION
                ends = jnp.concatenate(
                    [part[b * sub + sub - per : (b + 1) * sub] for b in range(4)], axis=0
                )
                at = pl.ds(pl.multiple_of(tok_rows + index * 4 * per, 4 * per), 4 * per)
                near_own[which, at, :] = ends.astype(jnp.bfloat16)

        return store

    def keep_query(index, rows, g, part):
        queries[g, rows, :] = part.astype(jnp.bfloat16)

    def others(a):
        for zz in range(nz):
            s = 2 * zz + 1 - c
            send(chunk(a, s), chunk(a, s), side_s.at[a, zz], w_r.at[a, s], side).wait_recv()

    def far(kind, src, dst, where):
        return send(far2.at[src], far2.at[dst], far_s.at[kind], far_r.at[dst], where)

    gives_up, takes_up = z < last - 1, (z > 0) & (z < last)
    helps, asks = z == last - 1, z == last

    def own_side():
        return far(0, 4 + c, 4 + c, side)

    def own_up():
        return far(1, 4 + c, 2 + c, above)

    def pass_side(kind, slot):
        return far(kind, slot, slot, side)

    def pass_up():
        return far(3, 2 + c, c, above)

    def near(where):
        return send(near_own, near_in, near_s, near_r, where)

    def halos():
        pl.when(gives_up)(lambda: own_up().start())
        pl.when(has_up & (c == 1))(lambda: near(up_other).start())
        pl.when(c == 0)(lambda: near(side).start())
        pl.when((c == 0) | helps)(lambda: own_side().start())

    def ask():
        return send(queries.at[2], asked, part_s.at[0], part_r.at[0], below)

    def answer():
        return send(part, got_part, part_s.at[1], part_r.at[1], above)

    def answer_log():
        return send(part_log, got_log, part_s.at[2], part_r.at[2], above)

    scale = DH ** (-0.5)
    far_off = 1 << 24

    def dots(q, k):
        return lax.dot_general(q, k, (((1,), (1,)), ((), ())), preferred_element_type=jnp.float32)

    def soft(scores, time_q, time_k, reach, first):
        gap = time_q - jnp.where(time_k >= first, time_k, far_off)
        scores = jnp.where((gap >= 0) & (gap <= reach), scores * scale, -jnp.inf)
        top = jnp.max(scores, axis=-1, keepdims=True)
        weight = jnp.exp(scores - top)
        return top, jnp.sum(weight, axis=-1, keepdims=True), weight.astype(jnp.bfloat16)

    def near_groups():
        def piece(index, carry):
            begin = index * block
            rows = pl.ds(pl.multiple_of(begin, block), block)
            q = queries[0, rows, :]
            tails = pl.ds(tok_rows, tail)
            scores = jnp.concatenate([dots(q, near_in[0, tails, :]), dots(q, pair0[0])], axis=1)
            lane = iota((1, tail + tok_rows), 1)
            time_k = jnp.where(lane < tail, tail_time(lane & (tail - 1)), row_time(lane - tail))
            time_q = row_time(iota((block, 1), 0) + begin)
            top0, sum0, weight = soft(scores, time_q, time_k, WIN1, -rank * tok_rows)
            got0 = jnp.dot(weight[:, :tail], near_in[1, tails, :], preferred_element_type=jnp.float32)
            got0 += jnp.dot(weight[:, tail:], pair0[1], preferred_element_type=jnp.float32)
            q = queries[1, rows, :]
            scores = jnp.concatenate(
                [dots(q, near_in[0, rows, :]), dots(q, near_own[0, rows, :])], axis=1
            )

            def step_of(place):
                return 4 * (place & (sub - 1)) + (place >> sub_log)

            lane = iota((1, 2 * block), 1)
            step_k = step_of(lane & (block - 1)) + jnp.where(lane < block, -block, 0)
            top1, sum1, weight = soft(
                scores, step_of(iota((block, 1), 0)), step_k, WIN2 // SECOND_DILATION, -rank * block
            )
            got1 = jnp.dot(weight[:, :block], near_in[1, rows, :], preferred_element_type=jnp.float32)
            got1 += jnp.dot(weight[:, block:], near_own[1, rows, :], preferred_element_type=jnp.float32)
            top = jnp.maximum(top0, top1)
            f0, f1 = jnp.exp(top0 - top), jnp.exp(top1 - top)
            got01[rows, :] = f0 * got0 + f1 * got1
            top01[rows, :] = top
            sum01[rows, :] = f0 * sum0 + f1 * sum1
            return carry

        lax.fori_loop(0, SECOND_DILATION, piece, 0)

    def far_piece(index, source, slots, reach_back, first, until=None):
        begin = index * block

        def rows_of(b):
            return pl.ds(pl.multiple_of(begin + b * sub, sub), sub)

        all_scores = []
        for b in range(4):
            keys = jnp.concatenate([far2[slot, 0, rows_of(b), :] for slot in slots], axis=0)
            all_scores.append(dots(source[rows_of(b), :], keys))
        scores = jnp.concatenate(all_scores, axis=0)
        step_q = iota((block, 1), 0) & (sub - 1)
        step_k = iota((1, len(slots) * sub), 1) - reach_back * sub
        seen = step_k if until is None else jnp.where(step_k < until, step_k, far_off)
        top, total, weight = soft(scores, step_q, seen, WIN3 // THIRD_DILATION, first)
        got = []
        for b in range(4):
            vals = jnp.concatenate([far2[slot, 1, rows_of(b), :] for slot in slots], axis=0)
            got.append(
                jnp.dot(weight[b * sub : (b + 1) * sub], vals, preferred_element_type=jnp.float32)
            )
        return top, total, jnp.concatenate(got, axis=0)

    def eye():
        return iota((block, block), 0) == iota((block, block), 1)

    def block_rows(index):
        return pl.ds(pl.multiple_of(index * block, block), block)

    def help_above():
        slots = [2 + c, 3 + c, 4 + c, 5]

        def piece(index, carry):
            top, total, got = far_piece(index, asked, slots, 4, -4 * sub, -c * sub)
            part[block_rows(index), :] = (got / total).astype(jnp.bfloat16)
            row = jnp.sum(jnp.where(eye(), top + jnp.log(total), 0.0), axis=0, keepdims=True)
            part_log[index] = jnp.broadcast_to(row, part_log.shape[1:])
            return carry

        lax.fori_loop(0, SECOND_DILATION, piece, 0)

    def settle(rows, top2, sum2, got2):
        top1 = top01[rows, :]
        top = jnp.maximum(top1, top2)
        f1, f2 = jnp.exp(top1 - top), jnp.exp(top2 - top)
        total = f1 * sum01[rows, :] + f2 * sum2
        mine[0, rows, :] = ((f1 * got01[rows, :] + f2 * got2) / total).astype(jnp.bfloat16)

    def far_here():
        slots = [4 + c - d for d in (4, 3, 2, 1, 0)]

        def piece(index, carry):
            settle(block_rows(index), *far_piece(index, queries.at[2], slots, 4, -rank * sub))
            return carry

        lax.fori_loop(0, SECOND_DILATION, piece, 0)

    def far_asked():
        slots = [3 + c, 4 + c]

        def piece(index, carry):
            rows = block_rows(index)
            top_a, sum_a, got_a = far_piece(index, queries.at[2], slots, 1, -c * sub)
            top_b = jnp.sum(jnp.where(eye(), got_log[index, 0:1, :], 0.0), axis=1, keepdims=True)
            top2 = jnp.maximum(top_a, top_b)
            fa, fb = jnp.exp(top_a - top2), jnp.exp(top_b - top2)
            got2 = fa * got_a + fb * got_part[rows, :].astype(jnp.float32)
            settle(rows, top2, fa * sum_a + fb, got2)
            return carry

        lax.fori_loop(0, SECOND_DILATION, piece, 0)

    def unturn():
        t = iota((tok_rows, tok_rows), 0)
        p = row_time(iota((tok_rows, tok_rows), 1))
        mine[1] = jnp.dot(
            jnp.where(p == t, 1.0, 0.0).astype(jnp.bfloat16), mine[0], preferred_element_type=jnp.float32
        ).astype(jnp.bfloat16)

    head = 2 * x + y
    quarter = tok_rows // 4

    def deal(k):
        return send(
            mine.at[1, pl.ds(k * quarter, quarter), :], heads_in.at[head], head_s.at[k], head_r.at[head], (rank, k)
        )

    def deal_self(k):
        return pltpu.make_async_copy(mine.at[1, pl.ds(k * quarter, quarter), :], heads_in.at[head], head_r.at[head])

    def turn_tokens():
        pl.when(stays)(lambda: tok_kept().wait())

        @pl.when(moves)
        def _():
            for q in range(pieces):
                t_x(1 - x, q).wait_recv()

        order()

    def key_value(which):
        others(which)
        project(which, keep_pair(which))

    def query():
        others(2)
        project(2, keep_query)

    def last_down(layer):
        if 0 < layer < last:
            go(downward[2], layer, "down").start()

    def run(layer):
        begin(layer)
        o_relay(layer, 1)
        lax.fori_loop(0, SECOND_DILATION, angles, 0)
        pl.when(stays)(turn_tokens)
        todo = events(layer)
        for q in range(3):
            handle(layer, todo[q])
            pl.when(moves)(lambda q=q: pass_token(q))
        o_relay(layer, 2)
        split = 9 if layer == 2 else 6 if layer != 1 else 7
        downs = [i for i, event in enumerate(todo) if event[1:3] == ("down", downward[1])]
        for i in range(3, split):
            handle(layer, todo[i])
            if i == 3:
                pl.when(moves)(lambda: pass_token(3))
            if layer == 2 and i == max(max(downs), 3):
                last_down(layer)
        late = todo[split:]
        if layer == 1:
            @pl.when(moves)
            def _():
                last_down(layer)
                for event in late:
                    handle(layer, event)

        o_relay(layer, 3)
        o_share(0).start()
        pl.when(moves)(turn_tokens)
        if layer == last:
            query()
            ask().start()
            key_value(0)
        else:
            key_value(0)
            key_value(1)
            halos()
        o_share(0).wait()
        o_share(1).start()
        if layer == 1:
            @pl.when(stays)
            def _():
                last_down(layer)
                for event in late:
                    handle(layer, event)
        else:
            for event in late:
                handle(layer, event)
        if layer == last:
            key_value(1)
            halos()
        else:
            query()

    for layer in range(nz):
        pl.when(z == layer)(functools.partial(run, layer))

    for slot in range(4):
        @pl.when((2 * z + slot < 4) | (asks & (c == 0) & (slot == 3)))
        def _(slot=slot):
            far2[slot] = jnp.zeros(far2.shape[1:], far2.dtype)

    @pl.when(rank == 0)
    def _():
        near_in[...] = jnp.zeros(near_in.shape, near_in.dtype)

    @pl.when(takes_up)
    def _():
        own_up().wait_recv()
        pl.when(gives_up)(lambda: pass_up().start())
        pass_side(2, 2 + c).start()

    pl.when(c == 1)(lambda: pass_side(0, 4).wait_recv())

    @pl.when(helps)
    def _():
        pl.when(c == 0)(lambda: pass_side(0, 5).wait_recv())
        pass_side(2, 3 - c).wait_recv()
        ask().wait_recv()
        help_above()
        answer().start()
        answer_log().start()

    pl.when(rank >= 1)(lambda: near(side).wait_recv())
    near_groups()
    o_share(1).wait()
    o_share(2).start()

    @pl.when(helps)
    def _():
        pass_up().wait_recv()
        pl.when(c == 1)(lambda: pass_side(4, 1).start())
        pl.when(c == 0)(lambda: pass_side(4, 1).wait_recv())

    pl.when(takes_up & gives_up)(lambda: pass_side(2, 3 - c).wait_recv())

    @pl.when(asks)
    def _():
        answer().wait_recv()
        answer_log().wait_recv()
        far_asked()

    pl.when(jnp.logical_not(asks))(far_here)
    unturn()
    for k in range(4):
        self_here = stays & (tp == k)
        pl.when(self_here)(lambda k=k: deal_self(k).start())
        pl.when(jnp.logical_not(self_here))(lambda k=k: deal(k).start())

    o_share(2).wait()
    for h in range(4):
        pltpu.make_async_copy(heads_in.at[h], heads_in.at[h], head_r.at[h]).wait()
    for zz in range(nz):
        for yy in range(2):
            acc = None
            for h in range(4):
                one = jnp.dot(heads_in[h], out_rows[h % 2, yy, h // 2, zz], preferred_element_type=jnp.float32)
                acc = one if acc is None else acc + one
            width = w_out.shape[1]
            s = 2 * zz + yy
            out[:, s * width : (s + 1) * width] = acc.astype(jnp.bfloat16)

    for k in range(4):
        pl.when(jnp.logical_not(stays & (tp == k)))(lambda k=k: deal(k).wait_send())

    @pl.when(moves)
    def _():
        for a in range(3):
            swapped(a).wait_send()
        for q in range(pieces):
            t_y(q).wait_send()
            t_x(x, q).wait_send()

    for a in range(4):
        for zz in range(nz):
            pl.when(has_up & (zz <= z))(lambda a=a, zz=zz: go(a, zz, "up").wait_send())
            pl.when(has_down & (zz >= z))(lambda a=a, zz=zz: go(a, zz, "down").wait_send())
            if a < 3:
                go(a, zz, "side").wait_send()
    pl.when((c == 0) | has_up)(lambda: near(side).wait_send())
    pl.when((c == 0) | helps)(lambda: own_side().wait_send())
    pl.when(gives_up)(lambda: own_up().wait_send())
    pl.when(takes_up)(lambda: pass_side(2, 2 + c).wait_send())
    pl.when(takes_up & gives_up)(lambda: pass_up().wait_send())
    pl.when(helps & (c == 1))(lambda: pass_side(4, 1).wait_send())
    pl.when(asks)(lambda: ask().wait_send())

    @pl.when(helps)
    def _():
        answer().wait_send()
        answer_log().wait_send()


def fits_kernel(n_sp, n_tp, tokens, w_query, w_out):
    tok_rows, depth = tokens.shape
    return (
        n_sp == 2 * LAYERS
        and n_tp == 4
        and w_query.shape[1] == GROUPS * DH
        and w_out.shape[0] == DH
        and w_out.shape[1] % 128 == 0
        and w_query.shape[0] % 16 == 0
        and tok_rows == WIN2
        and 4 * tok_rows == WIN3
        and 4 * WIN1 == tok_rows
    )


def one_kernel(n_sp, tokens, w_query, w_key, w_value, w_out):
    nz = n_sp // 2
    tok_rows, depth = tokens.shape
    cols = w_query.shape[1]
    bf, dma = jnp.bfloat16, pltpu.SemaphoreType.DMA
    return pl.pallas_call(
        functools.partial(layer_kernel, nz),
        out_shape=jax.ShapeDtypeStruct((tok_rows // 4, w_out.shape[1] * n_sp), bf),
        in_specs=[pl.BlockSpec(memory_space=pltpu.HBM)] * 5,
        out_specs=pl.BlockSpec(memory_space=pltpu.VMEM),
        scratch_shapes=[
            pltpu.VMEM((3, depth, cols), bf),
            pltpu.VMEM((3, *w_query.shape), bf),
            pltpu.VMEM((tok_rows, depth), bf),
            pltpu.VMEM((tok_rows, depth), bf),
            pltpu.VMEM((tok_rows, DH), jnp.float32),
            pltpu.VMEM((tok_rows, DH), jnp.float32),
            pltpu.VMEM((GROUPS, tok_rows, DH), bf),
            pltpu.VMEM((2, tok_rows, DH), bf),
            pltpu.VMEM((2, tok_rows + WIN1, DH), bf),
            pltpu.VMEM((2, tok_rows + WIN1, DH), bf),
            pltpu.VMEM((6, 2, tok_rows, DH), bf),
            pltpu.VMEM((2, 2, 2, nz, *w_out.shape), bf),
            pltpu.VMEM((2, tok_rows, DH), bf),
            pltpu.VMEM((4, tok_rows // 4, DH), bf),
            pltpu.VMEM((tok_rows, DH), jnp.float32),
            pltpu.VMEM((tok_rows, 1), jnp.float32),
            pltpu.VMEM((tok_rows, 1), jnp.float32),
            pltpu.VMEM((tok_rows, DH), bf),
            pltpu.VMEM((tok_rows, DH), bf),
            pltpu.VMEM((SECOND_DILATION, 8, DH), jnp.float32),
            pltpu.VMEM((tok_rows, DH), bf),
            pltpu.VMEM((SECOND_DILATION, 8, DH), jnp.float32),
            dma((3,)), dma((3,)), dma, dma((2, 4)), dma((4,)), dma((4,)), dma((3, n_sp)), dma((4, nz)), dma((4, nz)), dma((3, nz)),
            dma((nz,)), dma((3,)), dma((3,)),
            dma((5,)), dma((6,)), dma, dma, dma((4,)), dma((4,)), dma((3,)), dma((3,)),
        ],
        compiler_params=pltpu.CompilerParams(
            collective_id=0, has_side_effects=True, vmem_limit_bytes=60 * 1024 * 1024
        ),
    )(tokens, w_key, w_value, w_query, w_out)


def on_mesh(n_sp, n_tp, *operands):
    tokens, w_query, _, _, w_out = operands
    if fits_kernel(n_sp, n_tp, tokens, w_query, w_out):
        return one_kernel(n_sp, *operands)
    return on_device(*operands)


def solution(mesh):
    placed = (P("sp", None), P("sp", "tp"), P("sp", "tp"), P("sp", "tp"), P("tp", "sp"))
    body = functools.partial(on_mesh, mesh.shape["sp"], mesh.shape["tp"])
    return jax.shard_map(
        body, mesh=mesh, in_specs=placed, out_specs=P(("sp", "tp"), None), check_vma=False
    )
```

```python
import functools
import math

import jax
import jax.numpy as jnp
from jax import lax
from jax.experimental import pallas as pl
from jax.experimental.pallas import tpu as pltpu
from jax.sharding import PartitionSpec as P

GROUPS = 3
DH = 128
WIN1 = 128
WIN2 = 512
WIN3 = 2048
SECOND_DILATION = 4
THIRD_DILATION = 16


ROPE_BASE = 500000.0

LAYERS = 4


def from_behind(block, axis, distance):
    devices = range(lax.axis_size(axis))
    route = [(i - distance, i) for i in devices if i - distance in devices]
    return lax.ppermute(block, axis, route)


def rotate(projected, offset):
    tok_rows = projected.shape[0]
    head_size = projected.shape[-1]
    half_size = head_size // 2
    positions = (offset + jnp.arange(tok_rows, dtype=jnp.int32)).astype(jnp.float32)
    frequency = 1.0 / ROPE_BASE ** (jnp.arange(0, head_size, 2, dtype=jnp.float32) / head_size)
    angles = (positions[:, None] * frequency[None, :]).reshape(tok_rows, 1, 1, half_size)
    cosine = jnp.cos(angles)
    sine_part = jnp.sin(angles)
    first_half = projected[..., :half_size]
    second_half = projected[..., half_size:]
    return jnp.concatenate(
        [
            first_half * cosine - second_half * sine_part,
            second_half * cosine + first_half * sine_part,
        ],
        axis=-1,
    )


def window_attend(query_part, buffer, steps, stride, offset):
    tok_rows, heads_here, head_size = query_part.shape
    sub_rows = tok_rows // stride
    key_rows = buffer.shape[1] // stride
    query_sub = query_part.reshape(sub_rows, stride, heads_here, head_size).transpose(1, 2, 0, 3)
    pair_sub = buffer.reshape(2, key_rows, stride, heads_here, head_size).transpose(0, 2, 3, 1, 4)
    block_rows = math.gcd(sub_rows, steps) if sub_rows > steps else sub_rows
    block_list = sub_rows // block_rows
    query_blocks = query_sub.reshape(stride, heads_here, block_list, block_rows, head_size)
    key_blocks = jnp.stack(
        [
            pair_sub[:, :, :, index * block_rows : index * block_rows + block_rows + steps]
            for index in range(block_list)
        ],
        axis=3,
    )
    scores = jnp.einsum(
        "zhnqe,zhnke->zhnqk", query_blocks, key_blocks[0], preferred_element_type=jnp.float32
    ) * head_size ** (-0.5)
    query_index = (jnp.arange(block_list, dtype=jnp.int32) * block_rows)[
        :, None, None
    ] + jnp.arange(block_rows, dtype=jnp.int32)[None, :, None]
    key_index = (jnp.arange(block_list, dtype=jnp.int32) * block_rows)[:, None, None] + jnp.arange(
        block_rows + steps, dtype=jnp.int32
    )[None, None, :]
    spacing = query_index + steps - key_index
    residue = jnp.arange(stride, dtype=jnp.int32)[:, None, None, None]
    key_position = offset + (key_index[None] - steps) * stride + residue
    allowed = (spacing[None] >= 0) & (spacing[None] <= steps) & (key_position >= 0)
    scores = jnp.where(allowed[:, None], scores, -jnp.inf)
    row_max = jnp.max(scores, axis=-1)
    exponent = jnp.exp(scores - row_max[..., None])
    totals = jnp.sum(exponent, axis=-1)
    probs = (exponent / totals[..., None]).astype(jnp.bfloat16)
    mixed = jnp.einsum(
        "zhnqk,zhnke->zhnqe", probs, key_blocks[1], preferred_element_type=jnp.float32
    )
    mixed = mixed.reshape(stride, heads_here, sub_rows, head_size).transpose(2, 0, 1, 3)
    log_total = (row_max + jnp.log(totals)).reshape(stride, heads_here, sub_rows).transpose(2, 0, 1)
    return (mixed.reshape(tok_rows, heads_here, head_size), log_total.reshape(tok_rows, heads_here))


def reach_back(key_value, distance_max):
    tok_rows = key_value.shape[1]
    gathered = key_value
    pieces_held = 1
    while pieces_held < distance_max + 1:
        slice_share = min(pieces_held, distance_max + 1 - pieces_held)
        arrived = from_behind(
            gathered[:, gathered.shape[1] - slice_share * tok_rows :], "sp", pieces_held
        )
        gathered = jnp.concatenate([arrived, gathered], axis=1)
        pieces_held = pieces_held + slice_share
    return gathered


def on_device(tokens, w_query, w_key, w_value, w_out):
    tok_rows = tokens.shape[0]
    heads_here = w_out.shape[0] // DH
    offset = lax.axis_index("sp") * tok_rows
    weight_parts = (
        lax.all_gather(w_query, "sp", axis=0, tiled=True),
        lax.all_gather(w_key, "sp", axis=0, tiled=True),
        lax.all_gather(w_value, "sp", axis=0, tiled=True),
    )
    query_raw, key_raw, value_raw = tuple(
        (
            jnp.dot(tokens, weight_rows, preferred_element_type=jnp.float32)
            for weight_rows in weight_parts
        )
    )
    head_shape = (tok_rows, heads_here, GROUPS, DH)
    queries = rotate(query_raw.reshape(head_shape), offset).astype(jnp.bfloat16)
    keys_all = rotate(key_raw.reshape(head_shape), offset).astype(jnp.bfloat16)
    values_all = value_raw.astype(jnp.bfloat16).reshape(head_shape)
    windows = (WIN1, WIN2, WIN3)
    step_sizes = (1, SECOND_DILATION, THIRD_DILATION)
    outputs = []
    log_totals = []
    for group_index in range(GROUPS):
        key_value = jnp.stack([keys_all[:, :, group_index], values_all[:, :, group_index]])
        key_value = key_value.reshape(2, tok_rows, heads_here * DH)
        window = windows[group_index]
        if group_index == 0:
            near_rows = from_behind(key_value[:, tok_rows - window :], "sp", 1)
            buffer = jnp.concatenate([near_rows, key_value], axis=1)
        else:
            distance_max = (window + tok_rows - 1) // tok_rows
            buffer = reach_back(key_value, distance_max)
        group_out, log_total = window_attend(
            queries[:, :, group_index],
            buffer,
            window // step_sizes[group_index],
            step_sizes[group_index],
            offset,
        )
        outputs.append(group_out)
        log_totals.append(log_total)
    group_weights = jax.nn.softmax(jnp.stack(log_totals), axis=0)
    merged = jnp.sum(group_weights[..., None] * jnp.stack(outputs), axis=0).astype(jnp.bfloat16)
    merged = merged.reshape(tok_rows, heads_here * DH)
    w_whole = lax.all_gather(w_out, "sp", axis=1, tiled=True)
    return lax.psum_scatter(
        jnp.dot(merged, w_whole, preferred_element_type=jnp.float32).astype(jnp.bfloat16),
        "tp",
        scatter_dimension=0,
        tiled=True,
    )


def layer_kernel(
    nz,
    tokens, w_key, w_value, w_query, w_out, out,
    weights, stage, tok_in, tok_turned, cosine, sine, queries, pair0, near_own, near_in, far2,
    out_rows, mine, heads_in, got01, top01, sum01, asked, part, part_log, got_part, got_log,
    stage_s, swap_s, tok_k, t_r, ty_s, tx_s, w_r, up_s, down_s, side_s, o_r, o_s, o_r2, far_s, far_r, near_s, near_r, head_s, head_r, part_s, part_r,
):
    tok_rows, depth = tokens.shape
    k_rows, cols = w_key.shape
    sub = tok_rows // THIRD_DILATION
    sub_log = sub.bit_length() - 1
    block = tok_rows // SECOND_DILATION
    tail = WIN1
    last = nz - 1
    sp, tp = lax.axis_index("sp"), lax.axis_index("tp")
    z, y = sp // 2, sp % 2
    x, c = tp // 2, tp % 2
    rank = 2 * z + c
    stays = c == y
    moves = jnp.logical_not(stays)
    has_up, has_down = z < last, z > 0
    side = (sp, 2 * x + 1 - c)
    across_x = (sp, 2 * (1 - x) + c)
    across_y = (2 * z + 1 - y, tp)
    partner = (2 * z + 1 - y, 2 * x + 1 - c)
    above, below = (sp + 2, tp), (sp - 2, tp)
    up_other = (sp + 2, 2 * x)

    def send(src, dst, s_sem, r_sem, where):
        return pltpu.make_async_remote_copy(
            src_ref=src, dst_ref=dst, send_sem=s_sem, recv_sem=r_sem,
            device_id=where, device_id_type=pl.DeviceIdType.MESH,
        )

    parts = (w_key, w_value, w_query)
    upward, downward = (2, 0, 1), (0, 1, 2)

    def chunk(a, s):
        return weights.at[a, pl.ds(pl.multiple_of(s * k_rows, k_rows), k_rows), :]

    def o_chunk(zz):
        return out_rows.at[c, y, x, zz]

    def kept(a):
        return pltpu.make_async_copy(parts[a], chunk(a, rank), w_r.at[a, rank])

    def staged(a):
        return pltpu.make_async_copy(parts[a], stage.at[a], stage_s.at[a])

    def swapped(a):
        there = 2 * z + 1 - c
        return send(stage.at[a], chunk(a, there), swap_s.at[a], w_r.at[a, there], partner)

    def tok_kept():
        return pltpu.make_async_copy(tokens, tok_in, tok_k)

    pieces = ty_s.shape[0]
    piece_rows = tok_rows // 2 // pieces

    def piece_at(half, q):
        return pl.ds(pl.multiple_of(half * (tok_rows // 2) + q * piece_rows, piece_rows), piece_rows)

    def t_y(q):
        at = piece_at(x, q)
        return send(tokens.at[at, :], tok_in.at[at, :], ty_s.at[q], t_r.at[x, q], partner)

    def t_x(half, q):
        at = piece_at(half, q)
        return send(tok_in.at[at, :], tok_in.at[at, :], tx_s.at[q], t_r.at[half, q], across_x)

    def pass_token(q):
        t_y(q).wait_recv()
        t_x(x, q).start()

    def o_kept():
        return pltpu.make_async_copy(w_out, o_chunk(z), o_r.at[z])

    o_kept().start()

    @pl.when(stays)
    def _():
        for a in (2, 0, 1):
            kept(a).start()
        tok_kept().start()

    @pl.when(moves)
    def _():
        for a in (2, 0, 1):
            staged(a).start()

    barrier = pltpu.get_barrier_semaphore()

    def greet(where):
        pl.semaphore_signal(barrier, inc=1, device_id=where, device_id_type=pl.DeviceIdType.MESH)

    for dy in range(2):
        for dx in range(2):
            for dc in range(2):
                if dy + dx + dc:
                    greet((2 * z + (y + dy) % 2, 2 * ((x + dx) % 2) + (c + dc) % 2))
    pl.when(has_up)(lambda: greet(above))
    pl.when(has_down)(lambda: greet(below))
    pl.when(has_up & (c == 1))(lambda: greet(up_other))
    pl.when(has_down & (c == 0))(lambda: greet((sp - 2, 2 * x + 1)))
    pl.semaphore_wait(barrier, 7 + jnp.where(has_up, 1 + c, 0) + jnp.where(has_down, 2 - c, 0))

    def go(a, zz, kind):
        s = 2 * zz + c
        ref = chunk(a, s) if a < 3 else o_chunk(zz)
        r_sem = w_r.at[a, s] if a < 3 else o_r.at[zz]
        s_sem = {"up": up_s, "down": down_s, "side": side_s}[kind].at[a, zz]
        return send(ref, ref, s_sem, r_sem, {"up": above, "down": below, "side": side}[kind])

    def swap_order(layer):
        return {0: (2, 0, 1), last: (0, 1, 2)}.get(layer, (0, 2, 1))

    @pl.when(moves)
    def _():
        for layer in range(nz):
            @pl.when(z == layer)
            def _(layer=layer):
                for a in swap_order(layer):
                    staged(a).wait()
                    swapped(a).start()
        for q in range(pieces):
            t_y(q).start()

    def o_relay(layer, d):
        if layer - d >= 0:
            go(3, layer - d, "up").wait_recv()
            if layer < last:
                go(3, layer - d, "up").start()
        if layer + d < nz:
            go(3, layer + d, "down").wait_recv()
            if layer > 0:
                go(3, layer + d, "down").start()

    def o_share(axis):
        ref, where = (
            (out_rows.at[c, y, x], across_x),
            (out_rows.at[c, y], across_y),
            (out_rows.at[c], side),
        )[axis]
        return send(ref, ref, o_s.at[axis], o_r2.at[axis], where)

    def events(layer):
        listed = []
        for i in range(3):
            for d in range(1, layer + 1):
                listed.append((i * layer + d, "up", upward[i], layer - d, d))
            for d in range(1, last - layer + 1):
                listed.append((i * (last - layer) + d, "down", downward[i], layer + d, d))
        return sorted(listed)

    def handle(layer, event):
        _, kind, a, zz, d = event
        go(a, zz, kind).wait_recv()
        if kind == "up":
            if layer < last:
                go(a, zz, "up").start()
            if d == layer and a == upward[1] and layer < last:
                go(upward[2], layer, "up").start()
        else:
            if layer > 0:
                go(a, zz, "down").start()
        go(a, zz, "side").start()

    def begin(layer):
        o_kept().wait()
        if layer < last:
            go(3, layer, "up").start()
        if layer > 0:
            go(3, layer, "down").start()
        for a in swap_order(layer):
            pl.when(stays)(lambda a=a: kept(a).wait())
            pl.when(moves)(lambda a=a: go(a, layer, "side").wait_recv())
            if layer < last and (layer == 0 or a != upward[2]):
                go(a, layer, "up").start()
            if layer > 0 and (layer == last or a != downward[2]):
                go(a, layer, "down").start()
            go(a, layer, "side").start()

    def row_time(p):
        b, i = p >> sub_log, p & (sub - 1)
        return THIRD_DILATION * i + (b >> 2) + SECOND_DILATION * (b & 3)

    def tail_time(u):
        per = tail // THIRD_DILATION
        b, i = u >> (per.bit_length() - 1), u & (per - 1)
        return THIRD_DILATION * (sub - per + i) + (b >> 2) + SECOND_DILATION * (b & 3) - tok_rows

    def iota(shape, axis):
        return lax.broadcasted_iota(jnp.int32, shape, axis)

    def angles(index, carry):
        at = index * block
        rows = pl.ds(pl.multiple_of(at, block), block)
        pair_at = iota((1, DH), 1) & (DH // 2 - 1)
        freq = jnp.exp(pair_at.astype(jnp.float32) * (-2.0 * math.log(ROPE_BASE) / DH))
        angle = (row_time(iota((block, DH), 0) + at) + rank * tok_rows).astype(jnp.float32) * freq
        cosine[rows, :] = jnp.cos(angle)
        turned = jnp.sin(angle)
        sine[rows, :] = jnp.where(iota((block, DH), 1) < DH // 2, -turned, turned)
        return carry

    def order():
        p = row_time(iota((tok_rows, tok_rows), 0))
        t = iota((tok_rows, tok_rows), 1)
        pick = jnp.where(p == t, 1.0, 0.0).astype(jnp.bfloat16)

        def piece(index, carry):
            at = pl.ds(pl.multiple_of(index * 256, 256), 256)
            tok_turned[:, at] = jnp.dot(
                pick, tok_in[:, at], preferred_element_type=jnp.float32
            ).astype(jnp.bfloat16)
            return carry

        lax.fori_loop(0, depth // 256, piece, 0)

    def project(a, store):
        def piece(index, carry):
            both = pl.ds(pl.multiple_of(index * 2 * block, 2 * block), 2 * block)
            whole = jnp.dot(tok_turned[both, :], weights[a], preferred_element_type=jnp.float32)
            for k in range(2):
                rows = pl.ds(pl.multiple_of((2 * index + k) * block, block), block)
                for g in range(GROUPS):
                    part = whole[k * block : (k + 1) * block, g * DH : (g + 1) * DH]
                    if a != 1:
                        part = part * cosine[rows, :] + pltpu.roll(part, DH // 2, 1) * sine[rows, :]
                    store(2 * index + k, rows, g, part)
            return carry

        lax.fori_loop(0, SECOND_DILATION // 2, piece, 0, unroll=2)

    def keep_pair(which):
        def store(index, rows, g, part):
            if g == 2:
                far2[4 + c, which, rows, :] = part.astype(jnp.bfloat16)
            elif g == 1:
                near_own[which, rows, :] = part.astype(jnp.bfloat16)
            else:
                pair0[which, rows, :] = part.astype(jnp.bfloat16)
                per = tail // THIRD_DILATION
                ends = jnp.concatenate(
                    [part[b * sub + sub - per : (b + 1) * sub] for b in range(4)], axis=0
                )
                at = pl.ds(pl.multiple_of(tok_rows + index * 4 * per, 4 * per), 4 * per)
                near_own[which, at, :] = ends.astype(jnp.bfloat16)

        return store

    def keep_query(index, rows, g, part):
        queries[g, rows, :] = part.astype(jnp.bfloat16)

    def others(a):
        for zz in range(nz):
            s = 2 * zz + 1 - c
            send(chunk(a, s), chunk(a, s), side_s.at[a, zz], w_r.at[a, s], side).wait_recv()

    def far(kind, src, dst, where):
        return send(far2.at[src], far2.at[dst], far_s.at[kind], far_r.at[dst], where)

    gives_up, takes_up = z < last - 1, (z > 0) & (z < last)
    helps, asks = z == last - 1, z == last

    def own_side():
        return far(0, 4 + c, 4 + c, side)

    def own_up():
        return far(1, 4 + c, 2 + c, above)

    def pass_side(kind, slot):
        return far(kind, slot, slot, side)

    def pass_up():
        return far(3, 2 + c, c, above)

    def near(where):
        return send(near_own, near_in, near_s, near_r, where)

    def halos():
        pl.when(gives_up)(lambda: own_up().start())
        pl.when(has_up & (c == 1))(lambda: near(up_other).start())
        pl.when(c == 0)(lambda: near(side).start())
        pl.when((c == 0) | helps)(lambda: own_side().start())

    def ask():
        return send(queries.at[2], asked, part_s.at[0], part_r.at[0], below)

    def answer():
        return send(part, got_part, part_s.at[1], part_r.at[1], above)

    def answer_log():
        return send(part_log, got_log, part_s.at[2], part_r.at[2], above)

    scale = DH ** (-0.5)
    far_off = 1 << 24

    def dots(q, k):
        return lax.dot_general(q, k, (((1,), (1,)), ((), ())), preferred_element_type=jnp.float32)

    def soft(scores, time_q, time_k, reach, first):
        gap = time_q - jnp.where(time_k >= first, time_k, far_off)
        scores = jnp.where((gap >= 0) & (gap <= reach), scores * scale, -jnp.inf)
        top = jnp.max(scores, axis=-1, keepdims=True)
        weight = jnp.exp(scores - top)
        return top, jnp.sum(weight, axis=-1, keepdims=True), weight.astype(jnp.bfloat16)

    def near_groups():
        def piece(index, carry):
            begin = index * block
            rows = pl.ds(pl.multiple_of(begin, block), block)
            q = queries[0, rows, :]
            tails = pl.ds(tok_rows, tail)
            scores = jnp.concatenate([dots(q, near_in[0, tails, :]), dots(q, pair0[0])], axis=1)
            lane = iota((1, tail + tok_rows), 1)
            time_k = jnp.where(lane < tail, tail_time(lane & (tail - 1)), row_time(lane - tail))
            time_q = row_time(iota((block, 1), 0) + begin)
            top0, sum0, weight = soft(scores, time_q, time_k, WIN1, -rank * tok_rows)
            got0 = jnp.dot(weight[:, :tail], near_in[1, tails, :], preferred_element_type=jnp.float32)
            got0 += jnp.dot(weight[:, tail:], pair0[1], preferred_element_type=jnp.float32)
            q = queries[1, rows, :]
            scores = jnp.concatenate(
                [dots(q, near_in[0, rows, :]), dots(q, near_own[0, rows, :])], axis=1
            )

            def step_of(place):
                return 4 * (place & (sub - 1)) + (place >> sub_log)

            lane = iota((1, 2 * block), 1)
            step_k = step_of(lane & (block - 1)) + jnp.where(lane < block, -block, 0)
            top1, sum1, weight = soft(
                scores, step_of(iota((block, 1), 0)), step_k, WIN2 // SECOND_DILATION, -rank * block
            )
            got1 = jnp.dot(weight[:, :block], near_in[1, rows, :], preferred_element_type=jnp.float32)
            got1 += jnp.dot(weight[:, block:], near_own[1, rows, :], preferred_element_type=jnp.float32)
            top = jnp.maximum(top0, top1)
            f0, f1 = jnp.exp(top0 - top), jnp.exp(top1 - top)
            got01[rows, :] = f0 * got0 + f1 * got1
            top01[rows, :] = top
            sum01[rows, :] = f0 * sum0 + f1 * sum1
            return carry

        lax.fori_loop(0, SECOND_DILATION, piece, 0, unroll=4)

    def far_piece(index, source, slots, reach_back, first, until=None):
        begin = index * block

        def rows_of(b):
            return pl.ds(pl.multiple_of(begin + b * sub, sub), sub)

        all_scores = []
        for b in range(4):
            keys = jnp.concatenate([far2[slot, 0, rows_of(b), :] for slot in slots], axis=0)
            all_scores.append(dots(source[rows_of(b), :], keys))
        scores = jnp.concatenate(all_scores, axis=0)
        step_q = iota((block, 1), 0) & (sub - 1)
        step_k = iota((1, len(slots) * sub), 1) - reach_back * sub
        seen = step_k if until is None else jnp.where(step_k < until, step_k, far_off)
        top, total, weight = soft(scores, step_q, seen, WIN3 // THIRD_DILATION, first)
        got = []
        for b in range(4):
            vals = jnp.concatenate([far2[slot, 1, rows_of(b), :] for slot in slots], axis=0)
            got.append(
                jnp.dot(weight[b * sub : (b + 1) * sub], vals, preferred_element_type=jnp.float32)
            )
        return top, total, jnp.concatenate(got, axis=0)

    def eye():
        return iota((block, block), 0) == iota((block, block), 1)

    def block_rows(index):
        return pl.ds(pl.multiple_of(index * block, block), block)

    def help_above():
        slots = [2 + c, 3 + c, 4 + c, 5]

        def piece(index, carry):
            top, total, got = far_piece(index, asked, slots, 4, -4 * sub, -c * sub)
            part[block_rows(index), :] = (got / total).astype(jnp.bfloat16)
            row = jnp.sum(jnp.where(eye(), top + jnp.log(total), 0.0), axis=0, keepdims=True)
            part_log[index] = jnp.broadcast_to(row, part_log.shape[1:])
            return carry

        lax.fori_loop(0, SECOND_DILATION, piece, 0, unroll=4)

    def settle(rows, top2, sum2, got2):
        top1 = top01[rows, :]
        top = jnp.maximum(top1, top2)
        f1, f2 = jnp.exp(top1 - top), jnp.exp(top2 - top)
        total = f1 * sum01[rows, :] + f2 * sum2
        mine[0, rows, :] = ((f1 * got01[rows, :] + f2 * got2) / total).astype(jnp.bfloat16)

    def far_here():
        slots = [4 + c - d for d in (4, 3, 2, 1, 0)]

        def piece(index, carry):
            settle(block_rows(index), *far_piece(index, queries.at[2], slots, 4, -rank * sub))
            return carry

        lax.fori_loop(0, SECOND_DILATION, piece, 0, unroll=4)

    def far_asked():
        slots = [3 + c, 4 + c]

        def piece(index, carry):
            rows = block_rows(index)
            top_a, sum_a, got_a = far_piece(index, queries.at[2], slots, 1, -c * sub)
            top_b = jnp.sum(jnp.where(eye(), got_log[index, 0:1, :], 0.0), axis=1, keepdims=True)
            top2 = jnp.maximum(top_a, top_b)
            fa, fb = jnp.exp(top_a - top2), jnp.exp(top_b - top2)
            got2 = fa * got_a + fb * got_part[rows, :].astype(jnp.float32)
            settle(rows, top2, fa * sum_a + fb, got2)
            return carry

        lax.fori_loop(0, SECOND_DILATION, piece, 0, unroll=4)

    def unturn():
        t = iota((tok_rows, tok_rows), 0)
        p = row_time(iota((tok_rows, tok_rows), 1))
        mine[1] = jnp.dot(
            jnp.where(p == t, 1.0, 0.0).astype(jnp.bfloat16), mine[0], preferred_element_type=jnp.float32
        ).astype(jnp.bfloat16)

    head = 2 * x + y
    quarter = tok_rows // 4

    def deal(k):
        return send(
            mine.at[1, pl.ds(k * quarter, quarter), :], heads_in.at[head], head_s.at[k], head_r.at[head], (rank, k)
        )

    def deal_self(k):
        return pltpu.make_async_copy(mine.at[1, pl.ds(k * quarter, quarter), :], heads_in.at[head], head_r.at[head])

    def turn_tokens():
        pl.when(stays)(lambda: tok_kept().wait())

        @pl.when(moves)
        def _():
            for q in range(pieces):
                t_x(1 - x, q).wait_recv()

        order()

    def key_value(which):
        others(which)
        project(which, keep_pair(which))

    def query():
        others(2)
        project(2, keep_query)

    def last_down(layer):
        if 0 < layer < last:
            go(downward[2], layer, "down").start()

    def turn():
        lax.fori_loop(0, SECOND_DILATION, angles, 0)
        turn_tokens()

    def moves_pass(q):
        pl.when(moves)(lambda: pass_token(q))

    def run_end(layer):
        begin(layer)
        o_relay(layer, 1)
        todo = events(layer)
        moves_pass(0)
        moves_pass(1)
        pl.when(stays)(turn)
        handle(layer, todo[0])
        moves_pass(2)
        handle(layer, todo[1])
        moves_pass(3)
        handle(layer, todo[2])
        pl.when(moves)(turn)
        if layer == 0:
            key_value(0)
        else:
            query()
            ask().start()
        o_relay(layer, 2)
        for event in todo[3:6]:
            handle(layer, event)
        o_relay(layer, 3)
        o_share(0).start()
        if layer == 0:
            key_value(1)
            halos()
        else:
            key_value(0)
        o_share(0).wait()
        o_share(1).start()
        for event in todo[6:]:
            handle(layer, event)
        if layer == 0:
            query()
        else:
            key_value(1)
            halos()

    def run_mid(layer):
        begin(layer)
        o_relay(layer, 1)
        todo = events(layer)
        split = 9 if layer == last - 1 else 7
        downs = [i for i, event in enumerate(todo) if event[1:3] == ("down", downward[1])]
        for i in range(split):
            handle(layer, todo[i])
            if i < 4:
                moves_pass(i)
            if i == 1:
                pl.when(stays)(turn)
            if i == 3:
                o_relay(layer, 2)
            if layer == last - 1 and i == max(downs):
                last_down(layer)
        late = todo[split:]

        def finish():
            if late:
                last_down(layer)
            for event in late:
                handle(layer, event)

        o_share(0).start()
        pl.when(moves)(finish)
        pl.when(moves)(turn)
        key_value(0)
        key_value(1)
        halos()
        o_share(0).wait()
        o_share(1).start()
        pl.when(stays)(finish)
        query()

    def run(layer):
        (run_mid if 0 < layer < last else run_end)(layer)

    for layer in range(nz):
        pl.when(z == layer)(functools.partial(run, layer))

    for slot in range(4):
        @pl.when((2 * z + slot < 4) | (asks & (c == 0) & (slot == 3)))
        def _(slot=slot):
            far2[slot] = jnp.zeros(far2.shape[1:], far2.dtype)

    @pl.when(rank == 0)
    def _():
        near_in[...] = jnp.zeros(near_in.shape, near_in.dtype)

    @pl.when(takes_up)
    def _():
        own_up().wait_recv()
        pl.when(gives_up)(lambda: pass_up().start())
        pass_side(2, 2 + c).start()

    pl.when(c == 1)(lambda: pass_side(0, 4).wait_recv())

    @pl.when(helps)
    def _():
        pl.when(c == 0)(lambda: pass_side(0, 5).wait_recv())
        pass_side(2, 3 - c).wait_recv()
        ask().wait_recv()
        help_above()
        answer().start()
        answer_log().start()

    pl.when(rank >= 1)(lambda: near(side).wait_recv())
    near_groups()
    o_share(1).wait()
    o_share(2).start()

    @pl.when(helps)
    def _():
        pass_up().wait_recv()
        pl.when(c == 1)(lambda: pass_side(4, 1).start())
        pl.when(c == 0)(lambda: pass_side(4, 1).wait_recv())

    pl.when(takes_up & gives_up)(lambda: pass_side(2, 3 - c).wait_recv())

    @pl.when(asks)
    def _():
        answer().wait_recv()
        answer_log().wait_recv()
        far_asked()

    pl.when(jnp.logical_not(asks))(far_here)
    unturn()
    for k in range(4):
        self_here = stays & (tp == k)
        pl.when(self_here)(lambda k=k: deal_self(k).start())
        pl.when(jnp.logical_not(self_here))(lambda k=k: deal(k).start())

    o_share(2).wait()
    for h in range(4):
        pltpu.make_async_copy(heads_in.at[h], heads_in.at[h], head_r.at[h]).wait()
    merged = jnp.concatenate([heads_in[h] for h in range(4)], axis=1)
    width = w_out.shape[1]
    for zz in range(nz):
        for yy in range(2):
            rows = jnp.concatenate([out_rows[h % 2, yy, h // 2, zz] for h in range(4)], axis=0)
            s = 2 * zz + yy
            out[:, s * width : (s + 1) * width] = jnp.dot(
                merged, rows, preferred_element_type=jnp.float32
            ).astype(jnp.bfloat16)

    for k in range(4):
        pl.when(jnp.logical_not(stays & (tp == k)))(lambda k=k: deal(k).wait_send())

    @pl.when(moves)
    def _():
        for a in range(3):
            swapped(a).wait_send()
        for q in range(pieces):
            t_y(q).wait_send()
            t_x(x, q).wait_send()

    for a in range(4):
        for zz in range(nz):
            pl.when(has_up & (zz <= z))(lambda a=a, zz=zz: go(a, zz, "up").wait_send())
            pl.when(has_down & (zz >= z))(lambda a=a, zz=zz: go(a, zz, "down").wait_send())
            if a < 3:
                go(a, zz, "side").wait_send()
    pl.when((c == 0) | has_up)(lambda: near(side).wait_send())
    pl.when((c == 0) | helps)(lambda: own_side().wait_send())
    pl.when(gives_up)(lambda: own_up().wait_send())
    pl.when(takes_up)(lambda: pass_side(2, 2 + c).wait_send())
    pl.when(takes_up & gives_up)(lambda: pass_up().wait_send())
    pl.when(helps & (c == 1))(lambda: pass_side(4, 1).wait_send())
    pl.when(asks)(lambda: ask().wait_send())

    @pl.when(helps)
    def _():
        answer().wait_send()
        answer_log().wait_send()


def fits_kernel(n_sp, n_tp, tokens, w_query, w_out):
    tok_rows, depth = tokens.shape
    return (
        n_sp == 2 * LAYERS
        and n_tp == 4
        and w_query.shape[1] == GROUPS * DH
        and w_out.shape[0] == DH
        and w_out.shape[1] % 128 == 0
        and w_query.shape[0] % 16 == 0
        and tok_rows == WIN2
        and 4 * tok_rows == WIN3
        and 4 * WIN1 == tok_rows
    )


def one_kernel(n_sp, tokens, w_query, w_key, w_value, w_out):
    nz = n_sp // 2
    tok_rows, depth = tokens.shape
    cols = w_query.shape[1]
    bf, dma = jnp.bfloat16, pltpu.SemaphoreType.DMA
    return pl.pallas_call(
        functools.partial(layer_kernel, nz),
        out_shape=jax.ShapeDtypeStruct((tok_rows // 4, w_out.shape[1] * n_sp), bf),
        in_specs=[pl.BlockSpec(memory_space=pltpu.HBM)] * 5,
        out_specs=pl.BlockSpec(memory_space=pltpu.VMEM),
        scratch_shapes=[
            pltpu.VMEM((3, depth, cols), bf),
            pltpu.VMEM((3, *w_query.shape), bf),
            pltpu.VMEM((tok_rows, depth), bf),
            pltpu.VMEM((tok_rows, depth), bf),
            pltpu.VMEM((tok_rows, DH), jnp.float32),
            pltpu.VMEM((tok_rows, DH), jnp.float32),
            pltpu.VMEM((GROUPS, tok_rows, DH), bf),
            pltpu.VMEM((2, tok_rows, DH), bf),
            pltpu.VMEM((2, tok_rows + WIN1, DH), bf),
            pltpu.VMEM((2, tok_rows + WIN1, DH), bf),
            pltpu.VMEM((6, 2, tok_rows, DH), bf),
            pltpu.VMEM((2, 2, 2, nz, *w_out.shape), bf),
            pltpu.VMEM((2, tok_rows, DH), bf),
            pltpu.VMEM((4, tok_rows // 4, DH), bf),
            pltpu.VMEM((tok_rows, DH), jnp.float32),
            pltpu.VMEM((tok_rows, 1), jnp.float32),
            pltpu.VMEM((tok_rows, 1), jnp.float32),
            pltpu.VMEM((tok_rows, DH), bf),
            pltpu.VMEM((tok_rows, DH), bf),
            pltpu.VMEM((SECOND_DILATION, 8, DH), jnp.float32),
            pltpu.VMEM((tok_rows, DH), bf),
            pltpu.VMEM((SECOND_DILATION, 8, DH), jnp.float32),
            dma((3,)), dma((3,)), dma, dma((2, 4)), dma((4,)), dma((4,)), dma((3, n_sp)), dma((4, nz)), dma((4, nz)), dma((3, nz)),
            dma((nz,)), dma((3,)), dma((3,)),
            dma((5,)), dma((6,)), dma, dma, dma((4,)), dma((4,)), dma((3,)), dma((3,)),
        ],
        compiler_params=pltpu.CompilerParams(
            collective_id=0, has_side_effects=True, vmem_limit_bytes=60 * 1024 * 1024
        ),
    )(tokens, w_key, w_value, w_query, w_out)


def on_mesh(n_sp, n_tp, *operands):
    tokens, w_query, _, _, w_out = operands
    if fits_kernel(n_sp, n_tp, tokens, w_query, w_out):
        return one_kernel(n_sp, *operands)
    return on_device(*operands)


def solution(mesh):
    placed = (P("sp", None), P("sp", "tp"), P("sp", "tp"), P("sp", "tp"), P("tp", "sp"))
    body = functools.partial(on_mesh, mesh.shape["sp"], mesh.shape["tp"])
    return jax.shard_map(
        body, mesh=mesh, in_specs=placed, out_specs=P(("sp", "tp"), None), check_vma=False
    )
```

```python
import functools
import math

import jax
import jax.numpy as jnp
from jax import lax
from jax.experimental import pallas as pl
from jax.experimental.pallas import tpu as pltpu
from jax.sharding import PartitionSpec as P

GROUPS = 3
DH = 128
WIN1 = 128
WIN2 = 512
WIN3 = 2048
SECOND_DILATION = 4
THIRD_DILATION = 16


ROPE_BASE = 500000.0

LAYERS = 4


def from_behind(block, axis, distance):
    devices = range(lax.axis_size(axis))
    route = [(i - distance, i) for i in devices if i - distance in devices]
    return lax.ppermute(block, axis, route)


def rotate(projected, offset):
    tok_rows = projected.shape[0]
    head_size = projected.shape[-1]
    half_size = head_size // 2
    positions = (offset + jnp.arange(tok_rows, dtype=jnp.int32)).astype(jnp.float32)
    frequency = 1.0 / ROPE_BASE ** (jnp.arange(0, head_size, 2, dtype=jnp.float32) / head_size)
    angles = (positions[:, None] * frequency[None, :]).reshape(tok_rows, 1, 1, half_size)
    cosine = jnp.cos(angles)
    sine_part = jnp.sin(angles)
    first_half = projected[..., :half_size]
    second_half = projected[..., half_size:]
    return jnp.concatenate(
        [
            first_half * cosine - second_half * sine_part,
            second_half * cosine + first_half * sine_part,
        ],
        axis=-1,
    )


def window_attend(query_part, buffer, steps, stride, offset):
    tok_rows, heads_here, head_size = query_part.shape
    sub_rows = tok_rows // stride
    key_rows = buffer.shape[1] // stride
    query_sub = query_part.reshape(sub_rows, stride, heads_here, head_size).transpose(1, 2, 0, 3)
    pair_sub = buffer.reshape(2, key_rows, stride, heads_here, head_size).transpose(0, 2, 3, 1, 4)
    block_rows = math.gcd(sub_rows, steps) if sub_rows > steps else sub_rows
    block_list = sub_rows // block_rows
    query_blocks = query_sub.reshape(stride, heads_here, block_list, block_rows, head_size)
    key_blocks = jnp.stack(
        [
            pair_sub[:, :, :, index * block_rows : index * block_rows + block_rows + steps]
            for index in range(block_list)
        ],
        axis=3,
    )
    scores = jnp.einsum(
        "zhnqe,zhnke->zhnqk", query_blocks, key_blocks[0], preferred_element_type=jnp.float32
    ) * head_size ** (-0.5)
    query_index = (jnp.arange(block_list, dtype=jnp.int32) * block_rows)[
        :, None, None
    ] + jnp.arange(block_rows, dtype=jnp.int32)[None, :, None]
    key_index = (jnp.arange(block_list, dtype=jnp.int32) * block_rows)[:, None, None] + jnp.arange(
        block_rows + steps, dtype=jnp.int32
    )[None, None, :]
    spacing = query_index + steps - key_index
    residue = jnp.arange(stride, dtype=jnp.int32)[:, None, None, None]
    key_position = offset + (key_index[None] - steps) * stride + residue
    allowed = (spacing[None] >= 0) & (spacing[None] <= steps) & (key_position >= 0)
    scores = jnp.where(allowed[:, None], scores, -jnp.inf)
    row_max = jnp.max(scores, axis=-1)
    exponent = jnp.exp(scores - row_max[..., None])
    totals = jnp.sum(exponent, axis=-1)
    probs = (exponent / totals[..., None]).astype(jnp.bfloat16)
    mixed = jnp.einsum(
        "zhnqk,zhnke->zhnqe", probs, key_blocks[1], preferred_element_type=jnp.float32
    )
    mixed = mixed.reshape(stride, heads_here, sub_rows, head_size).transpose(2, 0, 1, 3)
    log_total = (row_max + jnp.log(totals)).reshape(stride, heads_here, sub_rows).transpose(2, 0, 1)
    return (mixed.reshape(tok_rows, heads_here, head_size), log_total.reshape(tok_rows, heads_here))


def reach_back(key_value, distance_max):
    tok_rows = key_value.shape[1]
    gathered = key_value
    pieces_held = 1
    while pieces_held < distance_max + 1:
        slice_share = min(pieces_held, distance_max + 1 - pieces_held)
        arrived = from_behind(
            gathered[:, gathered.shape[1] - slice_share * tok_rows :], "sp", pieces_held
        )
        gathered = jnp.concatenate([arrived, gathered], axis=1)
        pieces_held = pieces_held + slice_share
    return gathered


def on_device(tokens, w_query, w_key, w_value, w_out):
    tok_rows = tokens.shape[0]
    heads_here = w_out.shape[0] // DH
    offset = lax.axis_index("sp") * tok_rows
    weight_parts = (
        lax.all_gather(w_query, "sp", axis=0, tiled=True),
        lax.all_gather(w_key, "sp", axis=0, tiled=True),
        lax.all_gather(w_value, "sp", axis=0, tiled=True),
    )
    query_raw, key_raw, value_raw = tuple(
        (
            jnp.dot(tokens, weight_rows, preferred_element_type=jnp.float32)
            for weight_rows in weight_parts
        )
    )
    head_shape = (tok_rows, heads_here, GROUPS, DH)
    queries = rotate(query_raw.reshape(head_shape), offset).astype(jnp.bfloat16)
    keys_all = rotate(key_raw.reshape(head_shape), offset).astype(jnp.bfloat16)
    values_all = value_raw.astype(jnp.bfloat16).reshape(head_shape)
    windows = (WIN1, WIN2, WIN3)
    step_sizes = (1, SECOND_DILATION, THIRD_DILATION)
    outputs = []
    log_totals = []
    for group_index in range(GROUPS):
        key_value = jnp.stack([keys_all[:, :, group_index], values_all[:, :, group_index]])
        key_value = key_value.reshape(2, tok_rows, heads_here * DH)
        window = windows[group_index]
        if group_index == 0:
            near_rows = from_behind(key_value[:, tok_rows - window :], "sp", 1)
            buffer = jnp.concatenate([near_rows, key_value], axis=1)
        else:
            distance_max = (window + tok_rows - 1) // tok_rows
            buffer = reach_back(key_value, distance_max)
        group_out, log_total = window_attend(
            queries[:, :, group_index],
            buffer,
            window // step_sizes[group_index],
            step_sizes[group_index],
            offset,
        )
        outputs.append(group_out)
        log_totals.append(log_total)
    group_weights = jax.nn.softmax(jnp.stack(log_totals), axis=0)
    merged = jnp.sum(group_weights[..., None] * jnp.stack(outputs), axis=0).astype(jnp.bfloat16)
    merged = merged.reshape(tok_rows, heads_here * DH)
    w_whole = lax.all_gather(w_out, "sp", axis=1, tiled=True)
    return lax.psum_scatter(
        jnp.dot(merged, w_whole, preferred_element_type=jnp.float32).astype(jnp.bfloat16),
        "tp",
        scatter_dimension=0,
        tiled=True,
    )


def layer_kernel(
    nz,
    tokens, w_key, w_value, w_query, w_out, out,
    weights, stage, tok_in, tok_turned, cosine, sine, queries, pair0, near_own, near_in, far2,
    out_rows, mine, heads_in, got01, top01, sum01, asked, part, part_log, got_part, got_log, begun,
    stage_s, swap_s, tok_k, t_r, ty_s, tx_s, w_r, up_s, down_s, side_s, o_r, o_s, o_r2, far_s, far_r, near_s, near_r, head_s, head_r, part_s, part_r,
):
    tok_rows, depth = tokens.shape
    k_rows, cols = w_key.shape
    sub = tok_rows // THIRD_DILATION
    sub_log = sub.bit_length() - 1
    block = tok_rows // SECOND_DILATION
    tail = WIN1
    last = nz - 1
    sp, tp = lax.axis_index("sp"), lax.axis_index("tp")
    z, y = sp // 2, sp % 2
    x, c = tp // 2, tp % 2
    rank = 2 * z + c
    stays = c == y
    moves = jnp.logical_not(stays)
    has_up, has_down = z < last, z > 0
    side = (sp, 2 * x + 1 - c)
    across_x = (sp, 2 * (1 - x) + c)
    across_y = (2 * z + 1 - y, tp)
    partner = (2 * z + 1 - y, 2 * x + 1 - c)
    above, below = (sp + 2, tp), (sp - 2, tp)
    up_other = (sp + 2, 2 * x)

    def send(src, dst, s_sem, r_sem, where):
        return pltpu.make_async_remote_copy(
            src_ref=src, dst_ref=dst, send_sem=s_sem, recv_sem=r_sem,
            device_id=where, device_id_type=pl.DeviceIdType.MESH,
        )

    parts = (w_key, w_value, w_query)
    upward, downward = (2, 0, 1), (0, 1, 2)

    def chunk(a, s):
        return weights.at[a, pl.ds(pl.multiple_of(s * k_rows, k_rows), k_rows), :]

    def o_chunk(zz):
        return out_rows.at[c, y, x, zz]

    def kept(a):
        return pltpu.make_async_copy(parts[a], chunk(a, rank), w_r.at[a, rank])

    def staged(a):
        return pltpu.make_async_copy(parts[a], stage.at[a], stage_s.at[a])

    def swapped(a):
        there = 2 * z + 1 - c
        return send(stage.at[a], chunk(a, there), swap_s.at[a], w_r.at[a, there], partner)

    def tok_kept():
        return pltpu.make_async_copy(tokens, tok_in, tok_k)

    pieces = ty_s.shape[0]
    piece_rows = tok_rows // 2 // pieces

    def piece_at(half, q):
        return pl.ds(pl.multiple_of(half * (tok_rows // 2) + q * piece_rows, piece_rows), piece_rows)

    def t_y(q):
        at = piece_at(x, q)
        return send(tokens.at[at, :], tok_in.at[at, :], ty_s.at[q], t_r.at[x, q], partner)

    def t_x(half, q):
        at = piece_at(half, q)
        return send(tok_in.at[at, :], tok_in.at[at, :], tx_s.at[q], t_r.at[half, q], across_x)

    def pass_token(q):
        t_y(q).wait_recv()
        t_x(x, q).start()

    def o_kept():
        return pltpu.make_async_copy(w_out, o_chunk(z), o_r.at[z])

    o_kept().start()

    @pl.when(stays)
    def _():
        for a in (2, 0, 1):
            kept(a).start()
        tok_kept().start()

    @pl.when(moves)
    def _():
        for a in (2, 0, 1):
            staged(a).start()

    barrier = pltpu.get_barrier_semaphore()

    def greet(where):
        pl.semaphore_signal(barrier, inc=1, device_id=where, device_id_type=pl.DeviceIdType.MESH)

    for dy in range(2):
        for dx in range(2):
            for dc in range(2):
                if dy + dx + dc:
                    greet((2 * z + (y + dy) % 2, 2 * ((x + dx) % 2) + (c + dc) % 2))
    pl.when(has_up)(lambda: greet(above))
    pl.when(has_down)(lambda: greet(below))
    pl.when(has_up & (c == 1))(lambda: greet(up_other))
    pl.when(has_down & (c == 0))(lambda: greet((sp - 2, 2 * x + 1)))
    pl.semaphore_wait(barrier, 7 + jnp.where(has_up, 1 + c, 0) + jnp.where(has_down, 2 - c, 0))

    def go(a, zz, kind):
        s = 2 * zz + c
        ref = chunk(a, s) if a < 3 else o_chunk(zz)
        r_sem = w_r.at[a, s] if a < 3 else o_r.at[zz]
        s_sem = {"up": up_s, "down": down_s, "side": side_s}[kind].at[a, zz]
        return send(ref, ref, s_sem, r_sem, {"up": above, "down": below, "side": side}[kind])

    def swap_order(layer):
        return {0: (2, 0, 1), last: (0, 1, 2)}.get(layer, (0, 2, 1))

    @pl.when(moves)
    def _():
        for layer in range(nz):
            @pl.when(z == layer)
            def _(layer=layer):
                for a in swap_order(layer):
                    staged(a).wait()
                    swapped(a).start()
        for q in range(pieces):
            t_y(q).start()

    def o_relay(layer, d):
        if layer - d >= 0:
            go(3, layer - d, "up").wait_recv()
            if layer < last:
                go(3, layer - d, "up").start()
        if layer + d < nz:
            go(3, layer + d, "down").wait_recv()
            if layer > 0:
                go(3, layer + d, "down").start()

    def o_share(axis):
        ref, where = (
            (out_rows.at[c, y, x], across_x),
            (out_rows.at[c, y], across_y),
            (out_rows.at[c], side),
        )[axis]
        return send(ref, ref, o_s.at[axis], o_r2.at[axis], where)

    def events(layer):
        listed = []
        for i in range(3):
            for d in range(1, layer + 1):
                listed.append((i * layer + d, "up", upward[i], layer - d, d))
            for d in range(1, last - layer + 1):
                listed.append((i * (last - layer) + d, "down", downward[i], layer + d, d))
        return sorted(listed)

    def handle(layer, event):
        _, kind, a, zz, d = event
        go(a, zz, kind).wait_recv()
        if kind == "up":
            if layer < last:
                go(a, zz, "up").start()
            if d == layer and a == upward[1] and layer < last:
                go(upward[2], layer, "up").start()
        else:
            if layer > 0:
                go(a, zz, "down").start()
        go(a, zz, "side").start()

    def begin(layer):
        o_kept().wait()
        if layer < last:
            go(3, layer, "up").start()
        if layer > 0:
            go(3, layer, "down").start()
        for a in swap_order(layer):
            pl.when(stays)(lambda a=a: kept(a).wait())
            pl.when(moves)(lambda a=a: go(a, layer, "side").wait_recv())
            if layer < last and (layer == 0 or a != upward[2]):
                go(a, layer, "up").start()
            if layer > 0 and (layer == last or a != downward[2]):
                go(a, layer, "down").start()
            go(a, layer, "side").start()

    def row_time(p):
        b, i = p >> sub_log, p & (sub - 1)
        return THIRD_DILATION * i + (b >> 2) + SECOND_DILATION * (b & 3)

    def tail_time(u):
        per = tail // THIRD_DILATION
        b, i = u >> (per.bit_length() - 1), u & (per - 1)
        return THIRD_DILATION * (sub - per + i) + (b >> 2) + SECOND_DILATION * (b & 3) - tok_rows

    def iota(shape, axis):
        return lax.broadcasted_iota(jnp.int32, shape, axis)

    def angles(index, carry):
        at = index * block
        rows = pl.ds(pl.multiple_of(at, block), block)
        pair_at = iota((1, DH), 1) & (DH // 2 - 1)
        freq = jnp.exp(pair_at.astype(jnp.float32) * (-2.0 * math.log(ROPE_BASE) / DH))
        angle = (row_time(iota((block, DH), 0) + at) + rank * tok_rows).astype(jnp.float32) * freq
        cosine[rows, :] = jnp.cos(angle)
        turned = jnp.sin(angle)
        sine[rows, :] = jnp.where(iota((block, DH), 1) < DH // 2, -turned, turned)
        return carry

    def order():
        p = row_time(iota((tok_rows, tok_rows), 0))
        t = iota((tok_rows, tok_rows), 1)
        pick = jnp.where(p == t, 1.0, 0.0).astype(jnp.bfloat16)

        def piece(index, carry):
            at = pl.ds(pl.multiple_of(index * 256, 256), 256)
            tok_turned[:, at] = jnp.dot(
                pick, tok_in[:, at], preferred_element_type=jnp.float32
            ).astype(jnp.bfloat16)
            return carry

        lax.fori_loop(0, depth // 256, piece, 0)

    def product(both, a, span):
        return jnp.dot(tok_turned[both, span], weights[a, span, :], preferred_element_type=jnp.float32)

    def start_product(a, span):
        def piece(index, carry):
            both = pl.ds(pl.multiple_of(index * 2 * block, 2 * block), 2 * block)
            begun[both, :] = product(both, a, span)
            return carry

        lax.fori_loop(0, SECOND_DILATION // 2, piece, 0, unroll=2)

    def project(a, store, rest=None):
        def piece(index, carry):
            both = pl.ds(pl.multiple_of(index * 2 * block, 2 * block), 2 * block)
            whole = product(both, a, slice(0, depth) if rest is None else rest)
            if rest is not None:
                whole = whole + begun[both, :]
            for k in range(2):
                rows = pl.ds(pl.multiple_of((2 * index + k) * block, block), block)
                for g in range(GROUPS):
                    part = whole[k * block : (k + 1) * block, g * DH : (g + 1) * DH]
                    if a != 1:
                        part = part * cosine[rows, :] + pltpu.roll(part, DH // 2, 1) * sine[rows, :]
                    store(2 * index + k, rows, g, part)
            return carry

        lax.fori_loop(0, SECOND_DILATION // 2, piece, 0, unroll=2)

    def keep_pair(which):
        def store(index, rows, g, part):
            if g == 2:
                far2[4 + c, which, rows, :] = part.astype(jnp.bfloat16)
            elif g == 1:
                near_own[which, rows, :] = part.astype(jnp.bfloat16)
            else:
                pair0[which, rows, :] = part.astype(jnp.bfloat16)
                per = tail // THIRD_DILATION
                ends = jnp.concatenate(
                    [part[b * sub + sub - per : (b + 1) * sub] for b in range(4)], axis=0
                )
                at = pl.ds(pl.multiple_of(tok_rows + index * 4 * per, 4 * per), 4 * per)
                near_own[which, at, :] = ends.astype(jnp.bfloat16)

        return store

    def keep_query(index, rows, g, part):
        queries[g, rows, :] = part.astype(jnp.bfloat16)

    def others(a, layers=None):
        for zz in range(nz) if layers is None else layers:
            s = 2 * zz + 1 - c
            send(chunk(a, s), chunk(a, s), side_s.at[a, zz], w_r.at[a, s], side).wait_recv()

    def far(kind, src, dst, where):
        return send(far2.at[src], far2.at[dst], far_s.at[kind], far_r.at[dst], where)

    gives_up, takes_up = z < last - 1, (z > 0) & (z < last)
    helps, asks = z == last - 1, z == last

    def own_side():
        return far(0, 4 + c, 4 + c, side)

    def own_up():
        return far(1, 4 + c, 2 + c, above)

    def pass_side(kind, slot):
        return far(kind, slot, slot, side)

    def pass_up():
        return far(3, 2 + c, c, above)

    def near(where):
        return send(near_own, near_in, near_s, near_r, where)

    def halos():
        pl.when(gives_up)(lambda: own_up().start())
        pl.when(has_up & (c == 1))(lambda: near(up_other).start())
        pl.when(c == 0)(lambda: near(side).start())
        pl.when((c == 0) | helps)(lambda: own_side().start())

    def ask():
        return send(queries.at[2], asked, part_s.at[0], part_r.at[0], below)

    def answer():
        return send(part, got_part, part_s.at[1], part_r.at[1], above)

    def answer_log():
        return send(part_log, got_log, part_s.at[2], part_r.at[2], above)

    scale = DH ** (-0.5)
    far_off = 1 << 24

    def dots(q, k):
        return lax.dot_general(q, k, (((1,), (1,)), ((), ())), preferred_element_type=jnp.float32)

    def soft(scores, time_q, time_k, reach, first):
        gap = time_q - jnp.where(time_k >= first, time_k, far_off)
        scores = jnp.where((gap >= 0) & (gap <= reach), scores * scale, -jnp.inf)
        top = jnp.max(scores, axis=-1, keepdims=True)
        weight = jnp.exp(scores - top)
        return top, jnp.sum(weight, axis=-1, keepdims=True), weight.astype(jnp.bfloat16)

    def near_groups():
        def piece(index, carry):
            both = pl.ds(pl.multiple_of(index * 2 * block, 2 * block), 2 * block)
            q = queries[0, both, :]
            tails = pl.ds(tok_rows, tail)
            scores = jnp.concatenate([dots(q, near_in[0, tails, :]), dots(q, pair0[0])], axis=1)
            lane = iota((1, tail + tok_rows), 1)
            time_k = jnp.where(lane < tail, tail_time(lane & (tail - 1)), row_time(lane - tail))
            time_q = row_time(iota((2 * block, 1), 0) + index * 2 * block)
            tops, sums, weight = soft(scores, time_q, time_k, WIN1, -rank * tok_rows)
            gots = jnp.dot(weight[:, :tail], near_in[1, tails, :], preferred_element_type=jnp.float32)
            gots += jnp.dot(weight[:, tail:], pair0[1], preferred_element_type=jnp.float32)

            def step_of(place):
                return 4 * (place & (sub - 1)) + (place >> sub_log)

            lane = iota((1, 2 * block), 1)
            step_k = step_of(lane & (block - 1)) + jnp.where(lane < block, -block, 0)
            for k in range(2):
                rows = pl.ds(pl.multiple_of((2 * index + k) * block, block), block)
                half = slice(k * block, (k + 1) * block)
                top0, sum0, got0 = tops[half], sums[half], gots[half]
                q = queries[1, rows, :]
                scores = jnp.concatenate(
                    [dots(q, near_in[0, rows, :]), dots(q, near_own[0, rows, :])], axis=1
                )
                top1, sum1, weight = soft(
                    scores, step_of(iota((block, 1), 0)), step_k, WIN2 // SECOND_DILATION, -rank * block
                )
                got1 = jnp.dot(weight[:, :block], near_in[1, rows, :], preferred_element_type=jnp.float32)
                got1 += jnp.dot(weight[:, block:], near_own[1, rows, :], preferred_element_type=jnp.float32)
                top = jnp.maximum(top0, top1)
                f0, f1 = jnp.exp(top0 - top), jnp.exp(top1 - top)
                got01[rows, :] = f0 * got0 + f1 * got1
                top01[rows, :] = top
                sum01[rows, :] = f0 * sum0 + f1 * sum1
            return carry

        lax.fori_loop(0, SECOND_DILATION // 2, piece, 0, unroll=2)

    def far_piece(index, source, slots, reach_back, first, until=None):
        begin = index * block

        def rows_of(b):
            return pl.ds(pl.multiple_of(begin + b * sub, sub), sub)

        all_scores = []
        for b in range(4):
            keys = jnp.concatenate([far2[slot, 0, rows_of(b), :] for slot in slots], axis=0)
            all_scores.append(dots(source[rows_of(b), :], keys))
        scores = jnp.concatenate(all_scores, axis=0)
        step_q = iota((block, 1), 0) & (sub - 1)
        step_k = iota((1, len(slots) * sub), 1) - reach_back * sub
        seen = step_k if until is None else jnp.where(step_k < until, step_k, far_off)
        top, total, weight = soft(scores, step_q, seen, WIN3 // THIRD_DILATION, first)
        got = []
        for b in range(4):
            vals = jnp.concatenate([far2[slot, 1, rows_of(b), :] for slot in slots], axis=0)
            got.append(
                jnp.dot(weight[b * sub : (b + 1) * sub], vals, preferred_element_type=jnp.float32)
            )
        return top, total, jnp.concatenate(got, axis=0)

    def eye():
        return iota((block, block), 0) == iota((block, block), 1)

    def block_rows(index):
        return pl.ds(pl.multiple_of(index * block, block), block)

    def help_above():
        slots = [2 + c, 3 + c, 4 + c, 5]

        def piece(index, carry):
            top, total, got = far_piece(index, asked, slots, 4, -4 * sub, -c * sub)
            part[block_rows(index), :] = (got / total).astype(jnp.bfloat16)
            row = jnp.sum(jnp.where(eye(), top + jnp.log(total), 0.0), axis=0, keepdims=True)
            part_log[index] = jnp.broadcast_to(row, part_log.shape[1:])
            return carry

        lax.fori_loop(0, SECOND_DILATION, piece, 0, unroll=4)

    def settle(rows, top2, sum2, got2):
        top1 = top01[rows, :]
        top = jnp.maximum(top1, top2)
        f1, f2 = jnp.exp(top1 - top), jnp.exp(top2 - top)
        total = f1 * sum01[rows, :] + f2 * sum2
        mine[0, rows, :] = ((f1 * got01[rows, :] + f2 * got2) / total).astype(jnp.bfloat16)

    def far_here():
        slots = [4 + c - d for d in (4, 3, 2, 1, 0)]

        def piece(index, carry):
            settle(block_rows(index), *far_piece(index, queries.at[2], slots, 4, -rank * sub))
            return carry

        lax.fori_loop(0, SECOND_DILATION, piece, 0, unroll=4)

    def far_asked():
        slots = [3 + c, 4 + c]

        def piece(index, carry):
            rows = block_rows(index)
            top_a, sum_a, got_a = far_piece(index, queries.at[2], slots, 1, -c * sub)
            top_b = jnp.sum(jnp.where(eye(), got_log[index, 0:1, :], 0.0), axis=1, keepdims=True)
            top2 = jnp.maximum(top_a, top_b)
            fa, fb = jnp.exp(top_a - top2), jnp.exp(top_b - top2)
            got2 = fa * got_a + fb * got_part[rows, :].astype(jnp.float32)
            settle(rows, top2, fa * sum_a + fb, got2)
            return carry

        lax.fori_loop(0, SECOND_DILATION, piece, 0, unroll=4)

    def unturn():
        t = iota((tok_rows, tok_rows), 0)
        p = row_time(iota((tok_rows, tok_rows), 1))
        mine[1] = jnp.dot(
            jnp.where(p == t, 1.0, 0.0).astype(jnp.bfloat16), mine[0], preferred_element_type=jnp.float32
        ).astype(jnp.bfloat16)

    head = 2 * x + y
    quarter = tok_rows // 4

    def deal(k):
        return send(
            mine.at[1, pl.ds(k * quarter, quarter), :], heads_in.at[head], head_s.at[k], head_r.at[head], (rank, k)
        )

    def deal_self(k):
        return pltpu.make_async_copy(mine.at[1, pl.ds(k * quarter, quarter), :], heads_in.at[head], head_r.at[head])

    def turn_tokens():
        pl.when(stays)(lambda: tok_kept().wait())

        @pl.when(moves)
        def _():
            for q in range(pieces):
                t_x(1 - x, q).wait_recv()

        order()

    def key_value(which, layers=None, rest=None):
        others(which, layers)
        project(which, keep_pair(which), rest)

    def query(layers=None, rest=None):
        others(2, layers)
        project(2, keep_query, rest)

    def last_down(layer):
        if 0 < layer < last:
            go(downward[2], layer, "down").start()

    def turn():
        lax.fori_loop(0, SECOND_DILATION, angles, 0)
        turn_tokens()

    def moves_pass(q):
        pl.when(moves)(lambda: pass_token(q))

    def run_end(layer):
        begin(layer)
        o_relay(layer, 1)
        todo = events(layer)
        moves_pass(0)
        moves_pass(1)
        pl.when(stays)(turn)
        handle(layer, todo[0])
        moves_pass(2)
        handle(layer, todo[1])
        moves_pass(3)
        pl.when(moves)(turn)
        handle(layer, todo[2])
        if layer == 0:
            key_value(0)
        else:
            query()
            ask().start()
        o_relay(layer, 2)
        for event in todo[3:6]:
            handle(layer, event)
        o_relay(layer, 3)
        o_share(0).start()
        if layer == 0:
            key_value(1)
            halos()
        else:
            key_value(0)
        o_share(0).wait()
        o_share(1).start()
        for event in todo[6:]:
            handle(layer, event)
        if layer == 0:
            query()
        else:
            key_value(1)
            halos()

    def run_mid(layer):
        begin(layer)
        o_relay(layer, 1)
        todo = events(layer)
        split = 9 if layer == last - 1 else 7
        downs = [i for i, event in enumerate(todo) if event[1:3] == ("down", downward[1])]
        for i in range(split):
            if i == 8:
                pl.when(moves)(turn)
            handle(layer, todo[i])
            if i < 4:
                moves_pass(i)
            if i == 1:
                pl.when(stays)(turn)
            if i == 3:
                o_relay(layer, 2)
            if layer == last - 1 and i == max(downs):
                last_down(layer)
        late = todo[split:]

        def finish():
            if late:
                last_down(layer)
            for event in late[:1]:
                handle(layer, event)
            if late:
                pl.when(moves)(turn)
            for event in late[1:]:
                handle(layer, event)

        o_share(0).start()
        pl.when(moves)(finish)
        key_value(0)
        key_value(1)
        halos()
        o_share(0).wait()
        o_share(1).start()
        pl.when(stays)(finish)
        query()

    def run(layer):
        (run_mid if 0 < layer < last else run_end)(layer)

    for layer in range(nz):
        pl.when(z == layer)(functools.partial(run, layer))

    for slot in range(4):
        @pl.when((2 * z + slot < 4) | (asks & (c == 0) & (slot == 3)))
        def _(slot=slot):
            far2[slot] = jnp.zeros(far2.shape[1:], far2.dtype)

    @pl.when(rank == 0)
    def _():
        near_in[...] = jnp.zeros(near_in.shape, near_in.dtype)

    @pl.when(takes_up)
    def _():
        own_up().wait_recv()
        pl.when(gives_up)(lambda: pass_up().start())
        pass_side(2, 2 + c).start()

    pl.when(c == 1)(lambda: pass_side(0, 4).wait_recv())

    @pl.when(helps)
    def _():
        pl.when(c == 0)(lambda: pass_side(0, 5).wait_recv())
        pass_side(2, 3 - c).wait_recv()
        ask().wait_recv()
        help_above()
        answer().start()
        answer_log().start()

    pl.when(rank >= 1)(lambda: near(side).wait_recv())
    near_groups()
    o_share(1).wait()
    o_share(2).start()

    @pl.when(helps)
    def _():
        pass_up().wait_recv()
        pl.when(c == 1)(lambda: pass_side(4, 1).start())
        pl.when(c == 0)(lambda: pass_side(4, 1).wait_recv())

    pl.when(takes_up & gives_up)(lambda: pass_side(2, 3 - c).wait_recv())

    @pl.when(asks)
    def _():
        answer().wait_recv()
        answer_log().wait_recv()
        far_asked()

    pl.when(jnp.logical_not(asks))(far_here)
    unturn()
    for k in range(4):
        self_here = stays & (tp == k)
        pl.when(self_here)(lambda k=k: deal_self(k).start())
        pl.when(jnp.logical_not(self_here))(lambda k=k: deal(k).start())

    o_share(2).wait()
    for h in range(4):
        pltpu.make_async_copy(heads_in.at[h], heads_in.at[h], head_r.at[h]).wait()
    merged = jnp.concatenate([heads_in[h] for h in range(4)], axis=1)
    width = w_out.shape[1]
    for zz in range(nz):
        for yy in range(2):
            rows = jnp.concatenate([out_rows[h % 2, yy, h // 2, zz] for h in range(4)], axis=0)
            s = 2 * zz + yy
            out[:, s * width : (s + 1) * width] = jnp.dot(
                merged, rows, preferred_element_type=jnp.float32
            ).astype(jnp.bfloat16)

    for k in range(4):
        pl.when(jnp.logical_not(stays & (tp == k)))(lambda k=k: deal(k).wait_send())

    @pl.when(moves)
    def _():
        for a in range(3):
            swapped(a).wait_send()
        for q in range(pieces):
            t_y(q).wait_send()
            t_x(x, q).wait_send()

    for a in range(4):
        for zz in range(nz):
            pl.when(has_up & (zz <= z))(lambda a=a, zz=zz: go(a, zz, "up").wait_send())
            pl.when(has_down & (zz >= z))(lambda a=a, zz=zz: go(a, zz, "down").wait_send())
            if a < 3:
                go(a, zz, "side").wait_send()
    pl.when((c == 0) | has_up)(lambda: near(side).wait_send())
    pl.when((c == 0) | helps)(lambda: own_side().wait_send())
    pl.when(gives_up)(lambda: own_up().wait_send())
    pl.when(takes_up)(lambda: pass_side(2, 2 + c).wait_send())
    pl.when(takes_up & gives_up)(lambda: pass_up().wait_send())
    pl.when(helps & (c == 1))(lambda: pass_side(4, 1).wait_send())
    pl.when(asks)(lambda: ask().wait_send())

    @pl.when(helps)
    def _():
        answer().wait_send()
        answer_log().wait_send()


def fits_kernel(n_sp, n_tp, tokens, w_query, w_out):
    tok_rows, depth = tokens.shape
    return (
        n_sp == 2 * LAYERS
        and n_tp == 4
        and w_query.shape[1] == GROUPS * DH
        and w_out.shape[0] == DH
        and w_out.shape[1] % 128 == 0
        and w_query.shape[0] % 16 == 0
        and tok_rows == WIN2
        and 4 * tok_rows == WIN3
        and 4 * WIN1 == tok_rows
    )


def one_kernel(n_sp, tokens, w_query, w_key, w_value, w_out):
    nz = n_sp // 2
    tok_rows, depth = tokens.shape
    cols = w_query.shape[1]
    bf, dma = jnp.bfloat16, pltpu.SemaphoreType.DMA
    return pl.pallas_call(
        functools.partial(layer_kernel, nz),
        out_shape=jax.ShapeDtypeStruct((tok_rows // 4, w_out.shape[1] * n_sp), bf),
        in_specs=[pl.BlockSpec(memory_space=pltpu.HBM)] * 5,
        out_specs=pl.BlockSpec(memory_space=pltpu.VMEM),
        scratch_shapes=[
            pltpu.VMEM((3, depth, cols), bf),
            pltpu.VMEM((3, *w_query.shape), bf),
            pltpu.VMEM((tok_rows, depth), bf),
            pltpu.VMEM((tok_rows, depth), bf),
            pltpu.VMEM((tok_rows, DH), jnp.float32),
            pltpu.VMEM((tok_rows, DH), jnp.float32),
            pltpu.VMEM((GROUPS, tok_rows, DH), bf),
            pltpu.VMEM((2, tok_rows, DH), bf),
            pltpu.VMEM((2, tok_rows + WIN1, DH), bf),
            pltpu.VMEM((2, tok_rows + WIN1, DH), bf),
            pltpu.VMEM((6, 2, tok_rows, DH), bf),
            pltpu.VMEM((2, 2, 2, nz, *w_out.shape), bf),
            pltpu.VMEM((2, tok_rows, DH), bf),
            pltpu.VMEM((4, tok_rows // 4, DH), bf),
            pltpu.VMEM((tok_rows, DH), jnp.float32),
            pltpu.VMEM((tok_rows, 1), jnp.float32),
            pltpu.VMEM((tok_rows, 1), jnp.float32),
            pltpu.VMEM((tok_rows, DH), bf),
            pltpu.VMEM((tok_rows, DH), bf),
            pltpu.VMEM((SECOND_DILATION, 8, DH), jnp.float32),
            pltpu.VMEM((tok_rows, DH), bf),
            pltpu.VMEM((SECOND_DILATION, 8, DH), jnp.float32),
            pltpu.VMEM((tok_rows, cols), jnp.float32),
            dma((3,)), dma((3,)), dma, dma((2, 4)), dma((4,)), dma((4,)), dma((3, n_sp)), dma((4, nz)), dma((4, nz)), dma((3, nz)),
            dma((nz,)), dma((3,)), dma((3,)),
            dma((5,)), dma((6,)), dma, dma, dma((4,)), dma((4,)), dma((3,)), dma((3,)),
        ],
        compiler_params=pltpu.CompilerParams(
            collective_id=0, has_side_effects=True, vmem_limit_bytes=60 * 1024 * 1024
        ),
    )(tokens, w_key, w_value, w_query, w_out)


def on_mesh(n_sp, n_tp, *operands):
    tokens, w_query, _, _, w_out = operands
    if fits_kernel(n_sp, n_tp, tokens, w_query, w_out):
        return one_kernel(n_sp, *operands)
    return on_device(*operands)


def solution(mesh):
    placed = (P("sp", None), P("sp", "tp"), P("sp", "tp"), P("sp", "tp"), P("tp", "sp"))
    body = functools.partial(on_mesh, mesh.shape["sp"], mesh.shape["tp"])
    return jax.shard_map(
        body, mesh=mesh, in_specs=placed, out_specs=P(("sp", "tp"), None), check_vma=False
    )
```

```python
import functools
import math

import jax
import jax.numpy as jnp
from jax import lax
from jax.experimental import pallas as pl
from jax.experimental.pallas import tpu as pltpu
from jax.sharding import PartitionSpec as P

GROUPS = 3
DH = 128
WIN1 = 128
WIN2 = 512
WIN3 = 2048
SECOND_DILATION = 4
THIRD_DILATION = 16


ROPE_BASE = 500000.0

LAYERS = 4


def from_behind(block, axis, distance):
    devices = range(lax.axis_size(axis))
    route = [(i - distance, i) for i in devices if i - distance in devices]
    return lax.ppermute(block, axis, route)


def rotate(projected, offset):
    tok_rows = projected.shape[0]
    head_size = projected.shape[-1]
    half_size = head_size // 2
    positions = (offset + jnp.arange(tok_rows, dtype=jnp.int32)).astype(jnp.float32)
    frequency = 1.0 / ROPE_BASE ** (jnp.arange(0, head_size, 2, dtype=jnp.float32) / head_size)
    angles = (positions[:, None] * frequency[None, :]).reshape(tok_rows, 1, 1, half_size)
    cosine = jnp.cos(angles)
    sine_part = jnp.sin(angles)
    first_half = projected[..., :half_size]
    second_half = projected[..., half_size:]
    return jnp.concatenate(
        [
            first_half * cosine - second_half * sine_part,
            second_half * cosine + first_half * sine_part,
        ],
        axis=-1,
    )


def window_attend(query_part, buffer, steps, stride, offset):
    tok_rows, heads_here, head_size = query_part.shape
    sub_rows = tok_rows // stride
    key_rows = buffer.shape[1] // stride
    query_sub = query_part.reshape(sub_rows, stride, heads_here, head_size).transpose(1, 2, 0, 3)
    pair_sub = buffer.reshape(2, key_rows, stride, heads_here, head_size).transpose(0, 2, 3, 1, 4)
    block_rows = math.gcd(sub_rows, steps) if sub_rows > steps else sub_rows
    block_list = sub_rows // block_rows
    query_blocks = query_sub.reshape(stride, heads_here, block_list, block_rows, head_size)
    key_blocks = jnp.stack(
        [
            pair_sub[:, :, :, index * block_rows : index * block_rows + block_rows + steps]
            for index in range(block_list)
        ],
        axis=3,
    )
    scores = jnp.einsum(
        "zhnqe,zhnke->zhnqk", query_blocks, key_blocks[0], preferred_element_type=jnp.float32
    ) * head_size ** (-0.5)
    query_index = (jnp.arange(block_list, dtype=jnp.int32) * block_rows)[
        :, None, None
    ] + jnp.arange(block_rows, dtype=jnp.int32)[None, :, None]
    key_index = (jnp.arange(block_list, dtype=jnp.int32) * block_rows)[:, None, None] + jnp.arange(
        block_rows + steps, dtype=jnp.int32
    )[None, None, :]
    spacing = query_index + steps - key_index
    residue = jnp.arange(stride, dtype=jnp.int32)[:, None, None, None]
    key_position = offset + (key_index[None] - steps) * stride + residue
    allowed = (spacing[None] >= 0) & (spacing[None] <= steps) & (key_position >= 0)
    scores = jnp.where(allowed[:, None], scores, -jnp.inf)
    row_max = jnp.max(scores, axis=-1)
    exponent = jnp.exp(scores - row_max[..., None])
    totals = jnp.sum(exponent, axis=-1)
    probs = (exponent / totals[..., None]).astype(jnp.bfloat16)
    mixed = jnp.einsum(
        "zhnqk,zhnke->zhnqe", probs, key_blocks[1], preferred_element_type=jnp.float32
    )
    mixed = mixed.reshape(stride, heads_here, sub_rows, head_size).transpose(2, 0, 1, 3)
    log_total = (row_max + jnp.log(totals)).reshape(stride, heads_here, sub_rows).transpose(2, 0, 1)
    return (mixed.reshape(tok_rows, heads_here, head_size), log_total.reshape(tok_rows, heads_here))


def reach_back(key_value, distance_max):
    tok_rows = key_value.shape[1]
    gathered = key_value
    pieces_held = 1
    while pieces_held < distance_max + 1:
        slice_share = min(pieces_held, distance_max + 1 - pieces_held)
        arrived = from_behind(
            gathered[:, gathered.shape[1] - slice_share * tok_rows :], "sp", pieces_held
        )
        gathered = jnp.concatenate([arrived, gathered], axis=1)
        pieces_held = pieces_held + slice_share
    return gathered


def on_device(tokens, w_query, w_key, w_value, w_out):
    tok_rows = tokens.shape[0]
    heads_here = w_out.shape[0] // DH
    offset = lax.axis_index("sp") * tok_rows
    weight_parts = (
        lax.all_gather(w_query, "sp", axis=0, tiled=True),
        lax.all_gather(w_key, "sp", axis=0, tiled=True),
        lax.all_gather(w_value, "sp", axis=0, tiled=True),
    )
    query_raw, key_raw, value_raw = tuple(
        (
            jnp.dot(tokens, weight_rows, preferred_element_type=jnp.float32)
            for weight_rows in weight_parts
        )
    )
    head_shape = (tok_rows, heads_here, GROUPS, DH)
    queries = rotate(query_raw.reshape(head_shape), offset).astype(jnp.bfloat16)
    keys_all = rotate(key_raw.reshape(head_shape), offset).astype(jnp.bfloat16)
    values_all = value_raw.astype(jnp.bfloat16).reshape(head_shape)
    windows = (WIN1, WIN2, WIN3)
    step_sizes = (1, SECOND_DILATION, THIRD_DILATION)
    outputs = []
    log_totals = []
    for group_index in range(GROUPS):
        key_value = jnp.stack([keys_all[:, :, group_index], values_all[:, :, group_index]])
        key_value = key_value.reshape(2, tok_rows, heads_here * DH)
        window = windows[group_index]
        if group_index == 0:
            near_rows = from_behind(key_value[:, tok_rows - window :], "sp", 1)
            buffer = jnp.concatenate([near_rows, key_value], axis=1)
        else:
            distance_max = (window + tok_rows - 1) // tok_rows
            buffer = reach_back(key_value, distance_max)
        group_out, log_total = window_attend(
            queries[:, :, group_index],
            buffer,
            window // step_sizes[group_index],
            step_sizes[group_index],
            offset,
        )
        outputs.append(group_out)
        log_totals.append(log_total)
    group_weights = jax.nn.softmax(jnp.stack(log_totals), axis=0)
    merged = jnp.sum(group_weights[..., None] * jnp.stack(outputs), axis=0).astype(jnp.bfloat16)
    merged = merged.reshape(tok_rows, heads_here * DH)
    w_whole = lax.all_gather(w_out, "sp", axis=1, tiled=True)
    return lax.psum_scatter(
        jnp.dot(merged, w_whole, preferred_element_type=jnp.float32).astype(jnp.bfloat16),
        "tp",
        scatter_dimension=0,
        tiled=True,
    )


def layer_kernel(
    nz,
    tokens, w_key, w_value, w_query, w_out, out,
    weights, stage, tok_in, tok_turned, cosine, sine, queries, pair0, near_own, near_in, far2,
    out_rows, mine, heads_in, got01, top01, sum01, asked, part, part_log, got_part, got_log, begun,
    stage_s, swap_s, tok_k, t_r, ty_s, tx_s, w_r, up_s, down_s, side_s, o_r, o_s, o_r2, far_s, far_r, near_s, near_r, head_s, head_r, part_s, part_r,
):
    tok_rows, depth = tokens.shape
    k_rows, cols = w_key.shape
    sub = tok_rows // THIRD_DILATION
    sub_log = sub.bit_length() - 1
    block = tok_rows // SECOND_DILATION
    tail = WIN1
    last = nz - 1
    sp, tp = lax.axis_index("sp"), lax.axis_index("tp")
    z, y = sp // 2, sp % 2
    x, c = tp // 2, tp % 2
    rank = 2 * z + c
    stays = c == y
    moves = jnp.logical_not(stays)
    has_up, has_down = z < last, z > 0
    side = (sp, 2 * x + 1 - c)
    across_x = (sp, 2 * (1 - x) + c)
    across_y = (2 * z + 1 - y, tp)
    partner = (2 * z + 1 - y, 2 * x + 1 - c)
    above, below = (sp + 2, tp), (sp - 2, tp)
    up_other = (sp + 2, 2 * x)

    def send(src, dst, s_sem, r_sem, where):
        return pltpu.make_async_remote_copy(
            src_ref=src, dst_ref=dst, send_sem=s_sem, recv_sem=r_sem,
            device_id=where, device_id_type=pl.DeviceIdType.MESH,
        )

    parts = (w_key, w_value, w_query)
    upward, downward = (2, 0, 1), (0, 1, 2)

    def chunk(a, s):
        return weights.at[a, pl.ds(pl.multiple_of(s * k_rows, k_rows), k_rows), :]

    def o_chunk(zz):
        return out_rows.at[c, y, x, zz]

    def kept(a):
        return pltpu.make_async_copy(parts[a], chunk(a, rank), w_r.at[a, rank])

    def staged(a):
        return pltpu.make_async_copy(parts[a], stage.at[a], stage_s.at[a])

    def swapped(a):
        there = 2 * z + 1 - c
        return send(stage.at[a], chunk(a, there), swap_s.at[a], w_r.at[a, there], partner)

    def tok_kept():
        return pltpu.make_async_copy(tokens, tok_in, tok_k)

    pieces = ty_s.shape[0]
    piece_rows = tok_rows // 2 // pieces

    def piece_at(half, q):
        return pl.ds(pl.multiple_of(half * (tok_rows // 2) + q * piece_rows, piece_rows), piece_rows)

    def t_y(q):
        at = piece_at(x, q)
        return send(tokens.at[at, :], tok_in.at[at, :], ty_s.at[q], t_r.at[x, q], partner)

    def t_x(half, q):
        at = piece_at(half, q)
        return send(tok_in.at[at, :], tok_in.at[at, :], tx_s.at[q], t_r.at[half, q], across_x)

    def pass_token(q):
        t_y(q).wait_recv()
        t_x(x, q).start()

    def o_kept():
        return pltpu.make_async_copy(w_out, o_chunk(z), o_r.at[z])

    o_kept().start()

    @pl.when(stays)
    def _():
        for a in (2, 0, 1):
            kept(a).start()
        tok_kept().start()

    @pl.when(moves)
    def _():
        for a in (2, 0, 1):
            staged(a).start()

    barrier = pltpu.get_barrier_semaphore()

    def greet(where):
        pl.semaphore_signal(barrier, inc=1, device_id=where, device_id_type=pl.DeviceIdType.MESH)

    for dy in range(2):
        for dx in range(2):
            for dc in range(2):
                if dy + dx + dc:
                    greet((2 * z + (y + dy) % 2, 2 * ((x + dx) % 2) + (c + dc) % 2))
    pl.when(has_up)(lambda: greet(above))
    pl.when(has_down)(lambda: greet(below))
    pl.when(has_up & (c == 1))(lambda: greet(up_other))
    pl.when(has_down & (c == 0))(lambda: greet((sp - 2, 2 * x + 1)))
    pl.semaphore_wait(barrier, 7 + jnp.where(has_up, 1 + c, 0) + jnp.where(has_down, 2 - c, 0))

    def go(a, zz, kind):
        s = 2 * zz + c
        ref = chunk(a, s) if a < 3 else o_chunk(zz)
        r_sem = w_r.at[a, s] if a < 3 else o_r.at[zz]
        s_sem = {"up": up_s, "down": down_s, "side": side_s}[kind].at[a, zz]
        return send(ref, ref, s_sem, r_sem, {"up": above, "down": below, "side": side}[kind])

    def swap_order(layer):
        return {0: (2, 0, 1), last: (0, 1, 2)}.get(layer, (0, 2, 1))

    @pl.when(moves)
    def _():
        for layer in range(nz):
            @pl.when(z == layer)
            def _(layer=layer):
                for a in swap_order(layer):
                    staged(a).wait()
                    swapped(a).start()
        for q in range(pieces):
            t_y(q).start()

    def o_relay(layer, d):
        if layer - d >= 0:
            go(3, layer - d, "up").wait_recv()
            if layer < last:
                go(3, layer - d, "up").start()
        if layer + d < nz:
            go(3, layer + d, "down").wait_recv()
            if layer > 0:
                go(3, layer + d, "down").start()

    def o_share(axis):
        ref, where = (
            (out_rows.at[c, y, x], across_x),
            (out_rows.at[c, y], across_y),
            (out_rows.at[c], side),
        )[axis]
        return send(ref, ref, o_s.at[axis], o_r2.at[axis], where)

    def events(layer):
        listed = []
        for i in range(3):
            for d in range(1, layer + 1):
                listed.append((i * layer + d, "up", upward[i], layer - d, d))
            for d in range(1, last - layer + 1):
                listed.append((i * (last - layer) + d, "down", downward[i], layer + d, d))
        return sorted(listed)

    def handle(layer, event):
        _, kind, a, zz, d = event
        go(a, zz, kind).wait_recv()
        if kind == "up":
            if layer < last:
                go(a, zz, "up").start()
            if d == layer and a == upward[1] and layer < last:
                go(upward[2], layer, "up").start()
        else:
            if layer > 0:
                go(a, zz, "down").start()
        go(a, zz, "side").start()

    def begin(layer):
        o_kept().wait()
        if layer < last:
            go(3, layer, "up").start()
        if layer > 0:
            go(3, layer, "down").start()
        for a in swap_order(layer):
            pl.when(stays)(lambda a=a: kept(a).wait())
            pl.when(moves)(lambda a=a: go(a, layer, "side").wait_recv())
            if layer < last and (layer == 0 or a != upward[2]):
                go(a, layer, "up").start()
            if layer > 0 and (layer == last or a != downward[2]):
                go(a, layer, "down").start()
            go(a, layer, "side").start()

    def row_time(p):
        b, i = p >> sub_log, p & (sub - 1)
        return THIRD_DILATION * i + (b >> 2) + SECOND_DILATION * (b & 3)

    def tail_time(u):
        per = tail // THIRD_DILATION
        b, i = u >> (per.bit_length() - 1), u & (per - 1)
        return THIRD_DILATION * (sub - per + i) + (b >> 2) + SECOND_DILATION * (b & 3) - tok_rows

    def iota(shape, axis):
        return lax.broadcasted_iota(jnp.int32, shape, axis)

    def angles(index, carry):
        at = index * block
        rows = pl.ds(pl.multiple_of(at, block), block)
        pair_at = iota((1, DH), 1) & (DH // 2 - 1)
        freq = jnp.exp(pair_at.astype(jnp.float32) * (-2.0 * math.log(ROPE_BASE) / DH))
        angle = (row_time(iota((block, DH), 0) + at) + rank * tok_rows).astype(jnp.float32) * freq
        cosine[rows, :] = jnp.cos(angle)
        turned = jnp.sin(angle)
        sine[rows, :] = jnp.where(iota((block, DH), 1) < DH // 2, -turned, turned)
        return carry

    def order():
        p = row_time(iota((tok_rows, tok_rows), 0))
        t = iota((tok_rows, tok_rows), 1)
        pick = jnp.where(p == t, 1.0, 0.0).astype(jnp.bfloat16)

        def piece(index, carry):
            at = pl.ds(pl.multiple_of(index * 256, 256), 256)
            tok_turned[:, at] = jnp.dot(
                pick, tok_in[:, at], preferred_element_type=jnp.float32
            ).astype(jnp.bfloat16)
            return carry

        lax.fori_loop(0, depth // 256, piece, 0)

    def product(both, a, span):
        return jnp.dot(tok_turned[both, span], weights[a, span, :], preferred_element_type=jnp.float32)

    def start_product(a, span):
        def piece(index, carry):
            both = pl.ds(pl.multiple_of(index * 2 * block, 2 * block), 2 * block)
            begun[both, :] = product(both, a, span)
            return carry

        lax.fori_loop(0, SECOND_DILATION // 2, piece, 0, unroll=2)

    def project(a, store, rest=None):
        def piece(index, carry):
            both = pl.ds(pl.multiple_of(index * 2 * block, 2 * block), 2 * block)
            whole = product(both, a, slice(0, depth) if rest is None else rest)
            if rest is not None:
                whole = whole + begun[both, :]
            for k in range(2):
                rows = pl.ds(pl.multiple_of((2 * index + k) * block, block), block)
                for g in range(GROUPS):
                    part = whole[k * block : (k + 1) * block, g * DH : (g + 1) * DH]
                    if a != 1:
                        part = part * cosine[rows, :] + pltpu.roll(part, DH // 2, 1) * sine[rows, :]
                    store(2 * index + k, rows, g, part)
            return carry

        lax.fori_loop(0, SECOND_DILATION // 2, piece, 0, unroll=2)

    def keep_pair(which):
        def store(index, rows, g, part):
            if g == 2:
                far2[4 + c, which, rows, :] = part.astype(jnp.bfloat16)
            elif g == 1:
                near_own[which, rows, :] = part.astype(jnp.bfloat16)
            else:
                pair0[which, rows, :] = part.astype(jnp.bfloat16)
                per = tail // THIRD_DILATION
                ends = jnp.concatenate(
                    [part[b * sub + sub - per : (b + 1) * sub] for b in range(4)], axis=0
                )
                at = pl.ds(pl.multiple_of(tok_rows + index * 4 * per, 4 * per), 4 * per)
                near_own[which, at, :] = ends.astype(jnp.bfloat16)

        return store

    def keep_query(index, rows, g, part):
        queries[g, rows, :] = part.astype(jnp.bfloat16)

    def others(a, layers=None):
        for zz in range(nz) if layers is None else layers:
            s = 2 * zz + 1 - c
            send(chunk(a, s), chunk(a, s), side_s.at[a, zz], w_r.at[a, s], side).wait_recv()

    def far(kind, src, dst, where):
        return send(far2.at[src], far2.at[dst], far_s.at[kind], far_r.at[dst], where)

    gives_up, takes_up = z < last - 1, (z > 0) & (z < last)
    helps, asks = z == last - 1, z == last

    def own_side():
        return far(0, 4 + c, 4 + c, side)

    def own_up():
        return far(1, 4 + c, 2 + c, above)

    def pass_side(kind, slot):
        return far(kind, slot, slot, side)

    def pass_up():
        return far(3, 2 + c, c, above)

    def near(where):
        return send(near_own, near_in, near_s, near_r, where)

    def halos():
        pl.when(gives_up)(lambda: own_up().start())
        pl.when(has_up & (c == 1))(lambda: near(up_other).start())
        pl.when(c == 0)(lambda: near(side).start())
        pl.when((c == 0) | helps)(lambda: own_side().start())

    def ask():
        return send(queries.at[2], asked, part_s.at[0], part_r.at[0], below)

    def answer():
        return send(part, got_part, part_s.at[1], part_r.at[1], above)

    def answer_log():
        return send(part_log, got_log, part_s.at[2], part_r.at[2], above)

    scale = DH ** (-0.5)
    far_off = 1 << 24

    def dots(q, k):
        return lax.dot_general(q, k, (((1,), (1,)), ((), ())), preferred_element_type=jnp.float32)

    def soft(scores, time_q, time_k, reach, first):
        gap = time_q - jnp.where(time_k >= first, time_k, far_off)
        scores = jnp.where((gap >= 0) & (gap <= reach), scores, -jnp.inf)
        top = jnp.max(scores, axis=-1, keepdims=True)
        weight = jnp.exp2((scores - top) * (scale * math.log2(math.e)))
        return top * scale, jnp.sum(weight, axis=-1, keepdims=True), weight.astype(jnp.bfloat16)

    def near_groups():
        def piece(index, carry):
            both = pl.ds(pl.multiple_of(index * 2 * block, 2 * block), 2 * block)
            q = queries[0, both, :]
            tails = pl.ds(tok_rows, tail)
            scores = jnp.concatenate([dots(q, near_in[0, tails, :]), dots(q, pair0[0])], axis=1)
            lane = iota((1, tail + tok_rows), 1)
            time_k = jnp.where(lane < tail, tail_time(lane & (tail - 1)), row_time(lane - tail))
            time_q = row_time(iota((2 * block, 1), 0) + index * 2 * block)
            tops, sums, weight = soft(scores, time_q, time_k, WIN1, -rank * tok_rows)
            gots = jnp.dot(weight[:, :tail], near_in[1, tails, :], preferred_element_type=jnp.float32)
            gots += jnp.dot(weight[:, tail:], pair0[1], preferred_element_type=jnp.float32)

            def step_of(place):
                return 4 * (place & (sub - 1)) + (place >> sub_log)

            lane = iota((1, 2 * block), 1)
            step_k = step_of(lane & (block - 1)) + jnp.where(lane < block, -block, 0)
            for k in range(2):
                rows = pl.ds(pl.multiple_of((2 * index + k) * block, block), block)
                half = slice(k * block, (k + 1) * block)
                top0, sum0, got0 = tops[half], sums[half], gots[half]
                q = queries[1, rows, :]
                scores = jnp.concatenate(
                    [dots(q, near_in[0, rows, :]), dots(q, near_own[0, rows, :])], axis=1
                )
                top1, sum1, weight = soft(
                    scores, step_of(iota((block, 1), 0)), step_k, WIN2 // SECOND_DILATION, -rank * block
                )
                got1 = jnp.dot(weight[:, :block], near_in[1, rows, :], preferred_element_type=jnp.float32)
                got1 += jnp.dot(weight[:, block:], near_own[1, rows, :], preferred_element_type=jnp.float32)
                top = jnp.maximum(top0, top1)
                f0, f1 = jnp.exp(top0 - top), jnp.exp(top1 - top)
                got01[rows, :] = f0 * got0 + f1 * got1
                top01[rows, :] = top
                sum01[rows, :] = f0 * sum0 + f1 * sum1
            return carry

        lax.fori_loop(0, SECOND_DILATION // 2, piece, 0, unroll=2)

    def far_piece(index, source, slots, reach_back, first, until=None):
        begin = index * block

        def rows_of(b):
            return pl.ds(pl.multiple_of(begin + b * sub, sub), sub)

        all_scores = []
        for b in range(4):
            keys = jnp.concatenate([far2[slot, 0, rows_of(b), :] for slot in slots], axis=0)
            all_scores.append(dots(source[rows_of(b), :], keys))
        scores = jnp.concatenate(all_scores, axis=0)
        step_q = iota((block, 1), 0) & (sub - 1)
        step_k = iota((1, len(slots) * sub), 1) - reach_back * sub
        seen = step_k if until is None else jnp.where(step_k < until, step_k, far_off)
        top, total, weight = soft(scores, step_q, seen, WIN3 // THIRD_DILATION, first)
        got = []
        for b in range(4):
            vals = jnp.concatenate([far2[slot, 1, rows_of(b), :] for slot in slots], axis=0)
            got.append(
                jnp.dot(weight[b * sub : (b + 1) * sub], vals, preferred_element_type=jnp.float32)
            )
        return top, total, jnp.concatenate(got, axis=0)

    def eye():
        return iota((block, block), 0) == iota((block, block), 1)

    def block_rows(index):
        return pl.ds(pl.multiple_of(index * block, block), block)

    def help_above():
        slots = [2 + c, 3 + c, 4 + c, 5]

        def piece(index, carry):
            top, total, got = far_piece(index, asked, slots, 4, -4 * sub, -c * sub)
            part[block_rows(index), :] = (got / total).astype(jnp.bfloat16)
            row = jnp.sum(jnp.where(eye(), top + jnp.log(total), 0.0), axis=0, keepdims=True)
            part_log[index] = jnp.broadcast_to(row, part_log.shape[1:])
            return carry

        lax.fori_loop(0, SECOND_DILATION, piece, 0, unroll=4)

    def settle(rows, top2, sum2, got2):
        top1 = top01[rows, :]
        top = jnp.maximum(top1, top2)
        f1, f2 = jnp.exp(top1 - top), jnp.exp(top2 - top)
        total = f1 * sum01[rows, :] + f2 * sum2
        mine[0, rows, :] = ((f1 * got01[rows, :] + f2 * got2) / total).astype(jnp.bfloat16)

    def far_here():
        slots = [4 + c - d for d in (4, 3, 2, 1, 0)]

        def piece(index, carry):
            settle(block_rows(index), *far_piece(index, queries.at[2], slots, 4, -rank * sub))
            return carry

        lax.fori_loop(0, SECOND_DILATION, piece, 0, unroll=4)

    def far_asked():
        slots = [3 + c, 4 + c]

        def piece(index, carry):
            rows = block_rows(index)
            top_a, sum_a, got_a = far_piece(index, queries.at[2], slots, 1, -c * sub)
            top_b = jnp.sum(jnp.where(eye(), got_log[index, 0:1, :], 0.0), axis=1, keepdims=True)
            top2 = jnp.maximum(top_a, top_b)
            fa, fb = jnp.exp(top_a - top2), jnp.exp(top_b - top2)
            got2 = fa * got_a + fb * got_part[rows, :].astype(jnp.float32)
            settle(rows, top2, fa * sum_a + fb, got2)
            return carry

        lax.fori_loop(0, SECOND_DILATION, piece, 0, unroll=4)

    def unturn():
        t = iota((tok_rows, tok_rows), 0)
        p = row_time(iota((tok_rows, tok_rows), 1))
        mine[1] = jnp.dot(
            jnp.where(p == t, 1.0, 0.0).astype(jnp.bfloat16), mine[0], preferred_element_type=jnp.float32
        ).astype(jnp.bfloat16)

    head = 2 * x + y
    quarter = tok_rows // 4

    def deal(k):
        return send(
            mine.at[1, pl.ds(k * quarter, quarter), :], heads_in.at[head], head_s.at[k], head_r.at[head], (rank, k)
        )

    def deal_self(k):
        return pltpu.make_async_copy(mine.at[1, pl.ds(k * quarter, quarter), :], heads_in.at[head], head_r.at[head])

    def turn_tokens():
        pl.when(stays)(lambda: tok_kept().wait())

        @pl.when(moves)
        def _():
            for q in range(pieces):
                t_x(1 - x, q).wait_recv()

        order()

    def key_value(which, layers=None, rest=None):
        others(which, layers)
        project(which, keep_pair(which), rest)

    def query(layers=None, rest=None):
        others(2, layers)
        project(2, keep_query, rest)

    def last_down(layer):
        if 0 < layer < last:
            go(downward[2], layer, "down").start()

    def turn():
        lax.fori_loop(0, SECOND_DILATION, angles, 0)
        turn_tokens()

    def moves_pass(q):
        pl.when(moves)(lambda: pass_token(q))

    def run_end(layer):
        begin(layer)
        o_relay(layer, 1)
        todo = events(layer)
        moves_pass(0)
        moves_pass(1)
        pl.when(stays)(turn)
        handle(layer, todo[0])
        moves_pass(2)
        handle(layer, todo[1])
        moves_pass(3)
        pl.when(moves)(turn)
        handle(layer, todo[2])
        if layer == 0:
            key_value(0)
        else:
            query()
            ask().start()
        o_relay(layer, 2)
        for event in todo[3:6]:
            handle(layer, event)
        o_relay(layer, 3)
        o_share(0).start()
        if layer == 0:
            key_value(1)
            halos()
        else:
            key_value(0)
        o_share(0).wait()
        o_share(1).start()
        for event in todo[6:]:
            handle(layer, event)
        if layer == 0:
            query()
        else:
            key_value(1)
            halos()

    def run_mid(layer):
        begin(layer)
        o_relay(layer, 1)
        todo = events(layer)
        split = 9 if layer == last - 1 else 7
        downs = [i for i, event in enumerate(todo) if event[1:3] == ("down", downward[1])]
        for i in range(split):
            if i == 8:
                pl.when(moves)(turn)
            handle(layer, todo[i])
            if i < 4:
                moves_pass(i)
            if i == 1:
                pl.when(stays)(turn)
            if i == 3:
                o_relay(layer, 2)
            if layer == last - 1 and i == max(downs):
                last_down(layer)
        late = todo[split:]

        def finish():
            if late:
                last_down(layer)
            for event in late[:1]:
                handle(layer, event)
            if late:
                pl.when(moves)(turn)
            for event in late[1:]:
                handle(layer, event)

        o_share(0).start()
        pl.when(moves)(finish)
        key_value(0)
        key_value(1)
        halos()
        o_share(0).wait()
        o_share(1).start()
        pl.when(stays)(finish)
        query()

    def run(layer):
        (run_mid if 0 < layer < last else run_end)(layer)

    for layer in range(nz):
        pl.when(z == layer)(functools.partial(run, layer))

    for slot in range(4):
        @pl.when((2 * z + slot < 4) | (asks & (c == 0) & (slot == 3)))
        def _(slot=slot):
            far2[slot] = jnp.zeros(far2.shape[1:], far2.dtype)

    @pl.when(rank == 0)
    def _():
        near_in[...] = jnp.zeros(near_in.shape, near_in.dtype)

    @pl.when(takes_up)
    def _():
        own_up().wait_recv()
        pl.when(gives_up)(lambda: pass_up().start())
        pass_side(2, 2 + c).start()

    pl.when(c == 1)(lambda: pass_side(0, 4).wait_recv())

    @pl.when(helps)
    def _():
        pl.when(c == 0)(lambda: pass_side(0, 5).wait_recv())
        pass_side(2, 3 - c).wait_recv()
        ask().wait_recv()
        help_above()
        answer().start()
        answer_log().start()

    pl.when(rank >= 1)(lambda: near(side).wait_recv())
    near_groups()
    o_share(1).wait()
    o_share(2).start()

    @pl.when(helps)
    def _():
        pass_up().wait_recv()
        pl.when(c == 1)(lambda: pass_side(4, 1).start())
        pl.when(c == 0)(lambda: pass_side(4, 1).wait_recv())

    pl.when(takes_up & gives_up)(lambda: pass_side(2, 3 - c).wait_recv())

    @pl.when(asks)
    def _():
        answer().wait_recv()
        answer_log().wait_recv()
        far_asked()

    pl.when(jnp.logical_not(asks))(far_here)
    unturn()
    for k in range(4):
        self_here = stays & (tp == k)
        pl.when(self_here)(lambda k=k: deal_self(k).start())
        pl.when(jnp.logical_not(self_here))(lambda k=k: deal(k).start())

    o_share(2).wait()
    for h in range(4):
        pltpu.make_async_copy(heads_in.at[h], heads_in.at[h], head_r.at[h]).wait()
    merged = jnp.concatenate([heads_in[h] for h in range(4)], axis=1)
    width = w_out.shape[1]
    for zz in range(nz):
        for yy in range(2):
            rows = jnp.concatenate([out_rows[h % 2, yy, h // 2, zz] for h in range(4)], axis=0)
            s = 2 * zz + yy
            out[:, s * width : (s + 1) * width] = jnp.dot(
                merged, rows, preferred_element_type=jnp.float32
            ).astype(jnp.bfloat16)

    for k in range(4):
        pl.when(jnp.logical_not(stays & (tp == k)))(lambda k=k: deal(k).wait_send())

    @pl.when(moves)
    def _():
        for a in range(3):
            swapped(a).wait_send()
        for q in range(pieces):
            t_y(q).wait_send()
            t_x(x, q).wait_send()

    for a in range(4):
        for zz in range(nz):
            pl.when(has_up & (zz <= z))(lambda a=a, zz=zz: go(a, zz, "up").wait_send())
            pl.when(has_down & (zz >= z))(lambda a=a, zz=zz: go(a, zz, "down").wait_send())
            if a < 3:
                go(a, zz, "side").wait_send()
    pl.when((c == 0) | has_up)(lambda: near(side).wait_send())
    pl.when((c == 0) | helps)(lambda: own_side().wait_send())
    pl.when(gives_up)(lambda: own_up().wait_send())
    pl.when(takes_up)(lambda: pass_side(2, 2 + c).wait_send())
    pl.when(takes_up & gives_up)(lambda: pass_up().wait_send())
    pl.when(helps & (c == 1))(lambda: pass_side(4, 1).wait_send())
    pl.when(asks)(lambda: ask().wait_send())

    @pl.when(helps)
    def _():
        answer().wait_send()
        answer_log().wait_send()


def fits_kernel(n_sp, n_tp, tokens, w_query, w_out):
    tok_rows, depth = tokens.shape
    return (
        n_sp == 2 * LAYERS
        and n_tp == 4
        and w_query.shape[1] == GROUPS * DH
        and w_out.shape[0] == DH
        and w_out.shape[1] % 128 == 0
        and w_query.shape[0] % 16 == 0
        and tok_rows == WIN2
        and 4 * tok_rows == WIN3
        and 4 * WIN1 == tok_rows
    )


def one_kernel(n_sp, tokens, w_query, w_key, w_value, w_out):
    nz = n_sp // 2
    tok_rows, depth = tokens.shape
    cols = w_query.shape[1]
    bf, dma = jnp.bfloat16, pltpu.SemaphoreType.DMA
    return pl.pallas_call(
        functools.partial(layer_kernel, nz),
        out_shape=jax.ShapeDtypeStruct((tok_rows // 4, w_out.shape[1] * n_sp), bf),
        in_specs=[pl.BlockSpec(memory_space=pltpu.HBM)] * 5,
        out_specs=pl.BlockSpec(memory_space=pltpu.VMEM),
        scratch_shapes=[
            pltpu.VMEM((3, depth, cols), bf),
            pltpu.VMEM((3, *w_query.shape), bf),
            pltpu.VMEM((tok_rows, depth), bf),
            pltpu.VMEM((tok_rows, depth), bf),
            pltpu.VMEM((tok_rows, DH), jnp.float32),
            pltpu.VMEM((tok_rows, DH), jnp.float32),
            pltpu.VMEM((GROUPS, tok_rows, DH), bf),
            pltpu.VMEM((2, tok_rows, DH), bf),
            pltpu.VMEM((2, tok_rows + WIN1, DH), bf),
            pltpu.VMEM((2, tok_rows + WIN1, DH), bf),
            pltpu.VMEM((6, 2, tok_rows, DH), bf),
            pltpu.VMEM((2, 2, 2, nz, *w_out.shape), bf),
            pltpu.VMEM((2, tok_rows, DH), bf),
            pltpu.VMEM((4, tok_rows // 4, DH), bf),
            pltpu.VMEM((tok_rows, DH), jnp.float32),
            pltpu.VMEM((tok_rows, 1), jnp.float32),
            pltpu.VMEM((tok_rows, 1), jnp.float32),
            pltpu.VMEM((tok_rows, DH), bf),
            pltpu.VMEM((tok_rows, DH), bf),
            pltpu.VMEM((SECOND_DILATION, 8, DH), jnp.float32),
            pltpu.VMEM((tok_rows, DH), bf),
            pltpu.VMEM((SECOND_DILATION, 8, DH), jnp.float32),
            pltpu.VMEM((tok_rows, cols), jnp.float32),
            dma((3,)), dma((3,)), dma, dma((2, 4)), dma((4,)), dma((4,)), dma((3, n_sp)), dma((4, nz)), dma((4, nz)), dma((3, nz)),
            dma((nz,)), dma((3,)), dma((3,)),
            dma((5,)), dma((6,)), dma, dma, dma((4,)), dma((4,)), dma((3,)), dma((3,)),
        ],
        compiler_params=pltpu.CompilerParams(
            collective_id=0, has_side_effects=True, vmem_limit_bytes=60 * 1024 * 1024
        ),
    )(tokens, w_key, w_value, w_query, w_out)


def on_mesh(n_sp, n_tp, *operands):
    tokens, w_query, _, _, w_out = operands
    if fits_kernel(n_sp, n_tp, tokens, w_query, w_out):
        return one_kernel(n_sp, *operands)
    return on_device(*operands)


def solution(mesh):
    placed = (P("sp", None), P("sp", "tp"), P("sp", "tp"), P("sp", "tp"), P("tp", "sp"))
    body = functools.partial(on_mesh, mesh.shape["sp"], mesh.shape["tp"])
    return jax.shard_map(
        body, mesh=mesh, in_specs=placed, out_specs=P(("sp", "tp"), None), check_vma=False
    )
```
